512 devices in a mesh: sp: 16 (over z), dp: 32 (over y, x, core).
Axes of the slice: x: 4, y: 4, z: 16, core: 2. Of those that a mesh axis runs over, the one named last changes fastest.
Arguments:
- tokens: bfloat16 [64, 1024, 1024], P('dp', 'sp'), may hold values from -6 to 6
- norm_gain: float32 [1024], replicated, may hold values from 0.1 to 1.9
- w_query: bfloat16 [1024, 512], P('dp'), may hold values from -0.1875 to 0.1875
- w_key: bfloat16 [1024, 512], P('dp'), may hold values from -0.1875 to 0.1875
- w_value: bfloat16 [1024, 512], P('dp'), may hold values from -0.1875 to 0.1875
- w_rank_forward: bfloat16 [1024, 16], P('dp'), may hold values from -0.1875 to 0.1875
- w_rank_backward: bfloat16 [1024, 16], P('dp'), may hold values from -0.1875 to 0.1875
- up_forward: bfloat16 [16, 512], replicated, may hold values from -1.5 to 1.5
- up_backward: bfloat16 [16, 512], replicated, may hold values from -1.5 to 1.5
- bias_forward: float32 [512], replicated, may hold values from -1.5 to 3
- bias_backward: float32 [512], replicated, may hold values from -1.5 to 3
- out_gain: float32 [32], replicated, may hold values from 0.1 to 1.9
- w_out: bfloat16 [512, 1024], P('dp'), may hold values from -0.25 to 0.25
Outputs:
- mixed_out: bfloat16 [64, 1024, 1024], P('dp', 'sp')
The draws below stay inside these ranges and needn't reach their ends.
All inputs are finite; a program needn't handle non-finite values.
Results may differ from the reference program's by a relative error of at most 0.005.
Values may be sent and summed in bfloat16 or wider, within the bound.
No kernel may reach another device: no remote copies, remote signals or barrier semaphores. Data moves between devices by JAX's collectives and lax.ppermute only.
A program may use at most 64 MiB of HBM per device.

```python
import jax
import jax.numpy as jnp
from jax import lax

D = 1024
HK = 32
HV = 32
RANK = 16
BLOCK = 64
SEQS = 64
SEQ = 1024
DK = 512
DV = 512


def steps_of(stream_key, shape, split, least, top_value):
    gain = 1.0
    for dim, parts in split:
        draws = jax.random.uniform(jax.random.fold_in(jax.random.fold_in(stream_key, 6), dim), (parts,), jnp.float32, least / len(split), top_value / len(split))
        gain = gain * jnp.repeat(jnp.exp(draws), shape[dim] // parts).reshape((-1,) + (1,) * (len(shape) - 1 - dim))
    return gain


def scatter_about(rng, extent, spread, limit, shards=(), dtype=jnp.bfloat16):
    values = jax.random.normal(rng, extent, jnp.float32) * spread
    if len(shards) > 0:
        values = steps_of(rng, extent, shards, -0.22, 0.18) * values
    return jnp.clip(values, min=-limit, max=limit).astype(dtype)


def setup_inputs(seed: int = 0) -> dict:
    key_of = jax.random.split(jax.random.key(seed), 14)
    tokens = scatter_about(key_of[0], (SEQS, SEQ, D), 1.0, 6.0, ((0, 32), (1, 16)))
    norm_gain = jnp.clip(1.0 + 0.18 * jax.random.normal(key_of[1], (D,), jnp.float32), 0.1, 1.9)
    w_query = scatter_about(key_of[2], (D, DK), D ** -0.5, 0.1875, ((0, 32),))
    w_key = scatter_about(key_of[3], (D, DK), D ** -0.5, 0.1875, ((0, 32),))
    w_value = scatter_about(key_of[4], (D, DV), D ** -0.5, 0.1875, ((0, 32),))
    w_rank_forward = scatter_about(key_of[5], (D, RANK), D ** -0.5, 0.1875, ((0, 32),))
    w_rank_backward = scatter_about(key_of[6], (D, RANK), D ** -0.5, 0.1875, ((0, 32),))
    up_forward = scatter_about(key_of[7], (RANK, DK), RANK ** -0.5, 1.5)
    up_backward = scatter_about(key_of[8], (RANK, DK), RANK ** -0.5, 1.5)
    bias_forward = jnp.clip(jax.random.uniform(key_of[9], (DK,), jnp.float32, -1.5, 3.0), -1.5, 3.0)
    bias_backward = jnp.clip(jax.random.uniform(key_of[10], (DK,), jnp.float32, -1.5, 3.0), -1.5, 3.0)
    out_gain = jnp.clip(1.0 + 0.18 * jax.random.normal(key_of[11], (HV,), jnp.float32), 0.1, 1.9)
    w_out = scatter_about(key_of[12], (DV, D), DV ** -0.5, 0.25, ((0, 32),))
    return dict(tokens=tokens, norm_gain=norm_gain, w_query=w_query, w_key=w_key, w_value=w_value, w_rank_forward=w_rank_forward, w_rank_backward=w_rank_backward, up_forward=up_forward, up_backward=up_backward, bias_forward=bias_forward, bias_backward=bias_backward, out_gain=out_gain, w_out=w_out)


eps = 1e-06
precise = lax.Precision.HIGHEST

def rms_norm(values, norm_scale):
    return values * lax.rsqrt(lax.optimization_barrier(jnp.mean(values * values, axis=-1, keepdims=True)) + eps) * norm_scale

def one_way(queries, key_rows, value_rows, decay_rates):
    head_count, length, key_width = queries.shape
    value_width = value_rows.shape[-1]
    blocks = length // BLOCK

    def in_blocks(tensor):
        return tensor.reshape(head_count, blocks, BLOCK, tensor.shape[-1])
    query_blocks = in_blocks(queries)
    key_blocks = in_blocks(key_rows)
    value_blocks = in_blocks(value_rows)
    running = jnp.cumsum(in_blocks(decay_rates), axis=2)
    closing = running[:, :, -1:, :]
    query_decayed = query_blocks * jnp.exp(running)
    key_inverse = key_blocks * jnp.exp(-running)
    key_remain = key_blocks * jnp.exp(closing - running)
    triangle = jnp.tril(jnp.ones((BLOCK, BLOCK), jnp.float32))
    scores = jnp.einsum('hnid,hnjd->hnij', query_decayed, key_inverse, precision=precise) * triangle
    within = jnp.einsum('hnij,hnjv->hniv', scores, value_blocks, precision=precise)
    block_decay = jnp.exp(closing[:, :, 0, :])

    def advance(carried, inputs):
        query_now, key_now, value_now, decay_now = inputs
        emitted = jnp.einsum('hid,hdv->hiv', query_now, carried, precision=precise)
        carried = decay_now[..., None] * carried + jnp.einsum('hid,hiv->hdv', key_now, value_now, precision=precise)
        return (carried, emitted)
    initial = jnp.zeros((head_count, key_width, value_width), jnp.float32)
    stacked = tuple((jnp.moveaxis(tensor, 1, 0) for tensor in (query_decayed, key_remain, value_blocks, block_decay)))
    final_state, across = lax.scan(advance, initial, stacked)
    return (within + jnp.moveaxis(across, 0, 1)).reshape(head_count, length, value_width)

def both_ways(queries, key_rows, value_rows, rates_forward, rates_backward):
    forward = one_way(queries, key_rows, value_rows, rates_forward)
    backward = one_way(jnp.flip(queries, 1), jnp.flip(key_rows, 1), jnp.flip(value_rows, 1), jnp.flip(rates_backward, 1))
    return forward + jnp.flip(backward, 1)

def by_head(tensor, head_width):
    length = tensor.shape[0]
    return tensor.reshape(length, -1, head_width).transpose(1, 0, 2).astype(jnp.float32)

def attend(queries, key_rows, value_rows, rates_forward, rates_backward, out_gain):
    combined = both_ways(by_head(queries, HK) * HK ** (-0.5), by_head(key_rows, HK), by_head(value_rows, HV), by_head(rates_forward, HK), by_head(rates_backward, HK))
    normed = rms_norm(combined, out_gain).astype(jnp.bfloat16)
    return normed.transpose(1, 0, 2).reshape(normed.shape[1], -1)

def reference(tokens, norm_gain, w_query, w_key, w_value, w_rank_forward, w_rank_backward, up_forward, up_backward, bias_forward, bias_backward, out_gain, w_out):
    rate_scale = 2.0 / SEQ

    def one_sequence(sequence):
        normed = rms_norm(sequence.astype(jnp.float32), norm_gain).astype(jnp.bfloat16)
        queries = jnp.dot(normed, w_query, preferred_element_type=jnp.float32).astype(jnp.bfloat16)
        key_rows = jnp.dot(normed, w_key, preferred_element_type=jnp.float32).astype(jnp.bfloat16)
        value_rows = jnp.dot(normed, w_value, preferred_element_type=jnp.float32).astype(jnp.bfloat16)
        rank_forward = jnp.dot(normed, w_rank_forward, preferred_element_type=jnp.float32).astype(jnp.bfloat16)
        rank_backward = jnp.dot(normed, w_rank_backward, preferred_element_type=jnp.float32).astype(jnp.bfloat16)
        rates_forward = jax.nn.log_sigmoid(jnp.dot(rank_forward, up_forward, preferred_element_type=jnp.float32) + bias_forward) * rate_scale
        rates_backward = jax.nn.log_sigmoid(jnp.dot(rank_backward, up_backward, preferred_element_type=jnp.float32) + bias_backward) * rate_scale
        attended = attend(queries, key_rows, value_rows, rates_forward, rates_backward, out_gain)
        return jnp.dot(attended, w_out, preferred_element_type=jnp.float32).astype(jnp.bfloat16)
    return lax.map(one_sequence, tokens)
```

```python
import functools

import jax
import jax.numpy as jnp
from jax import lax
from jax.experimental import pallas as pl
from jax.experimental.pallas import tpu as pltpu
from jax.sharding import Mesh
from jax.sharding import PartitionSpec as P

DP = ("dp_0", "dp_1", "dp_2")
PLANE = ("dp_0", "dp_1")
HEAD = 32
HEADS = 16
WIDTH = 512
BLOCK = 64
LANES = 128
EPS = 1e-06
f32 = jnp.float32
bf16 = jnp.bfloat16


def dot(a, b):
    return jnp.dot(a, b, preferred_element_type=f32)


def dot_tn(a, b):
    return lax.dot_general(a, b, (((0,), (0,)), ((), ())), preferred_element_type=f32)


def dot_nt(a, b):
    return lax.dot_general(a, b, (((1,), (1,)), ((), ())), preferred_element_type=f32)


def halves(x):
    high = x.astype(bf16)
    return high, (x - high.astype(f32)).astype(bf16)


def grid_of(shape):
    return lax.broadcasted_iota(jnp.int32, shape, 0), lax.broadcasted_iota(jnp.int32, shape, 1)


def as_bf16(mask):
    return jnp.where(mask, 1.0, 0.0).astype(bf16)


def norm_kernel(tokens_ref, gain_ref, normed_ref):
    values = tokens_ref[...].astype(f32)
    scale = lax.rsqrt(jnp.mean(values * values, axis=-1, keepdims=True) + EPS)
    normed = (values * scale * gain_ref[...]).astype(bf16)
    for core in range(2):
        normed_ref[core] = jnp.concatenate(
            [normed[:, (2 * i + core) * 32 : (2 * i + core) * 32 + 32] for i in range(16)], axis=1
        )


def block_kernel(
    core_ref, normed_ref, own_ref, other_ref, up_ref, bias_ref,
    payload_ref, keys_ref, values_ref, running_ref,
):
    core = core_ref[0]
    length = BLOCK * HEADS
    projected = dot(normed_ref[core], own_ref[...]) + dot(normed_ref[1 - core], other_ref[...])
    rounded = projected.astype(bf16)
    keys = rounded[:, :WIDTH]
    values = rounded[:, WIDTH : 2 * WIDTH]
    ranks = rounded[:, 2 * WIDTH :]
    keys_ref[...] = keys
    values_ref[...] = values
    gates = dot(ranks, up_ref[...]) + bias_ref[...]
    rates = jax.nn.log_sigmoid(gates) * (2.0 / length)
    high, low = halves(rates)
    row, col = grid_of((128, 128))
    same = (row // BLOCK) == (col // BLOCK)

    def summed(mask, span):
        ones = as_bf16(mask)
        return dot(ones, high[:, span]) + dot(ones, low[:, span])

    fwd, bwd = slice(0, WIDTH), slice(WIDTH, 2 * WIDTH)
    running_ref[:, fwd] = summed(same & (col <= row), fwd)
    running_ref[:, bwd] = summed(same & (col >= row), bwd)
    keys32 = keys.astype(f32)
    remain = (
        (keys32 * jnp.exp(summed(same & (col > row), fwd))).astype(bf16),
        (keys32 * jnp.exp(summed(same & (col < row), bwd))).astype(bf16),
    )
    closing = 0.0
    for way, span in ((0, fwd), (1, bwd)):
        pick = as_bf16((col // HEAD) == 2 * way + row // BLOCK)
        closing = closing + dot_tn(high[:, span], pick) + dot_tn(low[:, span], pick)
    close_high, close_low = halves(closing)
    lane = lax.broadcasted_iota(jnp.int32, (WIDTH, LANES), 1)
    close_both = jnp.where(lane % 2 == 0, close_high.astype(f32), close_low.astype(f32))
    payload_ref[:, LANES:] = close_both.astype(bf16)
    diagonal = (row // HEAD) == (col // HEAD)
    erow, ecol = grid_of((4 * LANES, LANES))
    fold = as_bf16(((erow // LANES) * HEAD + erow % HEAD) == ecol)
    for group in range(4):
        lanes = slice(group * LANES, (group + 1) * LANES)
        parts = []
        for way in range(2):
            for seq in range(2):
                span = slice(seq * BLOCK, (seq + 1) * BLOCK)
                state = dot_tn(remain[way][span, lanes], values[span, lanes])
                parts.append(jnp.where(diagonal, state, 0.0).astype(bf16))
        folded = dot(jnp.concatenate(parts, axis=1), fold)
        payload_ref[lanes, :LANES] = folded.astype(bf16)


def scan_kernel(payload_ref, out_ref):
    row, col = grid_of((LANES, LANES))
    spread = as_bf16(((row // HEAD) == (col // HEAD)) & (row % HEAD < 2))
    closing = dot(payload_ref[:, LANES:], spread)
    decay = jnp.exp(closing)
    states = payload_ref[:, :LANES].astype(f32)
    lane = lax.broadcasted_iota(jnp.int32, (HEAD, LANES), 1)
    ahead = [None] * HEADS
    behind = [None] * HEADS

    def at(x, i):
        return x[i * HEAD : (i + 1) * HEAD, :]

    carried = jnp.zeros((HEAD, LANES), f32)
    for i in range(HEADS):
        ahead[i] = carried
        carried = at(decay, i) * carried + at(states, i)
    carried = jnp.zeros((HEAD, LANES), f32)
    for i in range(HEADS - 1, -1, -1):
        behind[i] = carried
        carried = at(decay, i) * carried + at(states, i)
    for i in range(HEADS):
        out_ref[i * HEAD : (i + 1) * HEAD, :] = jnp.where(
            lane < LANES // 2, ahead[i], behind[i]
        ).astype(bf16)


def query_kernel(
    core_ref, normed_ref, own_ref, other_ref, keys_ref, values_ref, running_ref,
    within_ref, queries_ref,
):
    core = core_ref[0]

    def weights(ref):
        both = jnp.concatenate([ref[:, 16:32, :WIDTH], ref[:, 16:32, WIDTH:]], axis=1)
        return both.reshape(WIDTH, WIDTH)

    projected = dot(normed_ref[core], weights(own_ref)) + dot(
        normed_ref[1 - core], weights(other_ref)
    )
    queries = projected.astype(bf16).astype(f32) * HEAD ** (-0.5)
    keys = keys_ref[...].astype(f32)
    decayed, inverse = [], []
    for way in range(2):
        running = running_ref[:, way * WIDTH : (way + 1) * WIDTH]
        decayed.append((queries * jnp.exp(running)).astype(bf16))
        inverse.append((keys * jnp.exp(-running)).astype(bf16))
        queries_ref[:, way * WIDTH : (way + 1) * WIDTH] = decayed[way]
    row, col = grid_of((4 * BLOCK, LANES))
    own_lanes = (row // BLOCK) == (col // HEAD)
    own_lanes_bf = as_bf16(own_lanes)
    srow, scol = grid_of((4 * BLOCK, BLOCK))
    lower = (srow % BLOCK) >= scol
    upper = (srow % BLOCK) <= scol
    for seq in range(2):
        span = slice(seq * BLOCK, (seq + 1) * BLOCK)
        for group in range(4):
            lanes = slice(group * LANES, (group + 1) * LANES)
            scores = 0.0
            for way, mask in ((0, lower), (1, upper)):
                one = decayed[way][span, lanes]
                stacked = jnp.concatenate([one] * 4, axis=0) * own_lanes_bf
                scores = scores + jnp.where(mask, dot_nt(stacked, inverse[way][span, lanes]), 0.0)
            spread = jnp.where(own_lanes, dot(scores.astype(bf16), values_ref[span, lanes]), 0.0)
            within_ref[span, lanes] = (
                spread[:BLOCK] + spread[BLOCK : 2 * BLOCK]
                + spread[2 * BLOCK : 3 * BLOCK] + spread[3 * BLOCK :]
            )


def out_kernel(core_ref, states_ref, within_ref, queries_ref, gain_ref, own_ref, other_ref, out_ref):
    core = core_ref[0]
    row, col = grid_of((LANES, LANES))
    diagonal = (row // HEAD) == (col // HEAD)
    rows = []
    for seq in range(2):
        span = slice(seq * BLOCK, (seq + 1) * BLOCK)
        pieces = []
        for group in range(4):
            lanes = slice(group * LANES, (group + 1) * LANES)
            total = within_ref[span, lanes]
            for way in range(2):
                widen = as_bf16(row == (2 * way + seq) * HEAD + col % HEAD)
                full = dot(states_ref[lanes, :], widen)
                full = jnp.where(diagonal, full, 0.0).astype(bf16)
                query = queries_ref[span, way * WIDTH + group * LANES : way * WIDTH + (group + 1) * LANES]
                total = total + dot(query, full)
            pieces.append(total)
        rows.append(jnp.concatenate(pieces, axis=1))
    combined = jnp.concatenate(rows, axis=0)
    high, low = halves(combined * combined)
    ones = as_bf16(diagonal)
    mean = jnp.concatenate(
        [
            dot(high[:, g * LANES : (g + 1) * LANES], ones)
            + dot(low[:, g * LANES : (g + 1) * LANES], ones)
            for g in range(4)
        ],
        axis=1,
    ) * (1.0 / HEAD)
    attended = (combined * lax.rsqrt(mean + EPS) * gain_ref[...]).astype(bf16)
    prow, pcol = grid_of((WIDTH, WIDTH))
    source = ((pcol % 256) // 16) * 32 + (pcol // 256) * 16 + pcol % 16
    shuffled = dot(attended, as_bf16(prow == source)).astype(bf16)
    first, second = shuffled[:, :256], shuffled[:, 256:]
    mine = jnp.where(core == 0, first, second)
    theirs = jnp.where(core == 0, second, first)
    out_ref[...] = (
        dot(mine, own_ref[:, :16, :].reshape(256, 1024))
        + dot(theirs, other_ref[:, :16, :].reshape(256, 1024))
    ).astype(bf16)


VMEM = pl.BlockSpec(memory_space=pltpu.VMEM)
SMEM = pl.BlockSpec(memory_space=pltpu.SMEM)


def call(kernel, outs, specs, cycles, *args):
    many = isinstance(outs, tuple)
    return pl.pallas_call(
        kernel,
        out_shape=outs,
        in_specs=specs,
        out_specs=(VMEM,) * len(outs) if many else VMEM,
        cost_estimate=pl.CostEstimate(flops=cycles, bytes_accessed=1 << 20, transcendentals=0),
        name=kernel.__name__,
    )(*args)


def spread_out(block):
    return jnp.broadcast_to(block[None], (16, *block.shape))


def swapped(x):
    return lax.ppermute(x, "dp_2", [(0, 1), (1, 0)])


def body(
    tokens, norm_gain, w_query, w_key, w_value, w_rank_forward, w_rank_backward,
    up_forward, up_backward, bias_forward, bias_backward, out_gain, w_out,
):
    seqs, toks, width = tokens.shape
    rows = seqs * toks
    shape = jax.ShapeDtypeStruct
    core = lax.axis_index("dp_2").astype(jnp.int32).reshape(1)
    first = jnp.concatenate(
        [w_key, w_value, w_rank_forward, w_rank_backward, jnp.zeros((32, 96), bf16)], axis=1
    )
    own = lax.all_to_all(spread_out(first), PLANE, 0, 0)
    other = swapped(own)
    normed = call(
        norm_kernel, shape((2, rows, 512), bf16), [VMEM, VMEM], 1 << 28,
        tokens.reshape(rows, width), norm_gain.reshape(1, width),
    )
    up = jnp.zeros((128, 1024), bf16)
    up = up.at[:16, :512].set(up_forward).at[16:32, 512:].set(up_backward)
    bias = jnp.concatenate([bias_forward, bias_backward]).reshape(1, 1024)
    payload, keys, values, running = call(
        block_kernel,
        (
            shape((WIDTH, 2 * LANES), bf16), shape((rows, WIDTH), bf16),
            shape((rows, WIDTH), bf16), shape((rows, 2 * WIDTH), f32),
        ),
        [SMEM] + [VMEM] * 5, 1 << 30,
        core, normed, own.reshape(512, 1152), other.reshape(512, 1152), up, bias,
    )
    inbound = lax.all_to_all(payload.reshape(HEADS, HEAD, 2 * LANES), "sp", 0, 0)
    second = jnp.concatenate(
        [w_out, jnp.concatenate([w_query[:16], w_query[16:]], axis=1)], axis=0
    )
    second, _ = lax.optimization_barrier((second, payload))
    own2 = lax.all_to_all(spread_out(second), PLANE, 0, 0)
    other2 = swapped(own2)
    states = call(
        scan_kernel, shape((WIDTH, LANES), bf16), [VMEM], 1 << 28,
        inbound.reshape(WIDTH, 2 * LANES),
    )
    returned = lax.all_to_all(states.reshape(HEADS, HEAD, LANES), "sp", 0, 0)
    within, queries = call(
        query_kernel,
        (shape((rows, WIDTH), f32), shape((rows, 2 * WIDTH), bf16)),
        [SMEM] + [VMEM] * 6, 1 << 30,
        core, normed, own2, other2, keys, values, running,
    )
    mixed = call(
        out_kernel, shape((rows, width), bf16), [SMEM] + [VMEM] * 6, 1 << 30,
        core, returned.reshape(WIDTH, LANES), within, queries,
        jnp.tile(out_gain, HEADS).reshape(1, WIDTH), own2, other2,
    )
    return mixed.reshape(seqs, toks, width)


def solution(mesh):
    finer = Mesh(mesh.devices.reshape(mesh.shape["sp"], 4, 4, 2), ("sp", "dp_0", "dp_1", "dp_2"))
    rows = P(DP, None)
    in_specs = (
        P(DP, "sp", None), P(), rows, rows, rows, rows, rows, P(), P(), P(), P(), P(), rows,
    )
    return jax.shard_map(
        body, mesh=finer, in_specs=in_specs, out_specs=P(DP, "sp", None), check_vma=False
    )
```

```python
import jax
import jax.numpy as jnp
from jax import lax
from jax.experimental import pallas as pl
from jax.experimental.pallas import tpu as pltpu
from jax.sharding import Mesh
from jax.sharding import PartitionSpec as P

DP = ("dp_0", "dp_1", "dp_2")
PLANE = ("dp_0", "dp_1")
HEAD = 32
HEADS = 16
WIDTH = 512
BLOCK = 64
LANES = 128
EPS = 1e-06
f32 = jnp.float32
bf16 = jnp.bfloat16


def dot(a, b):
    return jnp.dot(a, b, preferred_element_type=f32)


def dot_tn(a, b):
    return lax.dot_general(a, b, (((0,), (0,)), ((), ())), preferred_element_type=f32)


def dot_nt(a, b):
    return lax.dot_general(a, b, (((1,), (1,)), ((), ())), preferred_element_type=f32)


def halves(x):
    high = x.astype(bf16)
    return high, (x - high.astype(f32)).astype(bf16)


def grid_of(shape):
    return lax.broadcasted_iota(jnp.int32, shape, 0), lax.broadcasted_iota(jnp.int32, shape, 1)


def as_bf16(mask):
    return jnp.where(mask, 1.0, 0.0).astype(bf16)


def pack_kernel(key_ref, value_ref, forward_ref, backward_ref, out_ref):
    block = jnp.concatenate(
        [key_ref[...], value_ref[...], forward_ref[...], backward_ref[...], jnp.zeros((32, 96), bf16)],
        axis=1,
    )
    for i in range(16):
        out_ref[i] = block


def join_kernel(query_ref, query_in_ref, out_ref, out_in_ref, queries_ref, outs_ref):
    count = query_ref.shape[0]
    queries_ref[:count] = query_ref[...]
    queries_ref[count:] = query_in_ref[...]
    outs_ref[:count] = out_ref[...]
    outs_ref[count:] = out_in_ref[...]


def slot_of(index, axis):
    apart = index ^ lax.axis_index(axis)
    return apart ^ (apart >> 1)


def in_order(ref, major, minor):
    pieces = []
    for y in range(4):
        for x in range(4):
            at = {"dp_0": slot_of(y, "dp_0"), "dp_1": slot_of(x, "dp_1")}
            pieces.append(ref[at[major] * 4 + at[minor]])
    return jnp.concatenate(pieces, axis=0)


def norm_kernel(tokens_ref, gain_ref, normed_ref):
    values = tokens_ref[...].astype(f32)
    scale = lax.rsqrt(jnp.mean(values * values, axis=-1, keepdims=True) + EPS)
    normed = (values * scale * gain_ref[...]).astype(bf16)
    for core in range(2):
        normed_ref[core] = jnp.concatenate(
            [normed[:, (2 * i + core) * 32 : (2 * i + core) * 32 + 32] for i in range(16)], axis=1
        )


def block_kernel(
    normed_ref, own_ref, other_ref, up_forward_ref, up_backward_ref,
    bias_forward_ref, bias_backward_ref, payload_ref, keys_ref, values_ref, running_ref,
):
    core = lax.axis_index("dp_2")
    length = BLOCK * HEADS
    projected = dot(normed_ref[core], own_ref[...]) + dot(normed_ref[1 - core], other_ref[...])
    rounded = projected.astype(bf16)
    keys = rounded[:, :WIDTH]
    values = rounded[:, WIDTH : 2 * WIDTH]
    ranks = rounded[:, 2 * WIDTH :]
    keys_ref[...] = keys
    values_ref[...] = values
    gates = jnp.concatenate(
        [
            dot(ranks[:, :16], up_forward_ref[...]) + bias_forward_ref[...],
            dot(ranks[:, 16:32], up_backward_ref[...]) + bias_backward_ref[...],
        ],
        axis=1,
    )
    rates = jax.nn.log_sigmoid(gates) * (2.0 / length)
    high, low = halves(rates)
    row, col = grid_of((128, 128))
    same = (row // BLOCK) == (col // BLOCK)

    def summed(mask, span):
        ones = as_bf16(mask)
        return dot(ones, high[:, span]) + dot(ones, low[:, span])

    fwd, bwd = slice(0, WIDTH), slice(WIDTH, 2 * WIDTH)
    running_ref[:, fwd] = summed(same & (col <= row), fwd)
    running_ref[:, bwd] = summed(same & (col >= row), bwd)
    keys32 = keys.astype(f32)
    remain = (
        halves(keys32 * jnp.exp(summed(same & (col > row), fwd))),
        halves(keys32 * jnp.exp(summed(same & (col < row), bwd))),
    )
    closing = 0.0
    for way, span in ((0, fwd), (1, bwd)):
        pick = as_bf16((col // HEAD) == 2 * way + row // BLOCK)
        closing = closing + dot_tn(high[:, span], pick) + dot_tn(low[:, span], pick)
    close_high, close_low = halves(closing)
    lane = lax.broadcasted_iota(jnp.int32, (WIDTH, LANES), 1)
    close_both = jnp.where(lane % 2 == 0, close_high.astype(f32), close_low.astype(f32))
    payload_ref[:, LANES:] = close_both.astype(bf16)
    diagonal = (row // HEAD) == (col // HEAD)
    erow, ecol = grid_of((4 * LANES, LANES))
    fold = as_bf16(((erow // LANES) * HEAD + erow % HEAD) == ecol)
    for group in range(4):
        lanes = slice(group * LANES, (group + 1) * LANES)
        parts = []
        for way in range(2):
            for seq in range(2):
                span = slice(seq * BLOCK, (seq + 1) * BLOCK)
                value = values[span, lanes]
                state = dot_tn(remain[way][0][span, lanes], value) + dot_tn(
                    remain[way][1][span, lanes], value
                )
                parts.append(jnp.where(diagonal, state, 0.0).astype(bf16))
        folded = dot(jnp.concatenate(parts, axis=1), fold)
        payload_ref[lanes, :LANES] = folded.astype(bf16)


def scan_kernel(payload_ref, out_ref):
    row, col = grid_of((LANES, LANES))
    spread = as_bf16(((row // HEAD) == (col // HEAD)) & (row % HEAD < 2))
    closing = dot(payload_ref[:, LANES:], spread)
    decay = jnp.exp(closing)
    states = payload_ref[:, :LANES].astype(f32)
    lane = lax.broadcasted_iota(jnp.int32, (HEAD, LANES), 1)
    ahead = [None] * HEADS
    behind = [None] * HEADS

    def at(x, i):
        return x[i * HEAD : (i + 1) * HEAD, :]

    carried = jnp.zeros((HEAD, LANES), f32)
    for i in range(HEADS):
        ahead[i] = carried
        carried = at(decay, i) * carried + at(states, i)
    carried = jnp.zeros((HEAD, LANES), f32)
    for i in range(HEADS - 1, -1, -1):
        behind[i] = carried
        carried = at(decay, i) * carried + at(states, i)
    for i in range(HEADS):
        out_ref[i * HEAD : (i + 1) * HEAD, :] = jnp.where(
            lane < LANES // 2, ahead[i], behind[i]
        ).astype(bf16)


def prepare_kernel(keys_ref, running_ref, inverse_ref, decay_ref):
    keys = keys_ref[...].astype(f32)
    for way in range(2):
        lanes = slice(way * WIDTH, (way + 1) * WIDTH)
        running = running_ref[:, lanes]
        inverse_ref[:, lanes] = (keys * jnp.exp(-running)).astype(bf16)
        decay_ref[:, lanes] = jnp.exp(running)


def query_kernel(
    normed_ref, own_ref, other_ref, inverse_ref, values_ref, decay_ref,
    within_ref, high_ref, low_ref,
):
    core = lax.axis_index("dp_2")

    projected = dot(normed_ref[core], in_order(own_ref, "dp_1", "dp_0")) + dot(
        normed_ref[1 - core], in_order(other_ref, "dp_1", "dp_0")
    )
    queries = projected.astype(bf16).astype(f32) * HEAD ** (-0.5)
    decayed = []
    for way in range(2):
        lanes = slice(way * WIDTH, (way + 1) * WIDTH)
        high, low = halves(queries * decay_ref[:, lanes])
        decayed.append(high)
        high_ref[:, lanes] = high
        low_ref[:, lanes] = low
    row, col = grid_of((4 * BLOCK, LANES))
    own_lanes = (row // BLOCK) == (col // HEAD)
    own_lanes_bf = as_bf16(own_lanes)
    srow, scol = grid_of((4 * BLOCK, BLOCK))
    lower = (srow % BLOCK) >= scol
    upper = (srow % BLOCK) <= scol
    for seq in range(2):
        span = slice(seq * BLOCK, (seq + 1) * BLOCK)
        for group in range(4):
            lanes = slice(group * LANES, (group + 1) * LANES)
            scores = 0.0
            for way, mask in ((0, lower), (1, upper)):
                one = decayed[way][span, lanes]
                wide = slice(way * WIDTH + group * LANES, way * WIDTH + (group + 1) * LANES)
                stacked = jnp.concatenate([one] * 4, axis=0) * own_lanes_bf
                scores = scores + jnp.where(mask, dot_nt(stacked, inverse_ref[span, wide]), 0.0)
            spread = jnp.where(own_lanes, dot(scores.astype(bf16), values_ref[span, lanes]), 0.0)
            within_ref[span, lanes] = (
                spread[:BLOCK] + spread[BLOCK : 2 * BLOCK]
                + spread[2 * BLOCK : 3 * BLOCK] + spread[3 * BLOCK :]
            )


def out_kernel(
    states_ref, within_ref, high_ref, low_ref, gain_ref, own_ref, other_ref, out_ref
):
    core = lax.axis_index("dp_2")
    row, col = grid_of((LANES, LANES))
    diagonal = (row // HEAD) == (col // HEAD)
    rows = []
    for seq in range(2):
        span = slice(seq * BLOCK, (seq + 1) * BLOCK)
        pieces = []
        for group in range(4):
            lanes = slice(group * LANES, (group + 1) * LANES)
            total = within_ref[span, lanes]
            for way in range(2):
                widen = as_bf16(row == (2 * way + seq) * HEAD + col % HEAD)
                full = dot(states_ref[lanes, :], widen)
                full = jnp.where(diagonal, full, 0.0).astype(bf16)
                wide = slice(way * WIDTH + group * LANES, way * WIDTH + (group + 1) * LANES)
                total = total + dot(high_ref[span, wide], full) + dot(low_ref[span, wide], full)
            pieces.append(total)
        rows.append(jnp.concatenate(pieces, axis=1))
    combined = jnp.concatenate(rows, axis=0)
    high, low = halves(combined * combined)
    ones = as_bf16(diagonal)
    mean = jnp.concatenate(
        [
            dot(high[:, g * LANES : (g + 1) * LANES], ones)
            + dot(low[:, g * LANES : (g + 1) * LANES], ones)
            for g in range(4)
        ],
        axis=1,
    ) * (1.0 / HEAD)
    attended = (combined * lax.rsqrt(mean + EPS) * gain_ref[...]).astype(bf16)
    prow, pcol = grid_of((WIDTH, WIDTH))
    source = ((pcol % 256) // 16) * 32 + (pcol // 256) * 16 + pcol % 16
    shuffled = dot(attended, as_bf16(prow == source)).astype(bf16)
    first, second = shuffled[:, :256], shuffled[:, 256:]
    mine = jnp.where(core == 0, first, second)
    theirs = jnp.where(core == 0, second, first)
    out_ref[...] = (
        dot(mine, in_order(own_ref, "dp_0", "dp_1"))
        + dot(theirs, in_order(other_ref, "dp_0", "dp_1"))
    ).astype(bf16)


VMEM = pl.BlockSpec(memory_space=pltpu.VMEM)


def call(kernel, outs, specs, cycles, *args):
    many = isinstance(outs, tuple)
    return pl.pallas_call(
        kernel,
        out_shape=outs,
        in_specs=specs,
        out_specs=(VMEM,) * len(outs) if many else VMEM,
        cost_estimate=pl.CostEstimate(flops=cycles, bytes_accessed=1 << 20, transcendentals=0),
        compiler_params=pltpu.CompilerParams(vmem_limit_bytes=16 << 20),
    )(*args)


def swapped(x):
    return lax.ppermute(x, "dp_2", [(0, 1), (1, 0)])


def body(
    tokens, norm_gain, w_query, w_key, w_value, w_rank_forward, w_rank_backward,
    up_forward, up_backward, bias_forward, bias_backward, out_gain, w_out,
):
    seqs, toks, width = tokens.shape
    rows = seqs * toks
    shape = jax.ShapeDtypeStruct
    send = call(
        pack_kernel, shape((16, 32, 1152), bf16), [VMEM] * 4, 1 << 26,
        w_key, w_value, w_rank_forward, w_rank_backward,
    )
    own = lax.all_to_all(send, PLANE, 0, 0)
    other = swapped(own)
    normed = call(
        norm_kernel, shape((2, rows, 512), bf16), [VMEM, VMEM], 1 << 28,
        tokens.reshape(rows, width), norm_gain.reshape(1, width),
    )
    query_blocks, out_blocks = w_query[None], w_out[None]

    def widen(query_axis, out_axis, flip):
        pairs = [(i, i ^ flip) for i in range(4)]
        query_in = lax.ppermute(query_blocks, query_axis, pairs)
        out_in = lax.ppermute(out_blocks, out_axis, pairs)
        count = 2 * query_blocks.shape[0]
        return call(
            join_kernel, (shape((count, 32, 512), bf16), shape((count, 16, 1024), bf16)),
            [VMEM] * 4, 1 << 26, query_blocks, query_in, out_blocks, out_in,
        )

    query_blocks, out_blocks = widen("dp_0", "dp_1", 1)
    query_blocks, out_blocks = widen("dp_0", "dp_1", 3)
    query_blocks, out_blocks = widen("dp_1", "dp_0", 1)
    query_blocks, out_blocks = widen("dp_1", "dp_0", 3)
    payload, keys, values, running = call(
        block_kernel,
        (
            shape((WIDTH, 2 * LANES), bf16), shape((rows, WIDTH), bf16),
            shape((rows, WIDTH), bf16), shape((rows, 2 * WIDTH), f32),
        ),
        [VMEM] * 7, 1 << 30,
        normed, own.reshape(512, 1152), other.reshape(512, 1152), up_forward, up_backward,
        bias_forward.reshape(1, WIDTH), bias_backward.reshape(1, WIDTH),
    )
    inbound = lax.all_to_all(payload.reshape(HEADS, HEAD, 2 * LANES), "sp", 0, 0)
    inverse, decay = call(
        prepare_kernel,
        (shape((rows, 2 * WIDTH), bf16), shape((rows, 2 * WIDTH), f32)),
        [VMEM] * 2, 1 << 28, keys, running,
    )
    query_other = swapped(query_blocks)
    out_other = swapped(out_blocks)
    states = call(
        scan_kernel, shape((WIDTH, LANES), bf16), [VMEM], 1 << 28,
        inbound.reshape(WIDTH, 2 * LANES),
    )
    returned = lax.all_to_all(states.reshape(HEADS, HEAD, LANES), "sp", 0, 0)
    within, high, low = call(
        query_kernel,
        (
            shape((rows, WIDTH), f32), shape((rows, 2 * WIDTH), bf16),
            shape((rows, 2 * WIDTH), bf16),
        ),
        [VMEM] * 6, 1 << 30,
        normed, query_blocks, query_other, inverse, values, decay,
    )
    mixed = call(
        out_kernel, shape((rows, width), bf16), [VMEM] * 7, 1 << 30,
        returned.reshape(WIDTH, LANES), within, high, low,
        jnp.tile(out_gain, HEADS).reshape(1, WIDTH), out_blocks, out_other,
    )
    return mixed.reshape(seqs, toks, width)


def solution(mesh):
    finer = Mesh(mesh.devices.reshape(mesh.shape["sp"], 4, 4, 2), ("sp", "dp_0", "dp_1", "dp_2"))
    rows = P(DP, None)
    in_specs = (
        P(DP, "sp", None), P(), rows, rows, rows, rows, rows, P(), P(), P(), P(), P(), rows,
    )

    return jax.shard_map(
        body, mesh=finer, in_specs=in_specs, out_specs=P(DP, "sp", None), check_vma=False
    )
```

```python
import jax
import jax.numpy as jnp
from jax import lax
from jax.experimental import pallas as pl
from jax.experimental.pallas import tpu as pltpu
from jax.sharding import Mesh
from jax.sharding import PartitionSpec as P

DP = ("dp_0", "dp_1", "dp_2")
PLANE = ("dp_0", "dp_1")
HEAD = 32
HEADS = 16
WIDTH = 512
BLOCK = 64
LANES = 128
FIRST = 2 * WIDTH + LANES
EPS = 1e-06
f32 = jnp.float32
bf16 = jnp.bfloat16


def dot(a, b):
    return jnp.dot(a, b, preferred_element_type=f32)


def dot_tn(a, b):
    return lax.dot_general(a, b, (((0,), (0,)), ((), ())), preferred_element_type=f32)


def dot_nt(a, b):
    return lax.dot_general(a, b, (((1,), (1,)), ((), ())), preferred_element_type=f32)


def halves(x):
    high = x.astype(bf16)
    return high, (x - high.astype(f32)).astype(bf16)


def grid_of(shape):
    return lax.broadcasted_iota(jnp.int32, shape, 0), lax.broadcasted_iota(jnp.int32, shape, 1)


def as_bf16(mask):
    return jnp.where(mask, 1.0, 0.0).astype(bf16)


def pack_kernel(
    key_hbm, value_hbm, query_hbm, mix_hbm, forward_hbm, backward_hbm,
    out_ref, key_ref, value_ref, query_ref, mix_ref, forward_ref, backward_ref, sems,
):
    sources = (key_hbm, value_hbm, query_hbm, mix_hbm, forward_hbm, backward_hbm)
    targets = (key_ref, value_ref, query_ref, mix_ref, forward_ref, backward_ref)
    copies = [
        pltpu.make_async_copy(source, target, sems.at[i])
        for i, (source, target) in enumerate(zip(sources, targets))
    ]
    for copy in copies:
        copy.start()
    for copy in copies:
        copy.wait()
    row, col = grid_of((16, LANES))
    ranks = dot_tn(forward_ref[...], as_bf16(row == col)) + dot_tn(
        backward_ref[...], as_bf16(row + 16 == col)
    )
    mix = jnp.concatenate([mix_ref[:, :WIDTH], mix_ref[:, WIDTH:]], axis=0)
    even = lax.rem(lax.axis_index("sp"), 2) == 0
    shared = jnp.where(even, query_ref[...].astype(f32), mix.astype(f32)).astype(bf16)
    block = jnp.concatenate(
        [key_ref[...], value_ref[...], ranks.astype(bf16), shared], axis=1
    )
    for i in range(16):
        out_ref[i] = block


def norm_kernel(tokens_ref, gain_ref, normed_ref):
    values = tokens_ref[...].astype(f32)
    scale = lax.rsqrt(jnp.mean(values * values, axis=-1, keepdims=True) + EPS)
    normed = (values * scale * gain_ref[...]).astype(bf16)
    for core in range(2):
        normed_ref[core] = jnp.concatenate(
            [normed[:, (2 * i + core) * 32 : (2 * i + core) * 32 + 32] for i in range(16)], axis=1
        )


def rates_of(ranks, up_forward_ref, up_backward_ref, bias_forward_ref, bias_backward_ref):
    gates = jnp.concatenate(
        [
            dot(ranks[:, :16], up_forward_ref[...]) + bias_forward_ref[...],
            dot(ranks[:, 16:32], up_backward_ref[...]) + bias_backward_ref[...],
        ],
        axis=1,
    )
    return halves(jax.nn.log_sigmoid(gates) * (2.0 / (BLOCK * HEADS)))


def summed(parts, mask, way):
    row, col = grid_of((LANES, LANES))
    ones = as_bf16(mask(row, col) & ((row // BLOCK) == (col // BLOCK)))
    lanes = slice(way * WIDTH, (way + 1) * WIDTH)
    return dot(ones, parts[0][:, lanes]) + dot(ones, parts[1][:, lanes])


def block_kernel(
    normed_ref, own_ref, other_ref, up_forward_ref, up_backward_ref,
    bias_forward_ref, bias_backward_ref, payload_ref, rounded_ref,
):
    core = lax.axis_index("dp_2")
    projected = dot(normed_ref[core], own_ref[...].reshape(WIDTH, FIRST)) + dot(
        normed_ref[1 - core], other_ref[...].reshape(WIDTH, FIRST)
    )
    rounded = projected.astype(bf16)
    rounded_ref[...] = rounded
    values = rounded[:, WIDTH : 2 * WIDTH]
    parts = rates_of(
        rounded[:, 2 * WIDTH :], up_forward_ref, up_backward_ref, bias_forward_ref, bias_backward_ref
    )
    high, low = parts
    row, col = grid_of((LANES, LANES))
    fwd, bwd = slice(0, WIDTH), slice(WIDTH, 2 * WIDTH)
    keys32 = rounded[:, :WIDTH].astype(f32)
    remain = (
        halves(keys32 * jnp.exp(summed(parts, lambda r, c: c > r, 0))),
        halves(keys32 * jnp.exp(summed(parts, lambda r, c: c < r, 1))),
    )
    hrow, hcol = grid_of((HEADS, WIDTH))
    mine = hrow == hcol // HEAD
    erow, ecol = grid_of((WIDTH, LANES))
    srow, scol = grid_of((8, 128))
    close = 0.0
    for way, span in ((0, fwd), (1, bwd)):
        pick = as_bf16(srow == scol // BLOCK)
        sums = dot(pick, high[:, span]) + dot(pick, low[:, span])
        for seq in range(2):
            line = jnp.where(mine, sums[seq : seq + 1], 0.0)
            place = as_bf16(ecol == (2 * way + seq) * HEAD + erow % HEAD)
            line_high, line_low = halves(line)
            both = jnp.concatenate([line_high, line_low], axis=0)
            close = close + dot(both, place)
    tail = lax.broadcasted_iota(jnp.int32, (HEADS, 16, LANES), 1)
    payload_ref[:, HEAD:, :] = jnp.where(
        tail == 0,
        close[:HEADS][:, None, :],
        jnp.where(tail == 1, close[HEADS:][:, None, :], 0.0),
    ).astype(bf16)
    diagonal = (row // HEAD) == (col // HEAD)
    erow, ecol = grid_of((4 * LANES, LANES))
    fold = as_bf16(((erow // LANES) * HEAD + erow % HEAD) == ecol)
    for group in range(4):
        lanes = slice(group * LANES, (group + 1) * LANES)
        parts = []
        for way in range(2):
            for seq in range(2):
                span = slice(seq * BLOCK, (seq + 1) * BLOCK)
                value = values[span, lanes]
                state = dot_tn(remain[way][0][span, lanes], value) + dot_tn(
                    remain[way][1][span, lanes], value
                )
                parts.append(jnp.where(diagonal, state, 0.0).astype(bf16))
        folded = dot(jnp.concatenate(parts, axis=1), fold).astype(bf16)
        payload_ref[4 * group : 4 * group + 4, :HEAD, :] = folded.reshape(4, HEAD, LANES)


def scan_kernel(payload_ref, out_ref):
    row, col = grid_of((LANES, LANES))
    spread = as_bf16((row // HEAD) == (col // HEAD))
    crow, ccol = grid_of((HEAD, LANES))
    mine = ccol % HEAD == crow
    lines = payload_ref[:, HEAD : HEAD + 16, :].astype(f32)
    closing = 0.0
    for part in range(2):
        line = jnp.where(mine[None], lines[:, part : part + 1, :], 0.0)
        closing = closing + dot(line.astype(bf16).reshape(WIDTH, LANES), spread)
    decay = jnp.exp(closing)
    states = payload_ref[:, :HEAD, :].astype(f32).reshape(WIDTH, LANES)
    lane = lax.broadcasted_iota(jnp.int32, (HEAD, LANES), 1)
    ahead = [None] * HEADS
    behind = [None] * HEADS

    def at(x, i):
        return x[i * HEAD : (i + 1) * HEAD, :]

    carried = jnp.zeros((HEAD, LANES), f32)
    for i in range(HEADS):
        ahead[i] = carried
        carried = at(decay, i) * carried + at(states, i)
    carried = jnp.zeros((HEAD, LANES), f32)
    for i in range(HEADS - 1, -1, -1):
        behind[i] = carried
        carried = at(decay, i) * carried + at(states, i)
    for i in range(HEADS):
        out_ref[i * HEAD : (i + 1) * HEAD, :] = jnp.where(
            lane < LANES // 2, ahead[i], behind[i]
        ).astype(bf16)


def sort_kernel(near_ref, far_ref, query_ref, mix_ref):
    parity = lax.rem(lax.axis_index("sp"), 2)

    @pl.when(parity == 0)
    def _():
        query_ref[...] = near_ref[...]
        mix_ref[...] = far_ref[...]

    @pl.when(parity == 1)
    def _():
        query_ref[...] = far_ref[...]
        mix_ref[...] = near_ref[...]


def query_kernel(
    normed_ref, own_ref, other_ref, rounded_ref, up_forward_ref, up_backward_ref,
    bias_forward_ref, bias_backward_ref, out_ref,
):
    core = lax.axis_index("dp_2")
    projected = dot(normed_ref[core], own_ref[...].reshape(WIDTH, WIDTH)) + dot(
        normed_ref[1 - core], other_ref[...].reshape(WIDTH, WIDTH)
    )
    queries = projected.astype(bf16).astype(f32) * HEAD ** (-0.5)
    keys = rounded_ref[:, :WIDTH].astype(f32)
    parts = rates_of(
        rounded_ref[:, 2 * WIDTH :], up_forward_ref, up_backward_ref, bias_forward_ref, bias_backward_ref
    )
    decayed, inverse = [], []
    for way, mask in ((0, lambda r, c: c <= r), (1, lambda r, c: c >= r)):
        running = summed(parts, mask, way)
        product = queries * jnp.exp(running)
        out_ref[:, (way + 1) * WIDTH : (way + 2) * WIDTH] = product
        decayed.append(product.astype(bf16))
        inverse.append((keys * jnp.exp(-running)).astype(bf16))
    row, col = grid_of((4 * BLOCK, LANES))
    own_lanes = (row // BLOCK) == (col // HEAD)
    own_lanes_bf = as_bf16(own_lanes)
    srow, scol = grid_of((4 * BLOCK, BLOCK))
    lower = (srow % BLOCK) >= scol
    upper = (srow % BLOCK) <= scol
    for seq in range(2):
        span = slice(seq * BLOCK, (seq + 1) * BLOCK)
        for group in range(4):
            lanes = slice(group * LANES, (group + 1) * LANES)
            scores = 0.0
            for way, mask in ((0, lower), (1, upper)):
                one = decayed[way][span, lanes]
                stacked = jnp.concatenate([one] * 4, axis=0) * own_lanes_bf
                scores = scores + jnp.where(mask, dot_nt(stacked, inverse[way][span, lanes]), 0.0)
            spread = jnp.where(own_lanes, dot(scores.astype(bf16), rounded_ref[span, slice(WIDTH + group * LANES, WIDTH + (group + 1) * LANES)]), 0.0)
            out_ref[span, lanes] = (
                spread[:BLOCK] + spread[BLOCK : 2 * BLOCK]
                + spread[2 * BLOCK : 3 * BLOCK] + spread[3 * BLOCK :]
            )


def out_kernel(
    states_ref, parts_ref, gain_ref, own_ref, other_ref, out_ref
):
    core = lax.axis_index("dp_2")
    row, col = grid_of((LANES, LANES))
    diagonal = (row // HEAD) == (col // HEAD)
    rows = []
    for seq in range(2):
        span = slice(seq * BLOCK, (seq + 1) * BLOCK)
        pieces = []
        for group in range(4):
            lanes = slice(group * LANES, (group + 1) * LANES)
            total = parts_ref[span, lanes]
            for way in range(2):
                widen = as_bf16(row == (2 * way + seq) * HEAD + col % HEAD)
                full = dot(states_ref[lanes, :], widen)
                full = jnp.where(diagonal, full, 0.0).astype(bf16)
                start = (way + 1) * WIDTH + group * LANES
                high, low = halves(parts_ref[span, start : start + LANES])
                total = total + dot(high, full) + dot(low, full)
            pieces.append(total)
        rows.append(jnp.concatenate(pieces, axis=1))
    combined = jnp.concatenate(rows, axis=0)
    high, low = halves(combined * combined)
    ones = as_bf16(diagonal)
    mean = jnp.concatenate(
        [
            dot(high[:, g * LANES : (g + 1) * LANES], ones)
            + dot(low[:, g * LANES : (g + 1) * LANES], ones)
            for g in range(4)
        ],
        axis=1,
    ) * (1.0 / HEAD)
    attended = (combined * lax.rsqrt(mean + EPS) * gain_ref[...]).astype(bf16)
    prow, pcol = grid_of((WIDTH, WIDTH))
    source = ((pcol % 256) // 16) * 32 + (pcol // 256) * 16 + pcol % 16
    shuffled = dot(attended, as_bf16(prow == source)).astype(bf16)
    first, second = shuffled[:, :256], shuffled[:, 256:]
    mine = jnp.where(core == 0, first, second)
    theirs = jnp.where(core == 0, second, first)
    for half in range(2):
        rows = slice(half * 16, half * 16 + 16)
        out_ref[:, half * WIDTH : (half + 1) * WIDTH] = (
            dot(mine, own_ref[:, rows, :].reshape(256, WIDTH))
            + dot(theirs, other_ref[:, rows, :].reshape(256, WIDTH))
        ).astype(bf16)


VMEM = pl.BlockSpec(memory_space=pltpu.VMEM)


def call(kernel, outs, specs, cycles, *args, scratch=(), grant=16 << 20):
    many = isinstance(outs, tuple)
    return pl.pallas_call(
        kernel,
        out_shape=outs,
        in_specs=specs,
        out_specs=(VMEM,) * len(outs) if many else VMEM,
        scratch_shapes=scratch,
        cost_estimate=pl.CostEstimate(flops=cycles, bytes_accessed=1 << 20, transcendentals=0),
        compiler_params=pltpu.CompilerParams(vmem_limit_bytes=grant),
    )(*args)


def swapped(x):
    return lax.ppermute(x, "dp_2", [(0, 1), (1, 0)])


def body(
    tokens, norm_gain, w_query, w_key, w_value, w_rank_forward, w_rank_backward,
    up_forward, up_backward, bias_forward, bias_backward, out_gain, w_out,
):
    seqs, toks, width = tokens.shape
    rows = seqs * toks
    shape = jax.ShapeDtypeStruct
    hbm = pl.BlockSpec(memory_space=pltpu.HBM)
    sources = (w_key, w_value, w_query, w_out, w_rank_forward.T, w_rank_backward.T)
    send = call(
        pack_kernel, shape((16, 32, FIRST + WIDTH), bf16), [hbm] * 6, 1 << 26, *sources,
        scratch=[pltpu.VMEM(x.shape, bf16) for x in sources] + [pltpu.SemaphoreType.DMA((6,))],
        grant=None,
    )
    own = lax.all_to_all(send, PLANE, 0, 0)
    first_own = own[:, :, :FIRST]
    other = swapped(first_own)
    near_part = own[:, :, FIRST:]
    far_part = lax.ppermute(near_part, "sp", [(i, i ^ 1) for i in range(16)])
    normed = call(
        norm_kernel, shape((2, rows, 512), bf16), [VMEM, VMEM], 1 << 28,
        tokens.reshape(rows, width), norm_gain.reshape(1, width),
    )
    decays = (
        up_forward, up_backward, bias_forward.reshape(1, WIDTH), bias_backward.reshape(1, WIDTH)
    )
    payload, rounded = call(
        block_kernel, (shape((HEADS, 48, LANES), bf16), shape((rows, FIRST), bf16)),
        [VMEM] * 7, 1 << 30, normed, first_own, other, *decays,
    )
    inbound = lax.all_to_all(payload, "sp", 0, 0)
    query_own, mix_own = call(
        sort_kernel, (shape(near_part.shape, bf16),) * 2, [VMEM] * 2, 1 << 28,
        near_part, far_part,
    )
    query_other = swapped(query_own)
    mix_other = swapped(mix_own)
    states = call(
        scan_kernel, shape((WIDTH, LANES), bf16), [VMEM], 1 << 28,
        inbound,
    )
    returned = lax.all_to_all(states.reshape(HEADS, HEAD, LANES), "sp", 0, 0)
    parts = call(
        query_kernel, shape((rows, 3 * WIDTH), f32), [VMEM] * 8, 1 << 30,
        normed, query_own, query_other, rounded, *decays,
    )
    mixed = call(
        out_kernel, shape((rows, width), bf16), [VMEM] * 5, 1 << 30,
        returned.reshape(WIDTH, LANES), parts,
        jnp.tile(out_gain, HEADS).reshape(1, WIDTH), mix_own, mix_other,
    )
    return mixed.reshape(seqs, toks, width)


def solution(mesh):
    finer = Mesh(mesh.devices.reshape(mesh.shape["sp"], 4, 4, 2), ("sp", "dp_0", "dp_1", "dp_2"))
    rows = P(DP, None)
    in_specs = (
        P(DP, "sp", None), P(), rows, rows, rows, rows, rows, P(), P(), P(), P(), P(), rows,
    )

    return jax.shard_map(
        body, mesh=finer, in_specs=in_specs, out_specs=P(DP, "sp", None), check_vma=False
    )
```

```python
import jax
import jax.numpy as jnp
from jax import lax
from jax.experimental import pallas as pl
from jax.experimental.pallas import tpu as pltpu
from jax.sharding import Mesh
from jax.sharding import PartitionSpec as P

DP = ("dp_0", "dp_1", "dp_2")
PLANE = ("dp_0", "dp_1")
HEAD = 32
HEADS = 16
WIDTH = 512
BLOCK = 64
LANES = 128
ALL = 3 * WIDTH + LANES
EPS = 1e-06
f32 = jnp.float32
bf16 = jnp.bfloat16


def dot(a, b):
    return jnp.dot(a, b, preferred_element_type=f32)


def dot_tn(a, b):
    return lax.dot_general(a, b, (((0,), (0,)), ((), ())), preferred_element_type=f32)


def dot_nt(a, b):
    return lax.dot_general(a, b, (((1,), (1,)), ((), ())), preferred_element_type=f32)


def halves(x):
    high = x.astype(bf16)
    return high, (x - high.astype(f32)).astype(bf16)


def grid_of(shape):
    return lax.broadcasted_iota(jnp.int32, shape, 0), lax.broadcasted_iota(jnp.int32, shape, 1)


def as_bf16(mask):
    return jnp.where(mask, 1.0, 0.0).astype(bf16)


def pack_kernel(
    key_hbm, value_hbm, query_hbm, forward_hbm, backward_hbm,
    out_ref, key_ref, value_ref, query_ref, forward_ref, backward_ref, sems,
):
    sources = (key_hbm, value_hbm, query_hbm, forward_hbm, backward_hbm)
    targets = (key_ref, value_ref, query_ref, forward_ref, backward_ref)
    copies = [
        pltpu.make_async_copy(source, target, sems.at[i])
        for i, (source, target) in enumerate(zip(sources, targets))
    ]
    for copy in copies:
        copy.start()
    for copy in copies:
        copy.wait()
    row, col = grid_of((16, LANES))
    ranks = dot_tn(forward_ref[...], as_bf16(row == col)) + dot_tn(
        backward_ref[...], as_bf16(row + 16 == col)
    )
    block = jnp.concatenate(
        [key_ref[...], value_ref[...], query_ref[...], ranks.astype(bf16)], axis=1
    )
    for i in range(16):
        out_ref[i] = block


def join_kernel(first_ref, second_ref, out_ref):
    count = first_ref.shape[0]
    out_ref[:count] = first_ref[...]
    out_ref[count:] = second_ref[...]


def slot_of(index, axis):
    apart = index ^ lax.axis_index(axis)
    return apart ^ (apart >> 1)


def in_order(ref):
    pieces = []
    for y in range(4):
        for x in range(4):
            pieces.append(ref[slot_of(x, "dp_1") * 4 + slot_of(y, "dp_0")])
    return jnp.concatenate(pieces, axis=0)


def norm_kernel(tokens_ref, gain_ref, normed_ref):
    values = tokens_ref[...].astype(f32)
    scale = lax.rsqrt(jnp.mean(values * values, axis=-1, keepdims=True) + EPS)
    normed = (values * scale * gain_ref[...]).astype(bf16)
    for core in range(2):
        normed_ref[core] = jnp.concatenate(
            [normed[:, (2 * i + core) * 32 : (2 * i + core) * 32 + 32] for i in range(16)], axis=1
        )


def rates_of(ranks, up_forward_ref, up_backward_ref, bias_forward_ref, bias_backward_ref):
    gates = jnp.concatenate(
        [
            dot(ranks[:, :16], up_forward_ref[...]) + bias_forward_ref[...],
            dot(ranks[:, 16:32], up_backward_ref[...]) + bias_backward_ref[...],
        ],
        axis=1,
    )
    return halves(jax.nn.log_sigmoid(gates) * (2.0 / (BLOCK * HEADS)))


def summed(parts, mask, way):
    row, col = grid_of((LANES, LANES))
    ones = as_bf16(mask(row, col) & ((row // BLOCK) == (col // BLOCK)))
    lanes = slice(way * WIDTH, (way + 1) * WIDTH)
    return dot(ones, parts[0][:, lanes]) + dot(ones, parts[1][:, lanes])


def block_kernel(
    normed_ref, own_ref, other_ref, up_forward_ref, up_backward_ref,
    bias_forward_ref, bias_backward_ref, payload_ref, rounded_ref,
):
    core = lax.axis_index("dp_2")
    projected = dot(normed_ref[core], own_ref[...].reshape(WIDTH, ALL)) + dot(
        normed_ref[1 - core], other_ref[...].reshape(WIDTH, ALL)
    )
    rounded = projected.astype(bf16)
    rounded_ref[...] = rounded
    values = rounded[:, WIDTH : 2 * WIDTH]
    parts = rates_of(
        rounded[:, 3 * WIDTH :], up_forward_ref, up_backward_ref, bias_forward_ref, bias_backward_ref
    )
    high, low = parts
    row, col = grid_of((LANES, LANES))
    fwd, bwd = slice(0, WIDTH), slice(WIDTH, 2 * WIDTH)
    keys32 = rounded[:, :WIDTH].astype(f32)
    remain = (
        halves(keys32 * jnp.exp(summed(parts, lambda r, c: c > r, 0))),
        halves(keys32 * jnp.exp(summed(parts, lambda r, c: c < r, 1))),
    )
    hrow, hcol = grid_of((HEADS, WIDTH))
    mine = hrow == hcol // HEAD
    erow, ecol = grid_of((WIDTH, LANES))
    srow, scol = grid_of((8, 128))
    close = 0.0
    for way, span in ((0, fwd), (1, bwd)):
        pick = as_bf16(srow == scol // BLOCK)
        sums = dot(pick, high[:, span]) + dot(pick, low[:, span])
        for seq in range(2):
            line = jnp.where(mine, sums[seq : seq + 1], 0.0)
            place = as_bf16(ecol == (2 * way + seq) * HEAD + erow % HEAD)
            line_high, line_low = halves(line)
            both = jnp.concatenate([line_high, line_low], axis=0)
            close = close + dot(both, place)
    tail = lax.broadcasted_iota(jnp.int32, (HEADS, 16, LANES), 1)
    payload_ref[:, HEAD:, :] = jnp.where(
        tail == 0,
        close[:HEADS][:, None, :],
        jnp.where(tail == 1, close[HEADS:][:, None, :], 0.0),
    ).astype(bf16)
    diagonal = (row // HEAD) == (col // HEAD)
    erow, ecol = grid_of((4 * LANES, LANES))
    fold = as_bf16(((erow // LANES) * HEAD + erow % HEAD) == ecol)
    for group in range(4):
        lanes = slice(group * LANES, (group + 1) * LANES)
        parts = []
        for way in range(2):
            for seq in range(2):
                span = slice(seq * BLOCK, (seq + 1) * BLOCK)
                value = values[span, lanes]
                state = dot_tn(remain[way][0][span, lanes], value) + dot_tn(
                    remain[way][1][span, lanes], value
                )
                parts.append(jnp.where(diagonal, state, 0.0).astype(bf16))
        folded = dot(jnp.concatenate(parts, axis=1), fold).astype(bf16)
        payload_ref[4 * group : 4 * group + 4, :HEAD, :] = folded.reshape(4, HEAD, LANES)


def scan_kernel(payload_ref, out_ref):
    row, col = grid_of((LANES, LANES))
    spread = as_bf16((row // HEAD) == (col // HEAD))
    crow, ccol = grid_of((HEAD, LANES))
    mine = ccol % HEAD == crow
    lines = payload_ref[:, HEAD : HEAD + 16, :].astype(f32)
    closing = 0.0
    for part in range(2):
        line = jnp.where(mine[None], lines[:, part : part + 1, :], 0.0)
        closing = closing + dot(line.astype(bf16).reshape(WIDTH, LANES), spread)
    decay = jnp.exp(closing)
    states = payload_ref[:, :HEAD, :].astype(f32).reshape(WIDTH, LANES)
    lane = lax.broadcasted_iota(jnp.int32, (HEAD, LANES), 1)
    ahead = [None] * HEADS
    behind = [None] * HEADS

    def at(x, i):
        return x[i * HEAD : (i + 1) * HEAD, :]

    carried = jnp.zeros((HEAD, LANES), f32)
    for i in range(HEADS):
        ahead[i] = carried
        carried = at(decay, i) * carried + at(states, i)
    carried = jnp.zeros((HEAD, LANES), f32)
    for i in range(HEADS - 1, -1, -1):
        behind[i] = carried
        carried = at(decay, i) * carried + at(states, i)
    for i in range(HEADS):
        out_ref[i * HEAD : (i + 1) * HEAD, :] = jnp.where(
            lane < LANES // 2, ahead[i], behind[i]
        ).astype(bf16)


def query_kernel(
    rounded_ref, up_forward_ref, up_backward_ref, bias_forward_ref, bias_backward_ref, out_ref
):
    queries = rounded_ref[:, 2 * WIDTH : 3 * WIDTH].astype(f32) * HEAD ** (-0.5)
    keys = rounded_ref[:, :WIDTH].astype(f32)
    parts = rates_of(
        rounded_ref[:, 3 * WIDTH :], up_forward_ref, up_backward_ref, bias_forward_ref, bias_backward_ref
    )
    decayed, inverse = [], []
    for way, mask in ((0, lambda r, c: c <= r), (1, lambda r, c: c >= r)):
        running = summed(parts, mask, way)
        product = queries * jnp.exp(running)
        out_ref[:, (way + 1) * WIDTH : (way + 2) * WIDTH] = product
        decayed.append(product.astype(bf16))
        inverse.append((keys * jnp.exp(-running)).astype(bf16))
    row, col = grid_of((4 * BLOCK, LANES))
    own_lanes = (row // BLOCK) == (col // HEAD)
    own_lanes_bf = as_bf16(own_lanes)
    srow, scol = grid_of((4 * BLOCK, BLOCK))
    lower = (srow % BLOCK) >= scol
    upper = (srow % BLOCK) <= scol
    for seq in range(2):
        span = slice(seq * BLOCK, (seq + 1) * BLOCK)
        for group in range(4):
            lanes = slice(group * LANES, (group + 1) * LANES)
            scores = 0.0
            for way, mask in ((0, lower), (1, upper)):
                one = decayed[way][span, lanes]
                stacked = jnp.concatenate([one] * 4, axis=0) * own_lanes_bf
                scores = scores + jnp.where(mask, dot_nt(stacked, inverse[way][span, lanes]), 0.0)
            spread = jnp.where(own_lanes, dot(scores.astype(bf16), rounded_ref[span, slice(WIDTH + group * LANES, WIDTH + (group + 1) * LANES)]), 0.0)
            out_ref[span, lanes] = (
                spread[:BLOCK] + spread[BLOCK : 2 * BLOCK]
                + spread[2 * BLOCK : 3 * BLOCK] + spread[3 * BLOCK :]
            )


def out_kernel(
    states_ref, parts_ref, gain_ref, own_ref, other_ref, out_ref
):
    core = lax.axis_index("dp_2")
    row, col = grid_of((LANES, LANES))
    diagonal = (row // HEAD) == (col // HEAD)
    rows = []
    for seq in range(2):
        span = slice(seq * BLOCK, (seq + 1) * BLOCK)
        pieces = []
        for group in range(4):
            lanes = slice(group * LANES, (group + 1) * LANES)
            total = parts_ref[span, lanes]
            for way in range(2):
                widen = as_bf16(row == (2 * way + seq) * HEAD + col % HEAD)
                full = dot(states_ref[lanes, :], widen)
                full = jnp.where(diagonal, full, 0.0).astype(bf16)
                start = (way + 1) * WIDTH + group * LANES
                high, low = halves(parts_ref[span, start : start + LANES])
                total = total + dot(high, full) + dot(low, full)
            pieces.append(total)
        rows.append(jnp.concatenate(pieces, axis=1))
    combined = jnp.concatenate(rows, axis=0)
    high, low = halves(combined * combined)
    ones = as_bf16(diagonal)
    mean = jnp.concatenate(
        [
            dot(high[:, g * LANES : (g + 1) * LANES], ones)
            + dot(low[:, g * LANES : (g + 1) * LANES], ones)
            for g in range(4)
        ],
        axis=1,
    ) * (1.0 / HEAD)
    attended = (combined * lax.rsqrt(mean + EPS) * gain_ref[...]).astype(bf16)
    prow, pcol = grid_of((WIDTH, WIDTH))
    source = ((pcol % 256) // 16) * 32 + (pcol // 256) * 16 + pcol % 16
    shuffled = dot(attended, as_bf16(prow == source)).astype(bf16)
    first, second = shuffled[:, :256], shuffled[:, 256:]
    mine = jnp.where(core == 0, first, second)
    theirs = jnp.where(core == 0, second, first)
    out_ref[...] = (dot(mine, in_order(own_ref)) + dot(theirs, in_order(other_ref))).astype(bf16)


VMEM = pl.BlockSpec(memory_space=pltpu.VMEM)


def call(kernel, outs, specs, cycles, *args, scratch=(), grant=16 << 20):
    many = isinstance(outs, tuple)
    return pl.pallas_call(
        kernel,
        out_shape=outs,
        in_specs=specs,
        out_specs=(VMEM,) * len(outs) if many else VMEM,
        scratch_shapes=scratch,
        cost_estimate=pl.CostEstimate(flops=cycles, bytes_accessed=1 << 20, transcendentals=0),
        compiler_params=pltpu.CompilerParams(vmem_limit_bytes=grant),
    )(*args)


def swapped(x):
    return lax.ppermute(x, "dp_2", [(0, 1), (1, 0)])


def body(
    tokens, norm_gain, w_query, w_key, w_value, w_rank_forward, w_rank_backward,
    up_forward, up_backward, bias_forward, bias_backward, out_gain, w_out,
):
    seqs, toks, width = tokens.shape
    rows = seqs * toks
    shape = jax.ShapeDtypeStruct
    hbm = pl.BlockSpec(memory_space=pltpu.HBM)
    sources = (w_key, w_value, w_query, w_rank_forward.T, w_rank_backward.T)
    send = call(
        pack_kernel, shape((16, 32, ALL), bf16), [hbm] * 5, 1 << 26, *sources,
        scratch=[pltpu.VMEM(x.shape, bf16) for x in sources] + [pltpu.SemaphoreType.DMA((5,))],
        grant=None,
    )
    own = lax.all_to_all(send, PLANE, 0, 0)
    other = swapped(own)
    mix = w_out[None]
    for axis, flip in (("dp_0", 1), ("dp_0", 3), ("dp_1", 1), ("dp_1", 3)):
        arrived = lax.ppermute(mix, axis, [(i, i ^ flip) for i in range(4)])
        mix = call(
            join_kernel, shape((2 * mix.shape[0], 16, width), bf16), [VMEM] * 2, 1 << 26,
            mix, arrived,
        )
    mix_other = swapped(mix)
    normed = call(
        norm_kernel, shape((2, rows, 512), bf16), [VMEM, VMEM], 1 << 28,
        tokens.reshape(rows, width), norm_gain.reshape(1, width),
    )
    decays = (
        up_forward, up_backward, bias_forward.reshape(1, WIDTH), bias_backward.reshape(1, WIDTH)
    )
    payload, rounded = call(
        block_kernel, (shape((HEADS, 48, LANES), bf16), shape((rows, ALL), bf16)),
        [VMEM] * 7, 1 << 30, normed, own, other, *decays,
    )
    inbound = lax.all_to_all(payload, "sp", 0, 0)
    states = call(
        scan_kernel, shape((WIDTH, LANES), bf16), [VMEM], 1 << 28,
        inbound,
    )
    returned = lax.all_to_all(states.reshape(HEADS, HEAD, LANES), "sp", 0, 0)
    parts = call(query_kernel, shape((rows, 3 * WIDTH), f32), [VMEM] * 5, 1 << 30, rounded, *decays)
    mixed = call(
        out_kernel, shape((rows, width), bf16), [VMEM] * 5, 1 << 30,
        returned.reshape(WIDTH, LANES), parts,
        jnp.tile(out_gain, HEADS).reshape(1, WIDTH), mix, mix_other,
    )
    return mixed.reshape(seqs, toks, width)


def solution(mesh):
    finer = Mesh(mesh.devices.reshape(mesh.shape["sp"], 4, 4, 2), ("sp", "dp_0", "dp_1", "dp_2"))
    rows = P(DP, None)
    in_specs = (
        P(DP, "sp", None), P(), rows, rows, rows, rows, rows, P(), P(), P(), P(), P(), rows,
    )

    return jax.shard_map(
        body, mesh=finer, in_specs=in_specs, out_specs=P(DP, "sp", None), check_vma=False
    )
```

```python
import jax
import jax.numpy as jnp
from jax import lax
from jax.experimental import pallas as pl
from jax.experimental.pallas import tpu as pltpu
from jax.sharding import Mesh
from jax.sharding import PartitionSpec as P

DP = ("dp_0", "dp_1", "dp_2")
PLANE = ("dp_0", "dp_1")
HEAD = 32
HEADS = 16
WIDTH = 512
BLOCK = 64
LANES = 128
ALL = 3 * WIDTH + LANES
EPS = 1e-06
f32 = jnp.float32
bf16 = jnp.bfloat16


def dot(a, b):
    return jnp.dot(a, b, preferred_element_type=f32)


def dot_tn(a, b):
    return lax.dot_general(a, b, (((0,), (0,)), ((), ())), preferred_element_type=f32)


def dot_nt(a, b):
    return lax.dot_general(a, b, (((1,), (1,)), ((), ())), preferred_element_type=f32)


def halves(x):
    high = x.astype(bf16)
    return high, (x - high.astype(f32)).astype(bf16)


def grid_of(shape):
    return lax.broadcasted_iota(jnp.int32, shape, 0), lax.broadcasted_iota(jnp.int32, shape, 1)


def as_bf16(mask):
    return jnp.where(mask, 1.0, 0.0).astype(bf16)


def pack_kernel(
    key_hbm, value_hbm, query_hbm, forward_hbm, backward_hbm,
    out_ref, key_ref, value_ref, query_ref, forward_ref, backward_ref, sems,
):
    sources = (key_hbm, value_hbm, query_hbm, forward_hbm, backward_hbm)
    targets = (key_ref, value_ref, query_ref, forward_ref, backward_ref)
    copies = [
        pltpu.make_async_copy(source, target, sems.at[i])
        for i, (source, target) in enumerate(zip(sources, targets))
    ]
    for copy in copies:
        copy.start()
    for copy in copies:
        copy.wait()
    row, col = grid_of((16, LANES))
    ranks = dot_tn(forward_ref[...], as_bf16(row == col)) + dot_tn(
        backward_ref[...], as_bf16(row + 16 == col)
    )
    block = jnp.concatenate(
        [key_ref[...], value_ref[...], query_ref[...], ranks.astype(bf16)], axis=1
    )
    for i in range(16):
        out_ref[i] = block


def join_kernel(first_ref, second_ref, out_ref):
    count = first_ref.shape[0]
    out_ref[:count] = first_ref[...]
    out_ref[count:] = second_ref[...]


def slot_of(index, axis):
    apart = index ^ lax.axis_index(axis)
    return apart ^ (apart >> 1)


def in_order(ref):
    pieces = []
    for y in range(4):
        for x in range(4):
            pieces.append(ref[slot_of(x, "dp_1") * 4 + slot_of(y, "dp_0")])
    return jnp.concatenate(pieces, axis=0)


def norm_kernel(tokens_ref, gain_ref, normed_ref):
    values = tokens_ref[...].astype(f32)
    scale = lax.rsqrt(jnp.mean(values * values, axis=-1, keepdims=True) + EPS)
    normed = (values * scale * gain_ref[...]).astype(bf16)
    for core in range(2):
        normed_ref[core] = jnp.concatenate(
            [normed[:, (2 * i + core) * 32 : (2 * i + core) * 32 + 32] for i in range(16)], axis=1
        )


def rates_of(ranks, up_forward_ref, up_backward_ref, bias_forward_ref, bias_backward_ref):
    gates = jnp.concatenate(
        [
            dot(ranks[:, :16], up_forward_ref[...]) + bias_forward_ref[...],
            dot(ranks[:, 16:32], up_backward_ref[...]) + bias_backward_ref[...],
        ],
        axis=1,
    )
    return halves(jax.nn.log_sigmoid(gates) * (2.0 / (BLOCK * HEADS)))


def summed(parts, mask, way):
    row, col = grid_of((LANES, LANES))
    ones = as_bf16(mask(row, col) & ((row // BLOCK) == (col // BLOCK)))
    lanes = slice(way * WIDTH, (way + 1) * WIDTH)
    return dot(ones, parts[0][:, lanes]) + dot(ones, parts[1][:, lanes])


def block_kernel(
    normed_ref, own_ref, other_ref, up_forward_ref, up_backward_ref,
    bias_forward_ref, bias_backward_ref, payload_ref, rounded_ref,
):
    core = lax.axis_index("dp_2")
    projected = dot(normed_ref[core], own_ref[...].reshape(WIDTH, ALL)) + dot(
        normed_ref[1 - core], other_ref[...].reshape(WIDTH, ALL)
    )
    rounded = projected.astype(bf16)
    rounded_ref[...] = rounded
    values = rounded[:, WIDTH : 2 * WIDTH]
    parts = rates_of(
        rounded[:, 3 * WIDTH :], up_forward_ref, up_backward_ref, bias_forward_ref, bias_backward_ref
    )
    high, low = parts
    row, col = grid_of((LANES, LANES))
    fwd, bwd = slice(0, WIDTH), slice(WIDTH, 2 * WIDTH)
    keys32 = rounded[:, :WIDTH].astype(f32)
    remain = (
        halves(keys32 * jnp.exp(summed(parts, lambda r, c: c > r, 0))),
        halves(keys32 * jnp.exp(summed(parts, lambda r, c: c < r, 1))),
    )
    hrow, hcol = grid_of((HEADS, WIDTH))
    mine = hrow == hcol // HEAD
    erow, ecol = grid_of((WIDTH, LANES))
    srow, scol = grid_of((8, 128))
    close = 0.0
    for way, span in ((0, fwd), (1, bwd)):
        pick = as_bf16(srow == scol // BLOCK)
        sums = dot(pick, high[:, span]) + dot(pick, low[:, span])
        for seq in range(2):
            line = jnp.where(mine, sums[seq : seq + 1], 0.0)
            place = as_bf16(ecol == (2 * way + seq) * HEAD + erow % HEAD)
            line_high, line_low = halves(line)
            both = jnp.concatenate([line_high, line_low], axis=0)
            close = close + dot(both, place)
    tail = lax.broadcasted_iota(jnp.int32, (HEADS, 8, LANES), 1)
    payload_ref[:, HEAD:, :] = jnp.where(
        tail == 0,
        close[:HEADS][:, None, :],
        jnp.where(tail == 1, close[HEADS:][:, None, :], 0.0),
    ).astype(bf16)
    diagonal = (row // HEAD) == (col // HEAD)
    erow, ecol = grid_of((4 * LANES, LANES))
    fold = as_bf16(((erow // LANES) * HEAD + erow % HEAD) == ecol)
    for group in range(4):
        lanes = slice(group * LANES, (group + 1) * LANES)
        parts = []
        for way in range(2):
            for seq in range(2):
                span = slice(seq * BLOCK, (seq + 1) * BLOCK)
                value = values[span, lanes]
                state = dot_tn(remain[way][0][span, lanes], value) + dot_tn(
                    remain[way][1][span, lanes], value
                )
                parts.append(jnp.where(diagonal, state, 0.0).astype(bf16))
        folded = dot(jnp.concatenate(parts, axis=1), fold).astype(bf16)
        payload_ref[4 * group : 4 * group + 4, :HEAD, :] = folded.reshape(4, HEAD, LANES)


def scan_kernel(payload_ref, out_ref):
    row, col = grid_of((LANES, LANES))
    spread = as_bf16((row // HEAD) == (col // HEAD))
    crow, ccol = grid_of((HEAD, LANES))
    mine = ccol % HEAD == crow
    lines = payload_ref[:, HEAD : HEAD + 8, :].astype(f32)
    closing = 0.0
    for part in range(2):
        line = jnp.where(mine[None], lines[:, part : part + 1, :], 0.0)
        closing = closing + dot(line.astype(bf16).reshape(WIDTH, LANES), spread)
    decay = jnp.exp(closing)
    states = payload_ref[:, :HEAD, :].astype(f32).reshape(WIDTH, LANES)
    lane = lax.broadcasted_iota(jnp.int32, (HEAD, LANES), 1)
    ahead = [None] * HEADS
    behind = [None] * HEADS

    def at(x, i):
        return x[i * HEAD : (i + 1) * HEAD, :]

    carried = jnp.zeros((HEAD, LANES), f32)
    for i in range(HEADS):
        ahead[i] = carried
        carried = at(decay, i) * carried + at(states, i)
    carried = jnp.zeros((HEAD, LANES), f32)
    for i in range(HEADS - 1, -1, -1):
        behind[i] = carried
        carried = at(decay, i) * carried + at(states, i)
    for i in range(HEADS):
        out_ref[i * HEAD : (i + 1) * HEAD, :] = jnp.where(
            lane < LANES // 2, ahead[i], behind[i]
        ).astype(bf16)


def query_kernel(
    rounded_ref, up_forward_ref, up_backward_ref, bias_forward_ref, bias_backward_ref, out_ref
):
    queries = rounded_ref[:, 2 * WIDTH : 3 * WIDTH].astype(f32) * HEAD ** (-0.5)
    keys = rounded_ref[:, :WIDTH].astype(f32)
    parts = rates_of(
        rounded_ref[:, 3 * WIDTH :], up_forward_ref, up_backward_ref, bias_forward_ref, bias_backward_ref
    )
    decayed, inverse = [], []
    for way, mask in ((0, lambda r, c: c <= r), (1, lambda r, c: c >= r)):
        running = summed(parts, mask, way)
        product = queries * jnp.exp(running)
        out_ref[:, (way + 1) * WIDTH : (way + 2) * WIDTH] = product
        decayed.append(product.astype(bf16))
        inverse.append((keys * jnp.exp(-running)).astype(bf16))
    row, col = grid_of((4 * BLOCK, LANES))
    own_lanes = (row // BLOCK) == (col // HEAD)
    own_lanes_bf = as_bf16(own_lanes)
    srow, scol = grid_of((4 * BLOCK, BLOCK))
    lower = (srow % BLOCK) >= scol
    upper = (srow % BLOCK) <= scol
    for seq in range(2):
        span = slice(seq * BLOCK, (seq + 1) * BLOCK)
        for group in range(4):
            lanes = slice(group * LANES, (group + 1) * LANES)
            scores = 0.0
            for way, mask in ((0, lower), (1, upper)):
                one = decayed[way][span, lanes]
                stacked = jnp.concatenate([one] * 4, axis=0) * own_lanes_bf
                scores = scores + jnp.where(mask, dot_nt(stacked, inverse[way][span, lanes]), 0.0)
            spread = jnp.where(own_lanes, dot(scores.astype(bf16), rounded_ref[span, slice(WIDTH + group * LANES, WIDTH + (group + 1) * LANES)]), 0.0)
            out_ref[span, lanes] = (
                spread[:BLOCK] + spread[BLOCK : 2 * BLOCK]
                + spread[2 * BLOCK : 3 * BLOCK] + spread[3 * BLOCK :]
            )


def out_kernel(
    states_ref, parts_ref, gain_ref, own_ref, other_ref, out_ref
):
    core = lax.axis_index("dp_2")
    row, col = grid_of((LANES, LANES))
    diagonal = (row // HEAD) == (col // HEAD)
    rows = []
    for seq in range(2):
        span = slice(seq * BLOCK, (seq + 1) * BLOCK)
        pieces = []
        for group in range(4):
            lanes = slice(group * LANES, (group + 1) * LANES)
            total = parts_ref[span, lanes]
            for way in range(2):
                widen = as_bf16(row == (2 * way + seq) * HEAD + col % HEAD)
                full = dot(states_ref[lanes, :], widen)
                full = jnp.where(diagonal, full, 0.0).astype(bf16)
                start = (way + 1) * WIDTH + group * LANES
                high, low = halves(parts_ref[span, start : start + LANES])
                total = total + dot(high, full) + dot(low, full)
            pieces.append(total)
        rows.append(jnp.concatenate(pieces, axis=1))
    combined = jnp.concatenate(rows, axis=0)
    high, low = halves(combined * combined)
    ones = as_bf16(diagonal)
    mean = jnp.concatenate(
        [
            dot(high[:, g * LANES : (g + 1) * LANES], ones)
            + dot(low[:, g * LANES : (g + 1) * LANES], ones)
            for g in range(4)
        ],
        axis=1,
    ) * (1.0 / HEAD)
    attended = (combined * lax.rsqrt(mean + EPS) * gain_ref[...]).astype(bf16)
    prow, pcol = grid_of((WIDTH, WIDTH))
    source = ((pcol % 256) // 16) * 32 + (pcol // 256) * 16 + pcol % 16
    shuffled = dot(attended, as_bf16(prow == source)).astype(bf16)
    first, second = shuffled[:, :256], shuffled[:, 256:]
    mine = jnp.where(core == 0, first, second)
    theirs = jnp.where(core == 0, second, first)
    out_ref[...] = (dot(mine, in_order(own_ref)) + dot(theirs, in_order(other_ref))).astype(bf16)


VMEM = pl.BlockSpec(memory_space=pltpu.VMEM)


def call(kernel, outs, specs, cycles, *args, scratch=()):
    many = isinstance(outs, tuple)
    return pl.pallas_call(
        kernel,
        out_shape=outs,
        in_specs=specs,
        out_specs=(VMEM,) * len(outs) if many else VMEM,
        scratch_shapes=scratch,
        cost_estimate=pl.CostEstimate(flops=cycles, bytes_accessed=1 << 20, transcendentals=0),
        compiler_params=pltpu.CompilerParams(vmem_limit_bytes=16 << 20),
    )(*args)


def swapped(x):
    return lax.ppermute(x, "dp_2", [(0, 1), (1, 0)])


def body(
    tokens, norm_gain, w_query, w_key, w_value, w_rank_forward, w_rank_backward,
    up_forward, up_backward, bias_forward, bias_backward, out_gain, w_out,
):
    seqs, toks, width = tokens.shape
    rows = seqs * toks
    shape = jax.ShapeDtypeStruct
    hbm = pl.BlockSpec(memory_space=pltpu.HBM)
    sources = [
        pltpu.with_memory_space_constraint(x, pltpu.HBM)
        for x in (w_key, w_value, w_query, w_rank_forward.T, w_rank_backward.T)
    ]
    send = call(
        pack_kernel, shape((16, 32, ALL), bf16), [hbm] * 5, 1 << 26, *sources,
        scratch=[pltpu.VMEM(x.shape, bf16) for x in sources] + [pltpu.SemaphoreType.DMA((5,))],
    )
    own = lax.all_to_all(send, PLANE, 0, 0)
    other = swapped(own)
    mix = w_out[None]
    for axis, flip in (("dp_0", 1), ("dp_0", 3), ("dp_1", 1), ("dp_1", 3)):
        arrived = lax.ppermute(mix, axis, [(i, i ^ flip) for i in range(4)])
        mix = call(
            join_kernel, shape((2 * mix.shape[0], 16, width), bf16), [VMEM] * 2, 1 << 26,
            mix, arrived,
        )
    mix_other = swapped(mix)
    normed = call(
        norm_kernel, shape((2, rows, 512), bf16), [VMEM, VMEM], 1 << 28,
        tokens.reshape(rows, width), norm_gain.reshape(1, width),
    )
    decays = (
        up_forward, up_backward, bias_forward.reshape(1, WIDTH), bias_backward.reshape(1, WIDTH)
    )
    payload, rounded = call(
        block_kernel, (shape((HEADS, 40, LANES), bf16), shape((rows, ALL), bf16)),
        [VMEM] * 7, 1 << 30, normed, own, other, *decays,
    )
    inbound = lax.all_to_all(payload, "sp", 0, 0)
    states = call(
        scan_kernel, shape((WIDTH, LANES), bf16), [VMEM], 1 << 28,
        inbound,
    )
    returned = lax.all_to_all(states.reshape(HEADS, HEAD, LANES), "sp", 0, 0)
    parts = call(query_kernel, shape((rows, 3 * WIDTH), f32), [VMEM] * 5, 1 << 30, rounded, *decays)
    mixed = call(
        out_kernel, shape((rows, width), bf16), [VMEM] * 5, 1 << 30,
        returned.reshape(WIDTH, LANES), parts,
        jnp.tile(out_gain, HEADS).reshape(1, WIDTH), mix, mix_other,
    )
    return mixed.reshape(seqs, toks, width)


def solution(mesh):
    finer = Mesh(mesh.devices.reshape(mesh.shape["sp"], 4, 4, 2), ("sp", "dp_0", "dp_1", "dp_2"))
    rows = P(DP, None)
    in_specs = (
        P(DP, "sp", None), P(), rows, rows, rows, rows, rows, P(), P(), P(), P(), P(), rows,
    )

    return jax.shard_map(
        body, mesh=finer, in_specs=in_specs, out_specs=P(DP, "sp", None), check_vma=False
    )
```

```python
import jax
import jax.numpy as jnp
from jax import lax
from jax.experimental import pallas as pl
from jax.experimental.pallas import tpu as pltpu
from jax.sharding import Mesh
from jax.sharding import PartitionSpec as P

DP = ("dp_0", "dp_1", "dp_2")
PLANE = ("dp_0", "dp_1")
HEAD = 32
HEADS = 16
WIDTH = 512
BLOCK = 64
LANES = 128
ALL = 3 * WIDTH + LANES
SENT = ALL + LANES
EPS = 1e-06
f32 = jnp.float32
bf16 = jnp.bfloat16


def dot(a, b):
    return jnp.dot(a, b, preferred_element_type=f32)


def dot_tn(a, b):
    return lax.dot_general(a, b, (((0,), (0,)), ((), ())), preferred_element_type=f32)


def dot_nt(a, b):
    return lax.dot_general(a, b, (((1,), (1,)), ((), ())), preferred_element_type=f32)


def halves(x):
    high = x.astype(bf16)
    return high, (x - high.astype(f32)).astype(bf16)


def grid_of(shape):
    return lax.broadcasted_iota(jnp.int32, shape, 0), lax.broadcasted_iota(jnp.int32, shape, 1)


def as_bf16(mask):
    return jnp.where(mask, 1.0, 0.0).astype(bf16)


def pack_kernel(
    key_hbm, value_hbm, query_hbm, forward_hbm, backward_hbm, mix_hbm,
    out_ref, key_ref, value_ref, query_ref, forward_ref, backward_ref, mix_ref, sems,
):
    sources = (key_hbm, value_hbm, query_hbm, forward_hbm, backward_hbm, mix_hbm)
    targets = (key_ref, value_ref, query_ref, forward_ref, backward_ref, mix_ref)
    copies = [
        pltpu.make_async_copy(source, target, sems.at[i])
        for i, (source, target) in enumerate(zip(sources, targets))
    ]
    for copy in copies:
        copy.start()
    for copy in copies:
        copy.wait()
    row, col = grid_of((16, LANES))
    ranks = dot_tn(forward_ref[...], as_bf16(row == col)) + dot_tn(
        backward_ref[...], as_bf16(row + 16 == col)
    )
    block = jnp.concatenate(
        [key_ref[...], value_ref[...], query_ref[...], ranks.astype(bf16)], axis=1
    )
    for i in range(16):
        start = (i // 4) * 2 * LANES
        out_ref[i, :, :ALL] = block
        out_ref[i, :16, ALL:] = mix_ref[:, start : start + LANES]
        out_ref[i, 16:, ALL:] = mix_ref[:, start + LANES : start + 2 * LANES]


def join_kernel(first_ref, second_ref, out_ref):
    count = first_ref.shape[0]
    out_ref[:count] = first_ref[...]
    out_ref[count:] = second_ref[...]


def slot_of(index, axis):
    apart = index ^ lax.axis_index(axis)
    return apart ^ (apart >> 1)


def norm_kernel(tokens_ref, gain_ref, normed_ref):
    values = tokens_ref[...].astype(f32)
    scale = lax.rsqrt(jnp.mean(values * values, axis=-1, keepdims=True) + EPS)
    normed = (values * scale * gain_ref[...]).astype(bf16)
    for core in range(2):
        normed_ref[core] = jnp.concatenate(
            [normed[:, (2 * i + core) * 32 : (2 * i + core) * 32 + 32] for i in range(16)], axis=1
        )


def rates_of(ranks, up_forward_ref, up_backward_ref, bias_forward_ref, bias_backward_ref):
    gates = jnp.concatenate(
        [
            dot(ranks[:, :16], up_forward_ref[...]) + bias_forward_ref[...],
            dot(ranks[:, 16:32], up_backward_ref[...]) + bias_backward_ref[...],
        ],
        axis=1,
    )
    return halves(jax.nn.log_sigmoid(gates) * (2.0 / (BLOCK * HEADS)))


def summed(parts, mask, way):
    row, col = grid_of((LANES, LANES))
    ones = as_bf16(mask(row, col) & ((row // BLOCK) == (col // BLOCK)))
    lanes = slice(way * WIDTH, (way + 1) * WIDTH)
    return dot(ones, parts[0][:, lanes]) + dot(ones, parts[1][:, lanes])


def block_kernel(
    normed_ref, own_ref, other_ref, up_forward_ref, up_backward_ref,
    bias_forward_ref, bias_backward_ref, payload_ref, rounded_ref, mix_ref,
):
    core = lax.axis_index("dp_2")
    projected = dot(normed_ref[core], own_ref[:, :, :ALL].reshape(WIDTH, ALL)) + dot(
        normed_ref[1 - core], other_ref[:, :, :ALL].reshape(WIDTH, ALL)
    )
    mix_ref[0] = own_ref[:, :, ALL:]
    rounded = projected.astype(bf16)
    rounded_ref[...] = rounded
    values = rounded[:, WIDTH : 2 * WIDTH]
    parts = rates_of(
        rounded[:, 3 * WIDTH :], up_forward_ref, up_backward_ref, bias_forward_ref, bias_backward_ref
    )
    high, low = parts
    row, col = grid_of((LANES, LANES))
    fwd, bwd = slice(0, WIDTH), slice(WIDTH, 2 * WIDTH)
    keys32 = rounded[:, :WIDTH].astype(f32)
    remain = (
        halves(keys32 * jnp.exp(summed(parts, lambda r, c: c > r, 0))),
        halves(keys32 * jnp.exp(summed(parts, lambda r, c: c < r, 1))),
    )
    hrow, hcol = grid_of((HEADS, WIDTH))
    mine = hrow == hcol // HEAD
    erow, ecol = grid_of((WIDTH, LANES))
    srow, scol = grid_of((8, 128))
    close = 0.0
    for way, span in ((0, fwd), (1, bwd)):
        pick = as_bf16(srow == scol // BLOCK)
        sums = dot(pick, high[:, span]) + dot(pick, low[:, span])
        for seq in range(2):
            line = jnp.where(mine, sums[seq : seq + 1], 0.0)
            place = as_bf16(ecol == (2 * way + seq) * HEAD + erow % HEAD)
            line_high, line_low = halves(line)
            both = jnp.concatenate([line_high, line_low], axis=0)
            close = close + dot(both, place)
    tail = lax.broadcasted_iota(jnp.int32, (HEADS, 8, LANES), 1)
    payload_ref[:, HEAD:, :] = jnp.where(
        tail == 0,
        close[:HEADS][:, None, :],
        jnp.where(tail == 1, close[HEADS:][:, None, :], 0.0),
    ).astype(bf16)
    diagonal = (row // HEAD) == (col // HEAD)
    erow, ecol = grid_of((4 * LANES, LANES))
    fold = as_bf16(((erow // LANES) * HEAD + erow % HEAD) == ecol)
    for group in range(4):
        lanes = slice(group * LANES, (group + 1) * LANES)
        parts = []
        for way in range(2):
            for seq in range(2):
                span = slice(seq * BLOCK, (seq + 1) * BLOCK)
                value = values[span, lanes]
                state = dot_tn(remain[way][0][span, lanes], value) + dot_tn(
                    remain[way][1][span, lanes], value
                )
                parts.append(jnp.where(diagonal, state, 0.0).astype(bf16))
        folded = dot(jnp.concatenate(parts, axis=1), fold).astype(bf16)
        payload_ref[4 * group : 4 * group + 4, :HEAD, :] = folded.reshape(4, HEAD, LANES)


def scan_kernel(payload_ref, out_ref):
    row, col = grid_of((LANES, LANES))
    spread = as_bf16((row // HEAD) == (col // HEAD))
    crow, ccol = grid_of((HEAD, LANES))
    mine = ccol % HEAD == crow
    lines = payload_ref[:, HEAD : HEAD + 8, :].astype(f32)
    closing = 0.0
    for part in range(2):
        line = jnp.where(mine[None], lines[:, part : part + 1, :], 0.0)
        closing = closing + dot(line.astype(bf16).reshape(WIDTH, LANES), spread)
    decay = jnp.exp(closing)
    states = payload_ref[:, :HEAD, :].astype(f32).reshape(WIDTH, LANES)
    lane = lax.broadcasted_iota(jnp.int32, (HEAD, LANES), 1)
    ahead = [None] * HEADS
    behind = [None] * HEADS

    def at(x, i):
        return x[i * HEAD : (i + 1) * HEAD, :]

    carried = jnp.zeros((HEAD, LANES), f32)
    for i in range(HEADS):
        ahead[i] = carried
        carried = at(decay, i) * carried + at(states, i)
    carried = jnp.zeros((HEAD, LANES), f32)
    for i in range(HEADS - 1, -1, -1):
        behind[i] = carried
        carried = at(decay, i) * carried + at(states, i)
    for i in range(HEADS):
        out_ref[i * HEAD : (i + 1) * HEAD, :] = jnp.where(
            lane < LANES // 2, ahead[i], behind[i]
        ).astype(bf16)


def query_kernel(
    rounded_ref, up_forward_ref, up_backward_ref, bias_forward_ref, bias_backward_ref, out_ref
):
    queries = rounded_ref[:, 2 * WIDTH : 3 * WIDTH].astype(f32) * HEAD ** (-0.5)
    keys = rounded_ref[:, :WIDTH].astype(f32)
    parts = rates_of(
        rounded_ref[:, 3 * WIDTH :], up_forward_ref, up_backward_ref, bias_forward_ref, bias_backward_ref
    )
    decayed, inverse = [], []
    for way, mask in ((0, lambda r, c: c <= r), (1, lambda r, c: c >= r)):
        running = summed(parts, mask, way)
        product = queries * jnp.exp(running)
        out_ref[:, (way + 1) * WIDTH : (way + 2) * WIDTH] = product
        decayed.append(product.astype(bf16))
        inverse.append((keys * jnp.exp(-running)).astype(bf16))
    row, col = grid_of((4 * BLOCK, LANES))
    own_lanes = (row // BLOCK) == (col // HEAD)
    own_lanes_bf = as_bf16(own_lanes)
    srow, scol = grid_of((4 * BLOCK, BLOCK))
    lower = (srow % BLOCK) >= scol
    upper = (srow % BLOCK) <= scol
    for seq in range(2):
        span = slice(seq * BLOCK, (seq + 1) * BLOCK)
        for group in range(4):
            lanes = slice(group * LANES, (group + 1) * LANES)
            scores = 0.0
            for way, mask in ((0, lower), (1, upper)):
                one = decayed[way][span, lanes]
                stacked = jnp.concatenate([one] * 4, axis=0) * own_lanes_bf
                scores = scores + jnp.where(mask, dot_nt(stacked, inverse[way][span, lanes]), 0.0)
            spread = jnp.where(own_lanes, dot(scores.astype(bf16), rounded_ref[span, slice(WIDTH + group * LANES, WIDTH + (group + 1) * LANES)]), 0.0)
            out_ref[span, lanes] = (
                spread[:BLOCK] + spread[BLOCK : 2 * BLOCK]
                + spread[2 * BLOCK : 3 * BLOCK] + spread[3 * BLOCK :]
            )


def out_kernel(
    states_ref, parts_ref, gain_ref, own_ref, other_ref, out_ref
):
    core = lax.axis_index("dp_2")
    row, col = grid_of((LANES, LANES))
    diagonal = (row // HEAD) == (col // HEAD)
    rows = []
    for seq in range(2):
        span = slice(seq * BLOCK, (seq + 1) * BLOCK)
        pieces = []
        for group in range(4):
            lanes = slice(group * LANES, (group + 1) * LANES)
            total = parts_ref[span, lanes]
            for way in range(2):
                widen = as_bf16(row == (2 * way + seq) * HEAD + col % HEAD)
                full = dot(states_ref[lanes, :], widen)
                full = jnp.where(diagonal, full, 0.0).astype(bf16)
                start = (way + 1) * WIDTH + group * LANES
                high, low = halves(parts_ref[span, start : start + LANES])
                total = total + dot(high, full) + dot(low, full)
            pieces.append(total)
        rows.append(jnp.concatenate(pieces, axis=1))
    combined = jnp.concatenate(rows, axis=0)
    high, low = halves(combined * combined)
    ones = as_bf16(diagonal)
    mean = jnp.concatenate(
        [
            dot(high[:, g * LANES : (g + 1) * LANES], ones)
            + dot(low[:, g * LANES : (g + 1) * LANES], ones)
            for g in range(4)
        ],
        axis=1,
    ) * (1.0 / HEAD)
    attended = (combined * lax.rsqrt(mean + EPS) * gain_ref[...]).astype(bf16)
    prow, pcol = grid_of((WIDTH, WIDTH))
    source = ((pcol % 256) // 16) * 32 + (pcol // 256) * 16 + pcol % 16
    shuffled = dot(attended, as_bf16(prow == source)).astype(bf16)
    first, second = shuffled[:, :256], shuffled[:, 256:]
    mine = jnp.where(core == 0, first, second)
    theirs = jnp.where(core == 0, second, first)
    for quarter in range(4):
        slot = slot_of(quarter, "dp_0")
        for half in range(2):
            rows = slice(16 * half, 16 * half + 16)
            start = (2 * quarter + half) * LANES
            out_ref[:, start : start + LANES] = (
                dot(mine, own_ref[slot, :, rows, :].reshape(256, LANES))
                + dot(theirs, other_ref[slot, :, rows, :].reshape(256, LANES))
            ).astype(bf16)


VMEM = pl.BlockSpec(memory_space=pltpu.VMEM)


def call(kernel, outs, specs, cycles, *args, scratch=()):
    many = isinstance(outs, tuple)
    return pl.pallas_call(
        kernel,
        out_shape=outs,
        in_specs=specs,
        out_specs=(VMEM,) * len(outs) if many else VMEM,
        scratch_shapes=scratch,
        cost_estimate=pl.CostEstimate(flops=cycles, bytes_accessed=1 << 20, transcendentals=0),
        compiler_params=pltpu.CompilerParams(vmem_limit_bytes=16 << 20),
    )(*args)


def swapped(x):
    return lax.ppermute(x, "dp_2", [(0, 1), (1, 0)])


def body(
    tokens, norm_gain, w_query, w_key, w_value, w_rank_forward, w_rank_backward,
    up_forward, up_backward, bias_forward, bias_backward, out_gain, w_out,
):
    seqs, toks, width = tokens.shape
    rows = seqs * toks
    shape = jax.ShapeDtypeStruct
    hbm = pl.BlockSpec(memory_space=pltpu.HBM)
    sources = [
        pltpu.with_memory_space_constraint(x, pltpu.HBM)
        for x in (w_key, w_value, w_query, w_rank_forward.T, w_rank_backward.T, w_out)
    ]
    send = call(
        pack_kernel, shape((16, 32, SENT), bf16), [hbm] * 6, 1 << 26, *sources,
        scratch=[pltpu.VMEM(x.shape, bf16) for x in sources] + [pltpu.SemaphoreType.DMA((6,))],
    )
    own = lax.all_to_all(send, PLANE, 0, 0)
    other = swapped(own)
    normed = call(
        norm_kernel, shape((2, rows, 512), bf16), [VMEM, VMEM], 1 << 28,
        tokens.reshape(rows, width), norm_gain.reshape(1, width),
    )
    decays = (
        up_forward, up_backward, bias_forward.reshape(1, WIDTH), bias_backward.reshape(1, WIDTH)
    )
    payload, rounded, mix = call(
        block_kernel,
        (
            shape((HEADS, 40, LANES), bf16), shape((rows, ALL), bf16),
            shape((1, 16, 32, LANES), bf16),
        ),
        [VMEM] * 7, 1 << 30, normed, own, other, *decays,
    )
    inbound = lax.all_to_all(payload, "sp", 0, 0)
    for flip in (1, 3):
        arrived = lax.ppermute(mix, "dp_0", [(i, i ^ flip) for i in range(4)])
        mix = call(
            join_kernel, shape((2 * mix.shape[0], 16, 32, LANES), bf16), [VMEM] * 2, 1 << 26,
            mix, arrived,
        )
    mix_other = swapped(mix)
    states = call(
        scan_kernel, shape((WIDTH, LANES), bf16), [VMEM], 1 << 28,
        inbound,
    )
    returned = lax.all_to_all(states.reshape(HEADS, HEAD, LANES), "sp", 0, 0)
    parts = call(query_kernel, shape((rows, 3 * WIDTH), f32), [VMEM] * 5, 1 << 30, rounded, *decays)
    mixed = call(
        out_kernel, shape((rows, width), bf16), [VMEM] * 5, 1 << 30,
        returned.reshape(WIDTH, LANES), parts,
        jnp.tile(out_gain, HEADS).reshape(1, WIDTH), mix, mix_other,
    )
    return mixed.reshape(seqs, toks, width)


def solution(mesh):
    finer = Mesh(mesh.devices.reshape(mesh.shape["sp"], 4, 4, 2), ("sp", "dp_0", "dp_1", "dp_2"))
    rows = P(DP, None)
    in_specs = (
        P(DP, "sp", None), P(), rows, rows, rows, rows, rows, P(), P(), P(), P(), P(), rows,
    )

    return jax.shard_map(
        body, mesh=finer, in_specs=in_specs, out_specs=P(DP, "sp", None), check_vma=False
    )
```

```python
import jax
import jax.numpy as jnp
from jax import lax
from jax.experimental import pallas as pl
from jax.experimental.pallas import tpu as pltpu
from jax.sharding import Mesh
from jax.sharding import PartitionSpec as P

DP = ("dp_0", "dp_1", "dp_2")
PLANE = ("dp_0", "dp_1")
HEAD = 32
HEADS = 16
WIDTH = 512
BLOCK = 64
LANES = 128
ALL = 2 * WIDTH + LANES
SENT = ALL + 2 * LANES
EPS = 1e-06
f32 = jnp.float32
bf16 = jnp.bfloat16


def dot(a, b):
    return jnp.dot(a, b, preferred_element_type=f32)


def dot_tn(a, b):
    return lax.dot_general(a, b, (((0,), (0,)), ((), ())), preferred_element_type=f32)


def dot_nt(a, b):
    return lax.dot_general(a, b, (((1,), (1,)), ((), ())), preferred_element_type=f32)


def halves(x):
    high = x.astype(bf16)
    return high, (x - high.astype(f32)).astype(bf16)


def grid_of(shape):
    return lax.broadcasted_iota(jnp.int32, shape, 0), lax.broadcasted_iota(jnp.int32, shape, 1)


def as_bf16(mask):
    return jnp.where(mask, 1.0, 0.0).astype(bf16)


def pack_kernel(
    key_hbm, value_hbm, query_hbm, forward_hbm, backward_hbm, mix_hbm,
    out_ref, key_ref, value_ref, query_ref, forward_ref, backward_ref, mix_ref, sems,
):
    sources = (key_hbm, value_hbm, query_hbm, forward_hbm, backward_hbm, mix_hbm)
    targets = (key_ref, value_ref, query_ref, forward_ref, backward_ref, mix_ref)
    copies = [
        pltpu.make_async_copy(source, target, sems.at[i])
        for i, (source, target) in enumerate(zip(sources, targets))
    ]
    for copy in copies:
        copy.start()
    for copy in copies:
        copy.wait()
    row, col = grid_of((16, LANES))
    ranks = dot_tn(forward_ref[...], as_bf16(row == col)) + dot_tn(
        backward_ref[...], as_bf16(row + 16 == col)
    )
    block = jnp.concatenate(
        [key_ref[...], value_ref[...], ranks.astype(bf16)], axis=1
    )
    for i in range(16):
        start = (i // 4) * LANES
        out_ref[i, :, :ALL] = block
        out_ref[i, :, ALL : ALL + LANES] = query_ref[:, start : start + LANES]
        out_ref[i, :16, ALL + LANES :] = mix_ref[:, 2 * start : 2 * start + LANES]
        out_ref[i, 16:, ALL + LANES :] = mix_ref[:, 2 * start + LANES : 2 * start + 2 * LANES]


def join_kernel(first_ref, second_ref, out_ref):
    count = first_ref.shape[0]
    out_ref[:count] = first_ref[...]
    out_ref[count:] = second_ref[...]


def slot_of(index, axis):
    apart = index ^ lax.axis_index(axis)
    return apart ^ (apart >> 1)


def norm_kernel(tokens_ref, gain_ref, normed_ref):
    values = tokens_ref[...].astype(f32)
    scale = lax.rsqrt(jnp.mean(values * values, axis=-1, keepdims=True) + EPS)
    normed = (values * scale * gain_ref[...]).astype(bf16)
    for core in range(2):
        normed_ref[core] = jnp.concatenate(
            [normed[:, (2 * i + core) * 32 : (2 * i + core) * 32 + 32] for i in range(16)], axis=1
        )


def rates_of(ranks, up_forward_ref, up_backward_ref, bias_forward_ref, bias_backward_ref):
    gates = jnp.concatenate(
        [
            dot(ranks[:, :16], up_forward_ref[...]) + bias_forward_ref[...],
            dot(ranks[:, 16:32], up_backward_ref[...]) + bias_backward_ref[...],
        ],
        axis=1,
    )
    return halves(jax.nn.log_sigmoid(gates) * (2.0 / (BLOCK * HEADS)))


def summed(parts, mask, way):
    row, col = grid_of((LANES, LANES))
    ones = as_bf16(mask(row, col) & ((row // BLOCK) == (col // BLOCK)))
    lanes = slice(way * WIDTH, (way + 1) * WIDTH)
    return dot(ones, parts[0][:, lanes]) + dot(ones, parts[1][:, lanes])


def block_kernel(
    normed_ref, own_ref, other_ref, up_forward_ref, up_backward_ref,
    bias_forward_ref, bias_backward_ref, payload_ref, rounded_ref, mix_ref,
):
    core = lax.axis_index("dp_2")
    projected = dot(normed_ref[core], own_ref[:, :, :ALL].reshape(WIDTH, ALL)) + dot(
        normed_ref[1 - core], other_ref[:, :, :ALL].reshape(WIDTH, ALL)
    )
    mix_ref[0] = own_ref[:, :, ALL:]
    rounded = projected.astype(bf16)
    rounded_ref[...] = rounded
    values = rounded[:, WIDTH : 2 * WIDTH]
    parts = rates_of(
        rounded[:, 2 * WIDTH :], up_forward_ref, up_backward_ref, bias_forward_ref, bias_backward_ref
    )
    high, low = parts
    row, col = grid_of((LANES, LANES))
    fwd, bwd = slice(0, WIDTH), slice(WIDTH, 2 * WIDTH)
    keys32 = rounded[:, :WIDTH].astype(f32)
    remain = (
        halves(keys32 * jnp.exp(summed(parts, lambda r, c: c > r, 0))),
        halves(keys32 * jnp.exp(summed(parts, lambda r, c: c < r, 1))),
    )
    hrow, hcol = grid_of((HEADS, WIDTH))
    mine = hrow == hcol // HEAD
    erow, ecol = grid_of((WIDTH, LANES))
    srow, scol = grid_of((8, 128))
    close = 0.0
    for way, span in ((0, fwd), (1, bwd)):
        pick = as_bf16(srow == scol // BLOCK)
        sums = dot(pick, high[:, span]) + dot(pick, low[:, span])
        for seq in range(2):
            line = jnp.where(mine, sums[seq : seq + 1], 0.0)
            place = as_bf16(ecol == (2 * way + seq) * HEAD + erow % HEAD)
            line_high, line_low = halves(line)
            both = jnp.concatenate([line_high, line_low], axis=0)
            close = close + dot(both, place)
    tail = lax.broadcasted_iota(jnp.int32, (HEADS, 8, LANES), 1)
    payload_ref[:, HEAD:, :] = jnp.where(
        tail == 0,
        close[:HEADS][:, None, :],
        jnp.where(tail == 1, close[HEADS:][:, None, :], 0.0),
    ).astype(bf16)
    diagonal = (row // HEAD) == (col // HEAD)
    erow, ecol = grid_of((4 * LANES, LANES))
    fold = as_bf16(((erow // LANES) * HEAD + erow % HEAD) == ecol)
    for group in range(4):
        lanes = slice(group * LANES, (group + 1) * LANES)
        parts = []
        for way in range(2):
            for seq in range(2):
                span = slice(seq * BLOCK, (seq + 1) * BLOCK)
                value = values[span, lanes]
                state = dot_tn(remain[way][0][span, lanes], value) + dot_tn(
                    remain[way][1][span, lanes], value
                )
                parts.append(jnp.where(diagonal, state, 0.0).astype(bf16))
        folded = dot(jnp.concatenate(parts, axis=1), fold).astype(bf16)
        payload_ref[4 * group : 4 * group + 4, :HEAD, :] = folded.reshape(4, HEAD, LANES)


def scan_kernel(payload_ref, out_ref):
    row, col = grid_of((LANES, LANES))
    spread = as_bf16((row // HEAD) == (col // HEAD))
    crow, ccol = grid_of((HEAD, LANES))
    mine = ccol % HEAD == crow
    lines = payload_ref[:, HEAD : HEAD + 8, :].astype(f32)
    closing = 0.0
    for part in range(2):
        line = jnp.where(mine[None], lines[:, part : part + 1, :], 0.0)
        closing = closing + dot(line.astype(bf16).reshape(WIDTH, LANES), spread)
    decay = jnp.exp(closing)
    states = payload_ref[:, :HEAD, :].astype(f32).reshape(WIDTH, LANES)
    lane = lax.broadcasted_iota(jnp.int32, (HEAD, LANES), 1)
    ahead = [None] * HEADS
    behind = [None] * HEADS

    def at(x, i):
        return x[i * HEAD : (i + 1) * HEAD, :]

    carried = jnp.zeros((HEAD, LANES), f32)
    for i in range(HEADS):
        ahead[i] = carried
        carried = at(decay, i) * carried + at(states, i)
    carried = jnp.zeros((HEAD, LANES), f32)
    for i in range(HEADS - 1, -1, -1):
        behind[i] = carried
        carried = at(decay, i) * carried + at(states, i)
    for i in range(HEADS):
        out_ref[i * HEAD : (i + 1) * HEAD, :] = jnp.where(
            lane < LANES // 2, ahead[i], behind[i]
        ).astype(bf16)


def query_kernel(
    normed_ref, own_ref, other_ref, rounded_ref, up_forward_ref, up_backward_ref,
    bias_forward_ref, bias_backward_ref, out_ref, mix_ref,
):
    core = lax.axis_index("dp_2")

    def weights(ref):
        return jnp.concatenate(
            [
                ref[slot_of(quarter, "dp_0"), :, :, :LANES].reshape(WIDTH, LANES)
                for quarter in range(4)
            ],
            axis=1,
        )

    projected = dot(normed_ref[core], weights(own_ref)) + dot(
        normed_ref[1 - core], weights(other_ref)
    )
    queries = projected.astype(bf16).astype(f32) * HEAD ** (-0.5)
    for quarter in range(4):
        slot = slot_of(quarter, "dp_0")
        for half in range(2):
            rows = slice(16 * half, 16 * half + 16)
            mix_ref[2 * quarter + half, :, core] = own_ref[slot, :, rows, LANES:]
            mix_ref[2 * quarter + half, :, 1 - core] = other_ref[slot, :, rows, LANES:]
    keys = rounded_ref[:, :WIDTH].astype(f32)
    parts = rates_of(
        rounded_ref[:, 2 * WIDTH :], up_forward_ref, up_backward_ref, bias_forward_ref, bias_backward_ref
    )
    decayed, inverse = [], []
    for way, mask in ((0, lambda r, c: c <= r), (1, lambda r, c: c >= r)):
        running = summed(parts, mask, way)
        product = queries * jnp.exp(running)
        out_ref[:, (way + 1) * WIDTH : (way + 2) * WIDTH] = product
        decayed.append(product.astype(bf16))
        inverse.append((keys * jnp.exp(-running)).astype(bf16))
    row, col = grid_of((4 * BLOCK, LANES))
    own_lanes = (row // BLOCK) == (col // HEAD)
    own_lanes_bf = as_bf16(own_lanes)
    srow, scol = grid_of((4 * BLOCK, BLOCK))
    lower = (srow % BLOCK) >= scol
    upper = (srow % BLOCK) <= scol
    for seq in range(2):
        span = slice(seq * BLOCK, (seq + 1) * BLOCK)
        for group in range(4):
            lanes = slice(group * LANES, (group + 1) * LANES)
            scores = 0.0
            for way, mask in ((0, lower), (1, upper)):
                one = decayed[way][span, lanes]
                stacked = jnp.concatenate([one] * 4, axis=0) * own_lanes_bf
                scores = scores + jnp.where(mask, dot_nt(stacked, inverse[way][span, lanes]), 0.0)
            spread = jnp.where(own_lanes, dot(scores.astype(bf16), rounded_ref[span, slice(WIDTH + group * LANES, WIDTH + (group + 1) * LANES)]), 0.0)
            out_ref[span, lanes] = (
                spread[:BLOCK] + spread[BLOCK : 2 * BLOCK]
                + spread[2 * BLOCK : 3 * BLOCK] + spread[3 * BLOCK :]
            )


def out_kernel(
    states_ref, parts_ref, gain_ref, mix_ref, out_ref
):
    row, col = grid_of((LANES, LANES))
    diagonal = (row // HEAD) == (col // HEAD)
    rows = []
    for seq in range(2):
        span = slice(seq * BLOCK, (seq + 1) * BLOCK)
        pieces = []
        for group in range(4):
            lanes = slice(group * LANES, (group + 1) * LANES)
            total = parts_ref[span, lanes]
            for way in range(2):
                widen = as_bf16(row == (2 * way + seq) * HEAD + col % HEAD)
                full = dot(states_ref[lanes, :], widen)
                full = jnp.where(diagonal, full, 0.0).astype(bf16)
                start = (way + 1) * WIDTH + group * LANES
                high, low = halves(parts_ref[span, start : start + LANES])
                total = total + dot(high, full) + dot(low, full)
            pieces.append(total)
        rows.append(jnp.concatenate(pieces, axis=1))
    combined = jnp.concatenate(rows, axis=0)
    high, low = halves(combined * combined)
    ones = as_bf16(diagonal)
    mean = jnp.concatenate(
        [
            dot(high[:, g * LANES : (g + 1) * LANES], ones)
            + dot(low[:, g * LANES : (g + 1) * LANES], ones)
            for g in range(4)
        ],
        axis=1,
    ) * (1.0 / HEAD)
    attended = (combined * lax.rsqrt(mean + EPS) * gain_ref[...]).astype(bf16)
    for part in range(4):
        weights = jnp.concatenate(
            [mix_ref[2 * part + half].reshape(WIDTH, LANES) for half in range(2)], axis=1
        )
        out_ref[:, part * 2 * LANES : (part + 1) * 2 * LANES] = dot(attended, weights).astype(bf16)


VMEM = pl.BlockSpec(memory_space=pltpu.VMEM)


def call(kernel, outs, specs, cycles, *args, scratch=()):
    many = isinstance(outs, tuple)
    return pl.pallas_call(
        kernel,
        out_shape=outs,
        in_specs=specs,
        out_specs=(VMEM,) * len(outs) if many else VMEM,
        scratch_shapes=scratch,
        cost_estimate=pl.CostEstimate(flops=cycles, bytes_accessed=1 << 20, transcendentals=0),
        compiler_params=pltpu.CompilerParams(vmem_limit_bytes=16 << 20),
    )(*args)


def swapped(x):
    return lax.ppermute(x, "dp_2", [(0, 1), (1, 0)])


def body(
    tokens, norm_gain, w_query, w_key, w_value, w_rank_forward, w_rank_backward,
    up_forward, up_backward, bias_forward, bias_backward, out_gain, w_out,
):
    seqs, toks, width = tokens.shape
    rows = seqs * toks
    shape = jax.ShapeDtypeStruct
    hbm = pl.BlockSpec(memory_space=pltpu.HBM)
    sources = [
        pltpu.with_memory_space_constraint(x, pltpu.HBM)
        for x in (w_key, w_value, w_query, w_rank_forward.T, w_rank_backward.T, w_out)
    ]
    send = call(
        pack_kernel, shape((16, 32, SENT), bf16), [hbm] * 6, 1 << 26, *sources,
        scratch=[pltpu.VMEM(x.shape, bf16) for x in sources] + [pltpu.SemaphoreType.DMA((6,))],
    )
    own = lax.all_to_all(send, PLANE, 0, 0)
    other = swapped(own)
    normed = call(
        norm_kernel, shape((2, rows, 512), bf16), [VMEM, VMEM], 1 << 28,
        tokens.reshape(rows, width), norm_gain.reshape(1, width),
    )
    decays = (
        up_forward, up_backward, bias_forward.reshape(1, WIDTH), bias_backward.reshape(1, WIDTH)
    )
    payload, rounded, mix = call(
        block_kernel,
        (
            shape((HEADS, 40, LANES), bf16), shape((rows, ALL), bf16),
            shape((1, 16, 32, 2 * LANES), bf16),
        ),
        [VMEM] * 7, 1 << 30, normed, own, other, *decays,
    )
    inbound = lax.all_to_all(payload, "sp", 0, 0)
    for flip in (1, 3):
        arrived = lax.ppermute(mix, "dp_0", [(i, i ^ flip) for i in range(4)])
        mix = call(
            join_kernel, shape((2 * mix.shape[0], 16, 32, 2 * LANES), bf16), [VMEM] * 2, 1 << 26,
            mix, arrived,
        )
    mix_other = swapped(mix)
    states = call(
        scan_kernel, shape((WIDTH, LANES), bf16), [VMEM], 1 << 28,
        inbound,
    )
    returned = lax.all_to_all(states.reshape(HEADS, HEAD, LANES), "sp", 0, 0)
    parts, mix_all = call(
        query_kernel,
        (shape((rows, 3 * WIDTH), f32), shape((8, 16, 2, 16, LANES), bf16)),
        [VMEM] * 8, 1 << 30, normed, mix, mix_other, rounded, *decays,
    )
    mixed = call(
        out_kernel, shape((rows, width), bf16), [VMEM] * 4, 1 << 30,
        returned.reshape(WIDTH, LANES), parts,
        jnp.tile(out_gain, HEADS).reshape(1, WIDTH), mix_all,
    )
    return mixed.reshape(seqs, toks, width)


def solution(mesh):
    finer = Mesh(mesh.devices.reshape(mesh.shape["sp"], 4, 4, 2), ("sp", "dp_0", "dp_1", "dp_2"))
    rows = P(DP, None)
    in_specs = (
        P(DP, "sp", None), P(), rows, rows, rows, rows, rows, P(), P(), P(), P(), P(), rows,
    )

    return jax.shard_map(
        body, mesh=finer, in_specs=in_specs, out_specs=P(DP, "sp", None), check_vma=False
    )
```

```python
import jax
import jax.numpy as jnp
from jax import lax
from jax.experimental import pallas as pl
from jax.experimental.pallas import tpu as pltpu
from jax.sharding import Mesh
from jax.sharding import PartitionSpec as P

DP = ("dp_0", "dp_1", "dp_2")
PLANE = ("dp_0", "dp_1")
HEAD = 32
HEADS = 16
WIDTH = 512
BLOCK = 64
LANES = 128
ALL = 2 * WIDTH + LANES
COLUMNS = 8 * 32
SENT = COLUMNS + 32 + 32 + 8
EPS = 1e-06
f32 = jnp.float32
bf16 = jnp.bfloat16


def dot(a, b):
    return jnp.dot(a, b, preferred_element_type=f32)


def dot_tn(a, b):
    return lax.dot_general(a, b, (((0,), (0,)), ((), ())), preferred_element_type=f32)


def dot_nt(a, b):
    return lax.dot_general(a, b, (((1,), (1,)), ((), ())), preferred_element_type=f32)


def halves(x):
    high = x.astype(bf16)
    return high, (x - high.astype(f32)).astype(bf16)


def grid_of(shape):
    return lax.broadcasted_iota(jnp.int32, shape, 0), lax.broadcasted_iota(jnp.int32, shape, 1)


def as_bf16(mask):
    return jnp.where(mask, 1.0, 0.0).astype(bf16)


def pack_kernel(
    key_hbm, value_hbm, query_hbm, forward_hbm, backward_hbm, mix_hbm,
    out_ref, key_ref, value_ref, query_ref, forward_ref, backward_ref, mix_ref, sems,
):
    sources = (key_hbm, value_hbm, query_hbm, forward_hbm, backward_hbm, mix_hbm)
    targets = (key_ref, value_ref, query_ref, forward_ref, backward_ref, mix_ref)
    copies = [
        pltpu.make_async_copy(source, target, sems.at[i])
        for i, (source, target) in enumerate(zip(sources, targets))
    ]
    for copy in copies:
        copy.start()
    for copy in copies:
        copy.wait()
    row, col = grid_of((16, LANES))
    ranks = dot_tn(forward_ref[...], as_bf16(row == col)) + dot_tn(
        backward_ref[...], as_bf16(row + 16 == col)
    )
    packed = jnp.concatenate([ranks[8 * i : 8 * i + 8, :32] for i in range(4)], axis=1)
    for i in range(16):
        for group in range(4):
            lanes = slice(group * LANES, (group + 1) * LANES)
            out_ref[i, group * 32 : (group + 1) * 32] = key_ref[:, lanes]
            out_ref[i, (4 + group) * 32 : (5 + group) * 32] = value_ref[:, lanes]
        start = (i // 4) * LANES
        out_ref[i, COLUMNS : COLUMNS + 32] = query_ref[:, start : start + LANES]
        out_ref[i, COLUMNS + 32 : COLUMNS + 48] = mix_ref[:, 2 * start : 2 * start + LANES]
        out_ref[i, COLUMNS + 48 : COLUMNS + 64] = mix_ref[:, 2 * start + LANES : 2 * start + 2 * LANES]
        out_ref[i, COLUMNS + 64 :] = packed.astype(bf16)


def join_kernel(first_ref, second_ref, out_ref):
    count = first_ref.shape[0]
    out_ref[:count] = first_ref[...]
    out_ref[count:] = second_ref[...]


def slot_of(index, axis):
    apart = index ^ lax.axis_index(axis)
    return apart ^ (apart >> 1)


def normed_halves(tokens_ref, gain_ref):
    values = tokens_ref[...].astype(f32)
    scale = lax.rsqrt(jnp.mean(values * values, axis=-1, keepdims=True) + EPS)
    normed = (values * scale * gain_ref[...]).astype(bf16)
    return [
        jnp.concatenate(
            [normed[:, (2 * i + core) * 32 : (2 * i + core) * 32 + 32] for i in range(16)], axis=1
        )
        for core in range(2)
    ]


def norm_kernel(tokens_ref, gain_ref, normed_ref):
    for core, half in enumerate(normed_halves(tokens_ref, gain_ref)):
        normed_ref[core] = half


def rates_of(ranks, up_forward_ref, up_backward_ref, bias_forward_ref, bias_backward_ref):
    gates = jnp.concatenate(
        [
            dot(ranks[:, :16], up_forward_ref[...]) + bias_forward_ref[...],
            dot(ranks[:, 16:32], up_backward_ref[...]) + bias_backward_ref[...],
        ],
        axis=1,
    )
    return halves(jax.nn.log_sigmoid(gates) * (2.0 / (BLOCK * HEADS)))


def summed(parts, mask, way):
    row, col = grid_of((LANES, LANES))
    ones = as_bf16(mask(row, col) & ((row // BLOCK) == (col // BLOCK)))
    lanes = slice(way * WIDTH, (way + 1) * WIDTH)
    return dot(ones, parts[0][:, lanes]) + dot(ones, parts[1][:, lanes])


def block_kernel(
    normed_ref, own_ref, other_ref, up_forward_ref, up_backward_ref,
    bias_forward_ref, bias_backward_ref, payload_ref, rounded_ref, mix_ref,
):
    core = lax.axis_index("dp_2")
    mix_ref[0] = own_ref[:, COLUMNS : COLUMNS + 64, :]

    def columns(ref, first):
        return jnp.concatenate(
            [ref[:, g * 32 : (g + 1) * 32, :].reshape(WIDTH, LANES) for g in (first, first + 1)], axis=1
        )

    def rank_columns(ref):
        packed = ref[:, COLUMNS + 64 :, :].astype(f32)
        rows = jnp.stack([packed[:, :, 32 * i : 32 * i + 32] for i in range(4)], axis=1)
        return rows.reshape(WIDTH, 32).astype(bf16)

    mine, theirs = normed_ref[core], normed_ref[1 - core]
    pieces = [
        dot(mine, columns(own_ref, first)) + dot(theirs, columns(other_ref, first))
        for first in (0, 2, 4, 6)
    ]
    pieces.append(dot(mine, rank_columns(own_ref)) + dot(theirs, rank_columns(other_ref)))
    pieces.append(jnp.zeros((2 * BLOCK, LANES - 32), f32))
    rounded = jnp.concatenate(pieces, axis=1).astype(bf16)
    rounded_ref[...] = rounded
    values = rounded[:, WIDTH : 2 * WIDTH]
    parts = rates_of(
        rounded[:, 2 * WIDTH :], up_forward_ref, up_backward_ref, bias_forward_ref, bias_backward_ref
    )
    high, low = parts
    row, col = grid_of((LANES, LANES))
    fwd, bwd = slice(0, WIDTH), slice(WIDTH, 2 * WIDTH)
    keys32 = rounded[:, :WIDTH].astype(f32)
    remain = (
        halves(keys32 * jnp.exp(summed(parts, lambda r, c: c > r, 0))),
        halves(keys32 * jnp.exp(summed(parts, lambda r, c: c < r, 1))),
    )
    hrow, hcol = grid_of((HEADS, WIDTH))
    mine = hrow == hcol // HEAD
    erow, ecol = grid_of((WIDTH, LANES))
    srow, scol = grid_of((8, 128))
    close = 0.0
    for way, span in ((0, fwd), (1, bwd)):
        pick = as_bf16(srow == scol // BLOCK)
        sums = dot(pick, high[:, span]) + dot(pick, low[:, span])
        for seq in range(2):
            line = jnp.where(mine, sums[seq : seq + 1], 0.0)
            place = as_bf16(ecol == (2 * way + seq) * HEAD + erow % HEAD)
            line_high, line_low = halves(line)
            both = jnp.concatenate([line_high, line_low], axis=0)
            close = close + dot(both, place)
    tail = lax.broadcasted_iota(jnp.int32, (HEADS, 8, LANES), 1)
    payload_ref[:, HEAD:, :] = jnp.where(
        tail == 0,
        close[:HEADS][:, None, :],
        jnp.where(tail == 1, close[HEADS:][:, None, :], 0.0),
    ).astype(bf16)
    diagonal = (row // HEAD) == (col // HEAD)
    erow, ecol = grid_of((4 * LANES, LANES))
    fold = as_bf16(((erow // LANES) * HEAD + erow % HEAD) == ecol)
    for group in range(4):
        lanes = slice(group * LANES, (group + 1) * LANES)
        parts = []
        for way in range(2):
            for seq in range(2):
                span = slice(seq * BLOCK, (seq + 1) * BLOCK)
                value = values[span, lanes]
                both = jnp.concatenate([half[span, lanes] for half in remain[way]], axis=0)
                state = dot_tn(both, jnp.concatenate([value, value], axis=0))
                parts.append(jnp.where(diagonal, state, 0.0).astype(bf16))
        folded = dot(jnp.concatenate(parts, axis=1), fold).astype(bf16)
        payload_ref[4 * group : 4 * group + 4, :HEAD, :] = folded.reshape(4, HEAD, LANES)


def scan_kernel(payload_ref, out_ref):
    row, col = grid_of((LANES, LANES))
    spread = as_bf16((row // HEAD) == (col // HEAD))
    crow, ccol = grid_of((HEAD, LANES))
    mine = ccol % HEAD == crow
    lines = payload_ref[:, HEAD : HEAD + 8, :].astype(f32)
    closing = 0.0
    for part in range(2):
        line = jnp.where(mine[None], lines[:, part : part + 1, :], 0.0)
        closing = closing + dot(line.astype(bf16).reshape(WIDTH, LANES), spread)
    decay = jnp.exp(closing)
    states = payload_ref[:, :HEAD, :].astype(f32).reshape(WIDTH, LANES)
    lane = lax.broadcasted_iota(jnp.int32, (HEAD, LANES), 1)
    ahead = [None] * HEADS
    behind = [None] * HEADS

    def at(x, i):
        return x[i * HEAD : (i + 1) * HEAD, :]

    carried = jnp.zeros((HEAD, LANES), f32)
    for i in range(HEADS):
        ahead[i] = carried
        carried = at(decay, i) * carried + at(states, i)
    carried = jnp.zeros((HEAD, LANES), f32)
    for i in range(HEADS - 1, -1, -1):
        behind[i] = carried
        carried = at(decay, i) * carried + at(states, i)
    for i in range(HEADS):
        out_ref[i * HEAD : (i + 1) * HEAD, :] = jnp.where(
            lane < LANES // 2, ahead[i], behind[i]
        ).astype(bf16)


def query_kernel(
    tokens_ref, gain_ref, own_ref, other_ref, rounded_ref, up_forward_ref, up_backward_ref,
    bias_forward_ref, bias_backward_ref, out_ref,
):
    core = lax.axis_index("dp_2")

    def weights(ref):
        return jnp.concatenate(
            [
                ref[slot_of(quarter, "dp_0"), :, :32, :].reshape(WIDTH, LANES)
                for quarter in range(4)
            ],
            axis=1,
        )

    first, second = normed_halves(tokens_ref, gain_ref)
    projected = dot(jnp.where(core == 0, first, second), weights(own_ref)) + dot(
        jnp.where(core == 0, second, first), weights(other_ref)
    )
    queries = projected.astype(bf16).astype(f32) * HEAD ** (-0.5)
    keys = rounded_ref[:, :WIDTH].astype(f32)
    parts = rates_of(
        rounded_ref[:, 2 * WIDTH :], up_forward_ref, up_backward_ref, bias_forward_ref, bias_backward_ref
    )
    decayed, inverse = [], []
    for way, mask in ((0, lambda r, c: c <= r), (1, lambda r, c: c >= r)):
        running = summed(parts, mask, way)
        product = queries * jnp.exp(running)
        out_ref[:, (way + 1) * WIDTH : (way + 2) * WIDTH] = product
        decayed.append(product.astype(bf16))
        inverse.append((keys * jnp.exp(-running)).astype(bf16))
    row, col = grid_of((WIDTH, WIDTH))
    natural = ((col % 256) // 16) * HEAD + (col // 256) * 16 + col % 16
    values = dot(rounded_ref[:, WIDTH : 2 * WIDTH], as_bf16(row == natural)).astype(bf16)
    row, col = grid_of((WIDTH, 256))
    own_lanes = as_bf16((row // BLOCK) == (col // HEAD))
    srow, scol = grid_of((WIDTH, BLOCK))
    lower = (srow % BLOCK) >= scol
    upper = (srow % BLOCK) <= scol
    vrow, vcol = grid_of((WIDTH, LANES))
    own_values = (vrow // BLOCK) == (vcol // 16)
    for seq in range(2):
        span = slice(seq * BLOCK, (seq + 1) * BLOCK)
        for group in range(2):
            wide = slice(group * 256, (group + 1) * 256)
            scores = 0.0
            for way, mask in ((0, lower), (1, upper)):
                stacked = jnp.concatenate([decayed[way][span, wide]] * 8, axis=0) * own_lanes
                scores = scores + jnp.where(mask, dot_nt(stacked, inverse[way][span, wide]), 0.0)
            scores = scores.astype(bf16)
            for half in range(2):
                start = half * 256 + group * LANES
                spread = dot(scores, values[span, start : start + LANES])
                spread = jnp.where(own_values, spread, 0.0)
                total = spread[:BLOCK]
                for head in range(1, 8):
                    total = total + spread[head * BLOCK : (head + 1) * BLOCK]
                out_ref[span, start : start + LANES] = total


def out_kernel(states_ref, parts_ref, gain_ref, own_ref, other_ref, out_ref):
    core = lax.axis_index("dp_2")
    row, col = grid_of((LANES, 8 * LANES))
    source = (col // 256) * HEAD + ((col // LANES) % 2) * 16 + col % 16
    widen = as_bf16(row == source)
    row, col = grid_of((256, 8 * LANES))
    diagonal = (row // HEAD) == ((col % LANES) // 16)
    full = [
        jnp.where(diagonal, dot(states_ref[g * 256 : (g + 1) * 256, :], widen), 0.0).astype(bf16)
        for g in range(2)
    ]
    totals = [[], []]
    for seq in range(2):
        span = slice(seq * BLOCK, (seq + 1) * BLOCK)
        sides = [[], []]
        for group in range(2):
            queries = jnp.concatenate(
                [
                    parts_ref[span, (way + 1) * WIDTH + group * 256 : (way + 1) * WIDTH + group * 256 + 256]
                    for way in range(2)
                ],
                axis=1,
            )
            right = jnp.concatenate(
                [full[group][:, (2 * way + seq) * 256 : (2 * way + seq + 1) * 256] for way in range(2)],
                axis=0,
            )
            across = dot(jnp.concatenate(halves(queries), axis=0), right)
            across = across[:BLOCK] + across[BLOCK:]
            for half in range(2):
                start = half * 256 + group * LANES
                sides[half].append(
                    parts_ref[span, start : start + LANES] + across[:, half * LANES : (half + 1) * LANES]
                )
        for half in range(2):
            totals[half].append(jnp.concatenate(sides[half], axis=1))
    combined = [jnp.concatenate(total, axis=0) for total in totals]
    high, low = halves(combined[0] * combined[0] + combined[1] * combined[1])
    row, col = grid_of((256, 256))
    ones = as_bf16((row // 16) == (col // 16))
    scale = lax.rsqrt((dot(high, ones) + dot(low, ones)) * (1.0 / HEAD) + EPS)
    attended = [
        (combined[half] * scale * gain_ref[half : half + 1, :]).astype(bf16) for half in range(2)
    ]
    mine = jnp.where(core == 0, attended[0], attended[1])
    theirs = jnp.where(core == 0, attended[1], attended[0])
    for quarter in range(4):
        slot = slot_of(quarter, "dp_0")

        def weights(ref):
            return jnp.concatenate(
                [ref[slot, :, rows : rows + 16, :].reshape(256, LANES) for rows in (32, 48)], axis=1
            )

        out_ref[:, quarter * 256 : (quarter + 1) * 256] = (
            dot(mine, weights(own_ref)) + dot(theirs, weights(other_ref))
        ).astype(bf16)


VMEM = pl.BlockSpec(memory_space=pltpu.VMEM)


def call(kernel, outs, specs, cycles, *args, scratch=()):
    many = isinstance(outs, tuple)
    return pl.pallas_call(
        kernel,
        out_shape=outs,
        in_specs=specs,
        out_specs=(VMEM,) * len(outs) if many else VMEM,
        scratch_shapes=scratch,
        cost_estimate=pl.CostEstimate(flops=cycles, bytes_accessed=1 << 20, transcendentals=0),
        compiler_params=pltpu.CompilerParams(vmem_limit_bytes=16 << 20),
    )(*args)


def in_hbm(x):
    return pltpu.with_memory_space_constraint(x, pltpu.HBM)


def swapped(x):
    return lax.ppermute(x, "dp_2", [(0, 1), (1, 0)])


def body(
    tokens, norm_gain, w_query, w_key, w_value, w_rank_forward, w_rank_backward,
    up_forward, up_backward, bias_forward, bias_backward, out_gain, w_out,
):
    seqs, toks, width = tokens.shape
    rows = seqs * toks
    shape = jax.ShapeDtypeStruct
    tokens_flat, gain_flat = tokens.reshape(rows, width), norm_gain.reshape(1, width)
    hbm = pl.BlockSpec(memory_space=pltpu.HBM)
    sources = [
        in_hbm(x)
        for x in (w_key, w_value, w_query, w_rank_forward.T, w_rank_backward.T, w_out)
    ]
    send = call(
        pack_kernel, shape((16, SENT, LANES), bf16), [hbm] * 6, 1 << 26, *sources,
        scratch=[pltpu.VMEM(x.shape, bf16) for x in sources] + [pltpu.SemaphoreType.DMA((6,))],
    )
    own = lax.all_to_all(send, PLANE, 0, 0)
    other = swapped(own)
    normed = call(
        norm_kernel, shape((2, rows, 512), bf16), [VMEM, VMEM], 1 << 28,
        tokens_flat, gain_flat,
    )
    decays = (
        up_forward, up_backward, bias_forward.reshape(1, WIDTH), bias_backward.reshape(1, WIDTH)
    )
    payload, rounded, mix = call(
        block_kernel,
        (
            shape((HEADS, 40, LANES), bf16), pltpu.HBM((rows, ALL), bf16),
            shape((1, 16, 64, LANES), bf16),
        ),
        [VMEM] * 7, 1 << 30, normed, own, other, *decays,
    )
    inbound = lax.all_to_all(payload, "sp", 0, 0)
    for flip in (1, 3):
        arrived = lax.ppermute(mix, "dp_0", [(i, i ^ flip) for i in range(4)])
        mix = call(
            join_kernel, shape((2 * mix.shape[0], 16, 64, LANES), bf16), [VMEM] * 2, 1 << 26,
            mix, arrived,
        )
    mix_other = swapped(mix)
    states = call(
        scan_kernel, shape((WIDTH, LANES), bf16), [VMEM], 1 << 28,
        inbound,
    )
    returned = lax.all_to_all(states.reshape(HEADS, HEAD, LANES), "sp", 0, 0)
    parts = call(
        query_kernel, pltpu.HBM((rows, 3 * WIDTH), f32), [VMEM] * 9, 1 << 30,
        in_hbm(tokens_flat), gain_flat, mix, mix_other, in_hbm(rounded), *decays,
    )
    gain = jnp.tile(out_gain.reshape(2, 1, 16), (1, HEADS, 1)).reshape(2, 256)
    mixed = call(
        out_kernel, shape((rows, width), bf16), [VMEM] * 5, 1 << 30,
        returned.reshape(WIDTH, LANES), parts, gain, mix, mix_other,
    )
    return mixed.reshape(seqs, toks, width)


def solution(mesh):
    finer = Mesh(mesh.devices.reshape(mesh.shape["sp"], 4, 4, 2), ("sp", "dp_0", "dp_1", "dp_2"))
    rows = P(DP, None)
    in_specs = (
        P(DP, "sp", None), P(), rows, rows, rows, rows, rows, P(), P(), P(), P(), P(), rows,
    )

    return jax.shard_map(
        body, mesh=finer, in_specs=in_specs, out_specs=P(DP, "sp", None), check_vma=False
    )
```

```python
import jax
import jax.numpy as jnp
from jax import lax
from jax.experimental import pallas as pl
from jax.experimental.pallas import tpu as pltpu
from jax.sharding import Mesh
from jax.sharding import PartitionSpec as P

DP = ("dp_0", "dp_1", "dp_2")
PLANE = ("dp_0", "dp_1")
HEAD = 32
HEADS = 16
WIDTH = 512
BLOCK = 64
LANES = 128
ALL = 2 * WIDTH + LANES
COLUMNS = 8 * 32
SENT = COLUMNS + 32 + 32 + 8
EPS = 1e-06
f32 = jnp.float32
bf16 = jnp.bfloat16


def dot(a, b):
    return jnp.dot(a, b, preferred_element_type=f32)


def dot_tn(a, b):
    return lax.dot_general(a, b, (((0,), (0,)), ((), ())), preferred_element_type=f32)


def dot_nt(a, b):
    return lax.dot_general(a, b, (((1,), (1,)), ((), ())), preferred_element_type=f32)


def halves(x):
    high = x.astype(bf16)
    return high, (x - high.astype(f32)).astype(bf16)


def grid_of(shape):
    return lax.broadcasted_iota(jnp.int32, shape, 0), lax.broadcasted_iota(jnp.int32, shape, 1)


def as_bf16(mask):
    return jnp.where(mask, 1.0, 0.0).astype(bf16)


def pack_kernel(
    key_hbm, value_hbm, query_hbm, forward_hbm, backward_hbm, mix_hbm,
    out_ref, key_ref, value_ref, query_ref, forward_ref, backward_ref, mix_ref, sems,
):
    sources = (key_hbm, value_hbm, query_hbm, forward_hbm, backward_hbm, mix_hbm)
    targets = (key_ref, value_ref, query_ref, forward_ref, backward_ref, mix_ref)
    copies = [
        pltpu.make_async_copy(source, target, sems.at[i])
        for i, (source, target) in enumerate(zip(sources, targets))
    ]
    for copy in copies:
        copy.start()
    for copy in copies:
        copy.wait()
    row, col = grid_of((16, LANES))
    ranks = dot_tn(forward_ref[...], as_bf16(row == col)) + dot_tn(
        backward_ref[...], as_bf16(row + 16 == col)
    )
    packed = jnp.concatenate([ranks[8 * i : 8 * i + 8, :32] for i in range(4)], axis=1)
    for i in range(16):
        for group in range(4):
            lanes = slice(group * LANES, (group + 1) * LANES)
            out_ref[i, group * 32 : (group + 1) * 32] = key_ref[:, lanes]
            out_ref[i, (4 + group) * 32 : (5 + group) * 32] = value_ref[:, lanes]
        start = (i // 4) * LANES
        out_ref[i, COLUMNS : COLUMNS + 32] = query_ref[:, start : start + LANES]
        start = (i % 4) * 2 * LANES
        out_ref[i, COLUMNS + 32 : COLUMNS + 48] = mix_ref[:, start : start + LANES]
        out_ref[i, COLUMNS + 48 : COLUMNS + 64] = mix_ref[:, start + LANES : start + 2 * LANES]
        out_ref[i, COLUMNS + 64 :] = packed.astype(bf16)


def join_kernel(query_ref, query_in_ref, mix_ref, mix_in_ref, queries_ref, mixes_ref):
    queries_ref[:1] = query_ref[...]
    queries_ref[1:] = query_in_ref[...]
    mixes_ref[:1] = mix_ref[...]
    mixes_ref[1:] = mix_in_ref[...]


def stack_kernel(query_ref, query_in_ref, mix_ref, mix_in_ref, out_ref):
    out_ref[0, :2] = query_ref[...]
    out_ref[0, 2:] = query_in_ref[...]
    out_ref[1, :2] = mix_ref[...]
    out_ref[1, 2:] = mix_in_ref[...]


def slot_of(index, axis):
    apart = index ^ lax.axis_index(axis)
    return apart ^ (apart >> 1)


def normed_halves(tokens_ref, gain_ref):
    values = tokens_ref[...].astype(f32)
    scale = lax.rsqrt(jnp.mean(values * values, axis=-1, keepdims=True) + EPS)
    normed = (values * scale * gain_ref[...]).astype(bf16)
    return [
        jnp.concatenate(
            [normed[:, (2 * i + core) * 32 : (2 * i + core) * 32 + 32] for i in range(16)], axis=1
        )
        for core in range(2)
    ]


def norm_kernel(tokens_ref, gain_ref, normed_ref):
    for core, half in enumerate(normed_halves(tokens_ref, gain_ref)):
        normed_ref[core] = half


def rates_of(ranks, up_forward_ref, up_backward_ref, bias_forward_ref, bias_backward_ref):
    gates = jnp.concatenate(
        [
            dot(ranks[:, :16], up_forward_ref[...]) + bias_forward_ref[...],
            dot(ranks[:, 16:32], up_backward_ref[...]) + bias_backward_ref[...],
        ],
        axis=1,
    )
    return halves(jax.nn.log_sigmoid(gates) * (2.0 / (BLOCK * HEADS)))


def summed(parts, mask, way):
    row, col = grid_of((LANES, LANES))
    ones = as_bf16(mask(row, col) & ((row // BLOCK) == (col // BLOCK)))
    lanes = slice(way * WIDTH, (way + 1) * WIDTH)
    return dot(ones, parts[0][:, lanes]) + dot(ones, parts[1][:, lanes])


def block_kernel(
    normed_ref, own_ref, other_ref, up_forward_ref, up_backward_ref,
    bias_forward_ref, bias_backward_ref, payload_ref, rounded_ref, query_ref, mix_ref,
):
    core = lax.axis_index("dp_2")
    query_ref[0] = own_ref[:, COLUMNS : COLUMNS + 32, :]
    mix_ref[0] = own_ref[:, COLUMNS + 32 : COLUMNS + 64, :]

    def columns(ref, first):
        return jnp.concatenate(
            [ref[:, g * 32 : (g + 1) * 32, :].reshape(WIDTH, LANES) for g in (first, first + 1)], axis=1
        )

    def rank_columns(ref):
        packed = ref[:, COLUMNS + 64 :, :].astype(f32)
        rows = jnp.stack([packed[:, :, 32 * i : 32 * i + 32] for i in range(4)], axis=1)
        return rows.reshape(WIDTH, 32).astype(bf16)

    mine, theirs = normed_ref[core], normed_ref[1 - core]
    pieces = [
        dot(mine, columns(own_ref, first)) + dot(theirs, columns(other_ref, first))
        for first in (0, 2, 4, 6)
    ]
    pieces.append(dot(mine, rank_columns(own_ref)) + dot(theirs, rank_columns(other_ref)))
    pieces.append(jnp.zeros((2 * BLOCK, LANES - 32), f32))
    rounded = jnp.concatenate(pieces, axis=1).astype(bf16)
    rounded_ref[...] = rounded
    values = rounded[:, WIDTH : 2 * WIDTH]
    parts = rates_of(
        rounded[:, 2 * WIDTH :], up_forward_ref, up_backward_ref, bias_forward_ref, bias_backward_ref
    )
    high, low = parts
    row, col = grid_of((LANES, LANES))
    fwd, bwd = slice(0, WIDTH), slice(WIDTH, 2 * WIDTH)
    keys32 = rounded[:, :WIDTH].astype(f32)
    remain = (
        halves(keys32 * jnp.exp(summed(parts, lambda r, c: c > r, 0))),
        halves(keys32 * jnp.exp(summed(parts, lambda r, c: c < r, 1))),
    )
    hrow, hcol = grid_of((HEADS, WIDTH))
    mine = hrow == hcol // HEAD
    erow, ecol = grid_of((WIDTH, LANES))
    srow, scol = grid_of((8, 128))
    close = 0.0
    for way, span in ((0, fwd), (1, bwd)):
        pick = as_bf16(srow == scol // BLOCK)
        sums = dot(pick, high[:, span]) + dot(pick, low[:, span])
        for seq in range(2):
            line = jnp.where(mine, sums[seq : seq + 1], 0.0)
            place = as_bf16(ecol == (2 * way + seq) * HEAD + erow % HEAD)
            line_high, line_low = halves(line)
            both = jnp.concatenate([line_high, line_low], axis=0)
            close = close + dot(both, place)
    tail = lax.broadcasted_iota(jnp.int32, (HEADS, 8, LANES), 1)
    payload_ref[:, HEAD:, :] = jnp.where(
        tail == 0,
        close[:HEADS][:, None, :],
        jnp.where(tail == 1, close[HEADS:][:, None, :], 0.0),
    ).astype(bf16)
    diagonal = (row // HEAD) == (col // HEAD)
    erow, ecol = grid_of((4 * LANES, LANES))
    fold = as_bf16(((erow // LANES) * HEAD + erow % HEAD) == ecol)
    for group in range(4):
        lanes = slice(group * LANES, (group + 1) * LANES)
        parts = []
        for way in range(2):
            for seq in range(2):
                span = slice(seq * BLOCK, (seq + 1) * BLOCK)
                value = values[span, lanes]
                both = jnp.concatenate([half[span, lanes] for half in remain[way]], axis=0)
                state = dot_tn(both, jnp.concatenate([value, value], axis=0))
                parts.append(jnp.where(diagonal, state, 0.0).astype(bf16))
        folded = dot(jnp.concatenate(parts, axis=1), fold).astype(bf16)
        payload_ref[4 * group : 4 * group + 4, :HEAD, :] = folded.reshape(4, HEAD, LANES)


def scan_kernel(payload_ref, out_ref):
    row, col = grid_of((LANES, LANES))
    spread = as_bf16((row // HEAD) == (col // HEAD))
    crow, ccol = grid_of((HEAD, LANES))
    mine = ccol % HEAD == crow
    lines = payload_ref[:, HEAD : HEAD + 8, :].astype(f32)
    closing = 0.0
    for part in range(2):
        line = jnp.where(mine[None], lines[:, part : part + 1, :], 0.0)
        closing = closing + dot(line.astype(bf16).reshape(WIDTH, LANES), spread)
    decay = jnp.exp(closing)
    states = payload_ref[:, :HEAD, :].astype(f32).reshape(WIDTH, LANES)
    lane = lax.broadcasted_iota(jnp.int32, (HEAD, LANES), 1)
    ahead = [None] * HEADS
    behind = [None] * HEADS

    def at(x, i):
        return x[i * HEAD : (i + 1) * HEAD, :]

    carried = jnp.zeros((HEAD, LANES), f32)
    for i in range(HEADS):
        ahead[i] = carried
        carried = at(decay, i) * carried + at(states, i)
    carried = jnp.zeros((HEAD, LANES), f32)
    for i in range(HEADS - 1, -1, -1):
        behind[i] = carried
        carried = at(decay, i) * carried + at(states, i)
    for i in range(HEADS):
        out_ref[i * HEAD : (i + 1) * HEAD, :] = jnp.where(
            lane < LANES // 2, ahead[i], behind[i]
        ).astype(bf16)


def query_kernel(
    tokens_ref, gain_ref, own_ref, other_ref, rounded_ref, up_forward_ref, up_backward_ref,
    bias_forward_ref, bias_backward_ref, out_ref,
):
    core = lax.axis_index("dp_2")

    def weights(ref):
        return jnp.concatenate(
            [
                ref[0, slot_of(quarter, "dp_0")].reshape(WIDTH, LANES)
                for quarter in range(4)
            ],
            axis=1,
        )

    first, second = normed_halves(tokens_ref, gain_ref)
    projected = dot(jnp.where(core == 0, first, second), weights(own_ref)) + dot(
        jnp.where(core == 0, second, first), weights(other_ref)
    )
    queries = projected.astype(bf16).astype(f32) * HEAD ** (-0.5)
    keys = rounded_ref[:, :WIDTH].astype(f32)
    parts = rates_of(
        rounded_ref[:, 2 * WIDTH :], up_forward_ref, up_backward_ref, bias_forward_ref, bias_backward_ref
    )
    decayed, inverse = [], []
    for way, mask in ((0, lambda r, c: c <= r), (1, lambda r, c: c >= r)):
        running = summed(parts, mask, way)
        product = queries * jnp.exp(running)
        out_ref[:, (way + 1) * WIDTH : (way + 2) * WIDTH] = product
        decayed.append(product.astype(bf16))
        inverse.append((keys * jnp.exp(-running)).astype(bf16))
    row, col = grid_of((WIDTH, WIDTH))
    natural = ((col % 256) // 16) * HEAD + (col // 256) * 16 + col % 16
    values = dot(rounded_ref[:, WIDTH : 2 * WIDTH], as_bf16(row == natural)).astype(bf16)
    row, col = grid_of((WIDTH, 256))
    own_lanes = as_bf16((row // BLOCK) == (col // HEAD))
    srow, scol = grid_of((WIDTH, BLOCK))
    lower = (srow % BLOCK) >= scol
    upper = (srow % BLOCK) <= scol
    vrow, vcol = grid_of((WIDTH, LANES))
    own_values = (vrow // BLOCK) == (vcol // 16)
    for seq in range(2):
        span = slice(seq * BLOCK, (seq + 1) * BLOCK)
        for group in range(2):
            wide = slice(group * 256, (group + 1) * 256)
            scores = 0.0
            for way, mask in ((0, lower), (1, upper)):
                stacked = jnp.concatenate([decayed[way][span, wide]] * 8, axis=0) * own_lanes
                scores = scores + jnp.where(mask, dot_nt(stacked, inverse[way][span, wide]), 0.0)
            scores = scores.astype(bf16)
            for half in range(2):
                start = half * 256 + group * LANES
                spread = dot(scores, values[span, start : start + LANES])
                spread = jnp.where(own_values, spread, 0.0)
                total = spread[:BLOCK]
                for head in range(1, 8):
                    total = total + spread[head * BLOCK : (head + 1) * BLOCK]
                out_ref[span, start : start + LANES] = total


def out_kernel(
    states_ref, parts_hbm, gain_ref, own_ref, other_ref, out_ref, parts_ref, sem
):
    fetch = pltpu.make_async_copy(parts_hbm, parts_ref, sem)
    fetch.start()
    core = lax.axis_index("dp_2")
    row, col = grid_of((LANES, 8 * LANES))
    source = (col // 256) * HEAD + ((col // LANES) % 2) * 16 + col % 16
    widen = as_bf16(row == source)
    row, col = grid_of((256, 8 * LANES))
    diagonal = (row // HEAD) == ((col % LANES) // 16)
    full = [
        jnp.where(diagonal, dot(states_ref[g * 256 : (g + 1) * 256, :], widen), 0.0).astype(bf16)
        for g in range(2)
    ]
    fetch.wait()
    totals = [[], []]
    for seq in range(2):
        span = slice(seq * BLOCK, (seq + 1) * BLOCK)
        sides = [[], []]
        for group in range(2):
            queries = jnp.concatenate(
                [
                    parts_ref[span, (way + 1) * WIDTH + group * 256 : (way + 1) * WIDTH + group * 256 + 256]
                    for way in range(2)
                ],
                axis=1,
            )
            right = jnp.concatenate(
                [full[group][:, (2 * way + seq) * 256 : (2 * way + seq + 1) * 256] for way in range(2)],
                axis=0,
            )
            across = dot(jnp.concatenate(halves(queries), axis=0), right)
            across = across[:BLOCK] + across[BLOCK:]
            for half in range(2):
                start = half * 256 + group * LANES
                sides[half].append(
                    parts_ref[span, start : start + LANES] + across[:, half * LANES : (half + 1) * LANES]
                )
        for half in range(2):
            totals[half].append(jnp.concatenate(sides[half], axis=1))
    combined = [jnp.concatenate(total, axis=0) for total in totals]
    high, low = halves(combined[0] * combined[0] + combined[1] * combined[1])
    row, col = grid_of((256, 256))
    ones = as_bf16((row // 16) == (col // 16))
    scale = lax.rsqrt((dot(high, ones) + dot(low, ones)) * (1.0 / HEAD) + EPS)
    attended = [
        (combined[half] * scale * gain_ref[half : half + 1, :]).astype(bf16) for half in range(2)
    ]
    mine = jnp.where(core == 0, attended[0], attended[1])
    theirs = jnp.where(core == 0, attended[1], attended[0])
    for quarter in range(4):
        slot = slot_of(quarter, "dp_1")

        def weights(ref):
            return jnp.concatenate(
                [ref[1, slot, :, rows : rows + 16, :].reshape(256, LANES) for rows in (0, 16)], axis=1
            )

        out_ref[:, quarter * 256 : (quarter + 1) * 256] = (
            dot(mine, weights(own_ref)) + dot(theirs, weights(other_ref))
        ).astype(bf16)


VMEM = pl.BlockSpec(memory_space=pltpu.VMEM)


def call(kernel, outs, specs, cycles, *args, scratch=()):
    many = isinstance(outs, tuple)
    return pl.pallas_call(
        kernel,
        out_shape=outs,
        in_specs=specs,
        out_specs=(VMEM,) * len(outs) if many else VMEM,
        scratch_shapes=scratch,
        cost_estimate=pl.CostEstimate(flops=cycles, bytes_accessed=1 << 20, transcendentals=0),
        compiler_params=pltpu.CompilerParams(vmem_limit_bytes=16 << 20),
    )(*args)


def in_hbm(x):
    return pltpu.with_memory_space_constraint(x, pltpu.HBM)


def swapped(x):
    return lax.ppermute(x, "dp_2", [(0, 1), (1, 0)])


def body(
    tokens, norm_gain, w_query, w_key, w_value, w_rank_forward, w_rank_backward,
    up_forward, up_backward, bias_forward, bias_backward, out_gain, w_out,
):
    seqs, toks, width = tokens.shape
    rows = seqs * toks
    shape = jax.ShapeDtypeStruct
    tokens_flat, gain_flat = tokens.reshape(rows, width), norm_gain.reshape(1, width)
    hbm = pl.BlockSpec(memory_space=pltpu.HBM)
    sources = [
        in_hbm(x)
        for x in (w_key, w_value, w_query, w_rank_forward.T, w_rank_backward.T, w_out)
    ]
    send = call(
        pack_kernel, shape((16, SENT, LANES), bf16), [hbm] * 6, 1 << 26, *sources,
        scratch=[pltpu.VMEM(x.shape, bf16) for x in sources] + [pltpu.SemaphoreType.DMA((6,))],
    )
    own = lax.all_to_all(send, PLANE, 0, 0)
    other = swapped(own)
    normed = call(
        norm_kernel, shape((2, rows, 512), bf16), [VMEM, VMEM], 1 << 28,
        tokens_flat, gain_flat,
    )
    decays = (
        up_forward, up_backward, bias_forward.reshape(1, WIDTH), bias_backward.reshape(1, WIDTH)
    )
    payload, rounded, query, mix = call(
        block_kernel,
        (
            shape((HEADS, 40, LANES), bf16), pltpu.HBM((rows, ALL), bf16),
            shape((1, 16, 32, LANES), bf16), shape((1, 16, 32, LANES), bf16),
        ),
        [VMEM] * 7, 1 << 30, normed, own, other, *decays,
    )
    inbound = lax.all_to_all(payload, "sp", 0, 0)
    for step, flip in enumerate((1, 3)):
        pairs = [(i, i ^ flip) for i in range(4)]
        query_in = lax.ppermute(query, "dp_0", pairs)
        mix_in = lax.ppermute(mix, "dp_1", pairs)
        if step == 0:
            query, mix = call(
                join_kernel, (shape((2, 16, 32, LANES), bf16),) * 2, [VMEM] * 4, 1 << 26,
                query, query_in, mix, mix_in,
            )
        else:
            later = call(
                stack_kernel, shape((2, 4, 16, 32, LANES), bf16), [VMEM] * 4, 1 << 26,
                query, query_in, mix, mix_in,
            )
    later_other = swapped(later)
    states = call(
        scan_kernel, shape((WIDTH, LANES), bf16), [VMEM], 1 << 28,
        inbound,
    )
    returned = lax.all_to_all(states.reshape(HEADS, HEAD, LANES), "sp", 0, 0)
    parts = call(
        query_kernel, pltpu.HBM((rows, 3 * WIDTH), f32), [VMEM] * 9, 1 << 30,
        in_hbm(tokens_flat), gain_flat, later, later_other, in_hbm(rounded), *decays,
    )
    gain = jnp.tile(out_gain.reshape(2, 1, 16), (1, HEADS, 1)).reshape(2, 256)
    mixed = call(
        out_kernel, shape((rows, width), bf16), [VMEM, hbm] + [VMEM] * 3, 1 << 30,
        returned.reshape(WIDTH, LANES), in_hbm(parts), gain, later, later_other,
        scratch=[pltpu.VMEM((rows, 3 * WIDTH), f32), pltpu.SemaphoreType.DMA],
    )
    return mixed.reshape(seqs, toks, width)


def solution(mesh):
    finer = Mesh(mesh.devices.reshape(mesh.shape["sp"], 4, 4, 2), ("sp", "dp_0", "dp_1", "dp_2"))
    rows = P(DP, None)
    in_specs = (
        P(DP, "sp", None), P(), rows, rows, rows, rows, rows, P(), P(), P(), P(), P(), rows,
    )

    return jax.shard_map(
        body, mesh=finer, in_specs=in_specs, out_specs=P(DP, "sp", None), check_vma=False
    )
```

```python
import jax
import jax.numpy as jnp
from jax import lax
from jax.experimental import pallas as pl
from jax.experimental.pallas import tpu as pltpu
from jax.sharding import Mesh
from jax.sharding import PartitionSpec as P

DP = ("dp_0", "dp_1", "dp_2")
PLANE = ("dp_0", "dp_1")
HEAD = 32
HEADS = 16
WIDTH = 512
BLOCK = 64
LANES = 128
ALL = 2 * WIDTH + LANES
COLUMNS = 8 * 32
SENT = COLUMNS + 32 + 32 + 8
EPS = 1e-06
f32 = jnp.float32
bf16 = jnp.bfloat16


def dot(a, b):
    return jnp.dot(a, b, preferred_element_type=f32)


def dot_tn(a, b):
    return lax.dot_general(a, b, (((0,), (0,)), ((), ())), preferred_element_type=f32)


def dot_nt(a, b):
    return lax.dot_general(a, b, (((1,), (1,)), ((), ())), preferred_element_type=f32)


def halves(x):
    high = x.astype(bf16)
    return high, (x - high.astype(f32)).astype(bf16)


def grid_of(shape):
    return lax.broadcasted_iota(jnp.int32, shape, 0), lax.broadcasted_iota(jnp.int32, shape, 1)


def as_bf16(mask):
    return jnp.where(mask, 1.0, 0.0).astype(bf16)


def pack_kernel(
    key_hbm, value_hbm, query_hbm, forward_hbm, backward_hbm, mix_hbm,
    out_ref, key_ref, value_ref, query_ref, forward_ref, backward_ref, mix_ref, sems,
):
    sources = (key_hbm, value_hbm, query_hbm, forward_hbm, backward_hbm, mix_hbm)
    targets = (key_ref, value_ref, query_ref, forward_ref, backward_ref, mix_ref)
    copies = [
        pltpu.make_async_copy(source, target, sems.at[i])
        for i, (source, target) in enumerate(zip(sources, targets))
    ]
    for copy in copies:
        copy.start()
    for copy in copies:
        copy.wait()
    row, col = grid_of((16, LANES))
    ranks = dot_tn(forward_ref[...], as_bf16(row == col)) + dot_tn(
        backward_ref[...], as_bf16(row + 16 == col)
    )
    packed = jnp.concatenate([ranks[8 * i : 8 * i + 8, :32] for i in range(4)], axis=1)
    for i in range(16):
        for group in range(4):
            lanes = slice(group * LANES, (group + 1) * LANES)
            out_ref[i, group * 32 : (group + 1) * 32] = key_ref[:, lanes]
            out_ref[i, (4 + group) * 32 : (5 + group) * 32] = value_ref[:, lanes]
        start = (i // 4) * LANES
        out_ref[i, COLUMNS : COLUMNS + 32] = query_ref[:, start : start + LANES]
        out_ref[i, COLUMNS + 32 : COLUMNS + 48] = mix_ref[:, 2 * start : 2 * start + LANES]
        out_ref[i, COLUMNS + 48 : COLUMNS + 64] = mix_ref[:, 2 * start + LANES : 2 * start + 2 * LANES]
        out_ref[i, COLUMNS + 64 :] = packed.astype(bf16)


def join_kernel(first_ref, second_ref, out_ref):
    count = first_ref.shape[0]
    out_ref[:count] = first_ref[...]
    out_ref[count:] = second_ref[...]


def slot_of(index, axis):
    apart = index ^ lax.axis_index(axis)
    return apart ^ (apart >> 1)


def normed_halves(tokens_ref, gain_ref):
    values = tokens_ref[...].astype(f32)
    scale = lax.rsqrt(jnp.mean(values * values, axis=-1, keepdims=True) + EPS)
    normed = (values * scale * gain_ref[...]).astype(bf16)
    return [
        jnp.concatenate(
            [normed[:, (2 * i + core) * 32 : (2 * i + core) * 32 + 32] for i in range(16)], axis=1
        )
        for core in range(2)
    ]


def norm_kernel(tokens_ref, gain_ref, normed_ref):
    for core, half in enumerate(normed_halves(tokens_ref, gain_ref)):
        normed_ref[core] = half


def rates_of(ranks, up_forward_ref, up_backward_ref, bias_forward_ref, bias_backward_ref):
    gates = jnp.concatenate(
        [
            dot(ranks[:, :16], up_forward_ref[...]) + bias_forward_ref[...],
            dot(ranks[:, 16:32], up_backward_ref[...]) + bias_backward_ref[...],
        ],
        axis=1,
    )
    return halves(jax.nn.log_sigmoid(gates) * (2.0 / (BLOCK * HEADS)))


def summed(parts, mask, way):
    row, col = grid_of((LANES, LANES))
    ones = as_bf16(mask(row, col) & ((row // BLOCK) == (col // BLOCK)))
    lanes = slice(way * WIDTH, (way + 1) * WIDTH)
    return dot(ones, parts[0][:, lanes]) + dot(ones, parts[1][:, lanes])


def block_kernel(
    normed_ref, own_ref, other_ref, up_forward_ref, up_backward_ref,
    bias_forward_ref, bias_backward_ref, payload_ref, rounded_ref,
):
    core = lax.axis_index("dp_2")

    def columns(ref, first):
        return jnp.concatenate(
            [ref[:, g * 32 : (g + 1) * 32, :].reshape(WIDTH, LANES) for g in (first, first + 1)], axis=1
        )

    def rank_columns(ref):
        packed = ref[:, COLUMNS + 64 :, :].astype(f32)
        rows = jnp.stack([packed[:, :, 32 * i : 32 * i + 32] for i in range(4)], axis=1)
        return rows.reshape(WIDTH, 32).astype(bf16)

    mine, theirs = normed_ref[core], normed_ref[1 - core]
    pieces = [
        dot(mine, columns(own_ref, first)) + dot(theirs, columns(other_ref, first))
        for first in (0, 2, 4, 6)
    ]
    pieces.append(dot(mine, rank_columns(own_ref)) + dot(theirs, rank_columns(other_ref)))
    pieces.append(jnp.zeros((2 * BLOCK, LANES - 32), f32))
    rounded = jnp.concatenate(pieces, axis=1).astype(bf16)
    rounded_ref[...] = rounded
    values = rounded[:, WIDTH : 2 * WIDTH]
    parts = rates_of(
        rounded[:, 2 * WIDTH :], up_forward_ref, up_backward_ref, bias_forward_ref, bias_backward_ref
    )
    high, low = parts
    row, col = grid_of((LANES, LANES))
    fwd, bwd = slice(0, WIDTH), slice(WIDTH, 2 * WIDTH)
    keys32 = rounded[:, :WIDTH].astype(f32)
    remain = (
        halves(keys32 * jnp.exp(summed(parts, lambda r, c: c > r, 0))),
        halves(keys32 * jnp.exp(summed(parts, lambda r, c: c < r, 1))),
    )
    hrow, hcol = grid_of((HEADS, WIDTH))
    mine = hrow == hcol // HEAD
    erow, ecol = grid_of((WIDTH, LANES))
    srow, scol = grid_of((8, 128))
    close = 0.0
    for way, span in ((0, fwd), (1, bwd)):
        pick = as_bf16(srow == scol // BLOCK)
        sums = dot(pick, high[:, span]) + dot(pick, low[:, span])
        for seq in range(2):
            line = jnp.where(mine, sums[seq : seq + 1], 0.0)
            place = as_bf16(ecol == (2 * way + seq) * HEAD + erow % HEAD)
            line_high, line_low = halves(line)
            both = jnp.concatenate([line_high, line_low], axis=0)
            close = close + dot(both, place)
    tail = lax.broadcasted_iota(jnp.int32, (HEADS, 8, LANES), 1)
    payload_ref[:, HEAD:, :] = jnp.where(
        tail == 0,
        close[:HEADS][:, None, :],
        jnp.where(tail == 1, close[HEADS:][:, None, :], 0.0),
    ).astype(bf16)
    diagonal = (row // HEAD) == (col // HEAD)
    erow, ecol = grid_of((4 * LANES, LANES))
    fold = as_bf16(((erow // LANES) * HEAD + erow % HEAD) == ecol)
    for group in range(4):
        lanes = slice(group * LANES, (group + 1) * LANES)
        parts = []
        for way in range(2):
            for seq in range(2):
                span = slice(seq * BLOCK, (seq + 1) * BLOCK)
                value = values[span, lanes]
                both = jnp.concatenate([half[span, lanes] for half in remain[way]], axis=0)
                state = dot_tn(both, jnp.concatenate([value, value], axis=0))
                parts.append(jnp.where(diagonal, state, 0.0).astype(bf16))
        folded = dot(jnp.concatenate(parts, axis=1), fold).astype(bf16)
        payload_ref[4 * group : 4 * group + 4, :HEAD, :] = folded.reshape(4, HEAD, LANES)


def scan_kernel(payload_ref, out_ref):
    row, col = grid_of((LANES, LANES))
    spread = as_bf16((row // HEAD) == (col // HEAD))
    crow, ccol = grid_of((HEAD, LANES))
    mine = ccol % HEAD == crow
    lines = payload_ref[:, HEAD : HEAD + 8, :].astype(f32)
    closing = 0.0
    for part in range(2):
        line = jnp.where(mine[None], lines[:, part : part + 1, :], 0.0)
        closing = closing + dot(line.astype(bf16).reshape(WIDTH, LANES), spread)
    decay = jnp.exp(closing)
    states = payload_ref[:, :HEAD, :].astype(f32).reshape(WIDTH, LANES)
    lane = lax.broadcasted_iota(jnp.int32, (HEAD, LANES), 1)
    ahead = [None] * HEADS
    behind = [None] * HEADS

    def at(x, i):
        return x[i * HEAD : (i + 1) * HEAD, :]

    carried = jnp.zeros((HEAD, LANES), f32)
    for i in range(HEADS):
        ahead[i] = carried
        carried = at(decay, i) * carried + at(states, i)
    carried = jnp.zeros((HEAD, LANES), f32)
    for i in range(HEADS - 1, -1, -1):
        behind[i] = carried
        carried = at(decay, i) * carried + at(states, i)
    for i in range(HEADS):
        out_ref[i * HEAD : (i + 1) * HEAD, :] = jnp.where(
            lane < LANES // 2, ahead[i], behind[i]
        ).astype(bf16)


def query_kernel(
    tokens_ref, gain_ref, own_ref, other_ref, rounded_ref, up_forward_ref, up_backward_ref,
    bias_forward_ref, bias_backward_ref, out_ref,
):
    core = lax.axis_index("dp_2")

    def weights(ref):
        return jnp.concatenate(
            [
                ref[slot_of(quarter, "dp_0"), :, :32, :].reshape(WIDTH, LANES)
                for quarter in range(4)
            ],
            axis=1,
        )

    first, second = normed_halves(tokens_ref, gain_ref)
    projected = dot(jnp.where(core == 0, first, second), weights(own_ref)) + dot(
        jnp.where(core == 0, second, first), weights(other_ref)
    )
    queries = projected.astype(bf16).astype(f32) * HEAD ** (-0.5)
    keys = rounded_ref[:, :WIDTH].astype(f32)
    parts = rates_of(
        rounded_ref[:, 2 * WIDTH :], up_forward_ref, up_backward_ref, bias_forward_ref, bias_backward_ref
    )
    decayed, inverse = [], []
    for way, mask in ((0, lambda r, c: c <= r), (1, lambda r, c: c >= r)):
        running = summed(parts, mask, way)
        product = queries * jnp.exp(running)
        out_ref[:, (way + 1) * WIDTH : (way + 2) * WIDTH] = product
        decayed.append(product.astype(bf16))
        inverse.append((keys * jnp.exp(-running)).astype(bf16))
    row, col = grid_of((WIDTH, WIDTH))
    natural = ((col % 256) // 16) * HEAD + (col // 256) * 16 + col % 16
    values = dot(rounded_ref[:, WIDTH : 2 * WIDTH], as_bf16(row == natural)).astype(bf16)
    row, col = grid_of((WIDTH, 256))
    own_lanes = as_bf16((row // BLOCK) == (col // HEAD))
    srow, scol = grid_of((WIDTH, BLOCK))
    lower = (srow % BLOCK) >= scol
    upper = (srow % BLOCK) <= scol
    vrow, vcol = grid_of((WIDTH, LANES))
    own_values = (vrow // BLOCK) == (vcol // 16)
    for seq in range(2):
        span = slice(seq * BLOCK, (seq + 1) * BLOCK)
        for group in range(2):
            wide = slice(group * 256, (group + 1) * 256)
            scores = 0.0
            for way, mask in ((0, lower), (1, upper)):
                stacked = jnp.concatenate([decayed[way][span, wide]] * 8, axis=0) * own_lanes
                scores = scores + jnp.where(mask, dot_nt(stacked, inverse[way][span, wide]), 0.0)
            scores = scores.astype(bf16)
            for half in range(2):
                start = half * 256 + group * LANES
                spread = dot(scores, values[span, start : start + LANES])
                spread = jnp.where(own_values, spread, 0.0)
                total = spread[:BLOCK]
                for head in range(1, 8):
                    total = total + spread[head * BLOCK : (head + 1) * BLOCK]
                out_ref[span, start : start + LANES] = total


def out_kernel(states_ref, parts_ref, gain_ref, own_ref, other_ref, out_ref):
    core = lax.axis_index("dp_2")
    row, col = grid_of((LANES, 8 * LANES))
    source = (col // 256) * HEAD + ((col // LANES) % 2) * 16 + col % 16
    widen = as_bf16(row == source)
    row, col = grid_of((256, 8 * LANES))
    diagonal = (row // HEAD) == ((col % LANES) // 16)
    full = [
        jnp.where(diagonal, dot(states_ref[g * 256 : (g + 1) * 256, :], widen), 0.0).astype(bf16)
        for g in range(2)
    ]
    totals = [[], []]
    for seq in range(2):
        span = slice(seq * BLOCK, (seq + 1) * BLOCK)
        sides = [[], []]
        for group in range(2):
            queries = jnp.concatenate(
                [
                    parts_ref[span, (way + 1) * WIDTH + group * 256 : (way + 1) * WIDTH + group * 256 + 256]
                    for way in range(2)
                ],
                axis=1,
            )
            right = jnp.concatenate(
                [full[group][:, (2 * way + seq) * 256 : (2 * way + seq + 1) * 256] for way in range(2)],
                axis=0,
            )
            across = dot(jnp.concatenate(halves(queries), axis=0), right)
            across = across[:BLOCK] + across[BLOCK:]
            for half in range(2):
                start = half * 256 + group * LANES
                sides[half].append(
                    parts_ref[span, start : start + LANES] + across[:, half * LANES : (half + 1) * LANES]
                )
        for half in range(2):
            totals[half].append(jnp.concatenate(sides[half], axis=1))
    combined = [jnp.concatenate(total, axis=0) for total in totals]
    high, low = halves(combined[0] * combined[0] + combined[1] * combined[1])
    row, col = grid_of((256, 256))
    ones = as_bf16((row // 16) == (col // 16))
    scale = lax.rsqrt((dot(high, ones) + dot(low, ones)) * (1.0 / HEAD) + EPS)
    attended = [
        (combined[half] * scale * gain_ref[half : half + 1, :]).astype(bf16) for half in range(2)
    ]
    mine = jnp.where(core == 0, attended[0], attended[1])
    theirs = jnp.where(core == 0, attended[1], attended[0])
    for quarter in range(4):
        slot = slot_of(quarter, "dp_0")

        def weights(ref):
            return jnp.concatenate(
                [ref[slot, :, rows : rows + 16, :].reshape(256, LANES) for rows in (32, 48)], axis=1
            )

        out_ref[:, quarter * 256 : (quarter + 1) * 256] = (
            dot(mine, weights(own_ref)) + dot(theirs, weights(other_ref))
        ).astype(bf16)


VMEM = pl.BlockSpec(memory_space=pltpu.VMEM)


def call(kernel, outs, specs, cycles, *args, scratch=()):
    many = isinstance(outs, tuple)
    return pl.pallas_call(
        kernel,
        out_shape=outs,
        in_specs=specs,
        out_specs=(VMEM,) * len(outs) if many else VMEM,
        scratch_shapes=scratch,
        cost_estimate=pl.CostEstimate(flops=cycles, bytes_accessed=1 << 20, transcendentals=0),
        compiler_params=pltpu.CompilerParams(vmem_limit_bytes=16 << 20),
    )(*args)


def in_hbm(x):
    return pltpu.with_memory_space_constraint(x, pltpu.HBM)


def swapped(x):
    return lax.ppermute(x, "dp_2", [(0, 1), (1, 0)])


def body(
    tokens, norm_gain, w_query, w_key, w_value, w_rank_forward, w_rank_backward,
    up_forward, up_backward, bias_forward, bias_backward, out_gain, w_out,
):
    seqs, toks, width = tokens.shape
    rows = seqs * toks
    shape = jax.ShapeDtypeStruct
    tokens_flat, gain_flat = tokens.reshape(rows, width), norm_gain.reshape(1, width)
    hbm = pl.BlockSpec(memory_space=pltpu.HBM)
    sources = [
        in_hbm(x)
        for x in (w_key, w_value, w_query, w_rank_forward.T, w_rank_backward.T, w_out)
    ]
    send = call(
        pack_kernel, shape((16, SENT, LANES), bf16), [hbm] * 6, 1 << 26, *sources,
        scratch=[pltpu.VMEM(x.shape, bf16) for x in sources] + [pltpu.SemaphoreType.DMA((6,))],
    )
    own = lax.all_to_all(send, PLANE, 0, 0)
    other = swapped(own)
    mix = own[None, :, COLUMNS : COLUMNS + 64, :]
    for flip in (1, 3):
        arrived = lax.ppermute(mix, "dp_0", [(i, i ^ flip) for i in range(4)])
        mix = call(
            join_kernel, shape((2 * mix.shape[0], 16, 64, LANES), bf16), [VMEM] * 2, 1 << 26,
            mix, arrived,
        )
    normed = call(
        norm_kernel, shape((2, rows, 512), bf16), [VMEM, VMEM], 1 << 28,
        tokens_flat, gain_flat,
    )
    decays = (
        up_forward, up_backward, bias_forward.reshape(1, WIDTH), bias_backward.reshape(1, WIDTH)
    )
    payload, rounded = call(
        block_kernel,
        (
            shape((HEADS, 40, LANES), bf16), pltpu.HBM((rows, ALL), bf16),
        ),
        [VMEM] * 7, 1 << 30, normed, own, other, *decays,
    )
    inbound = lax.all_to_all(payload, "sp", 0, 0)
    mix_other = swapped(mix)
    states = call(
        scan_kernel, shape((WIDTH, LANES), bf16), [VMEM], 1 << 28,
        inbound,
    )
    returned = lax.all_to_all(states.reshape(HEADS, HEAD, LANES), "sp", 0, 0)
    parts = call(
        query_kernel, pltpu.HBM((rows, 3 * WIDTH), f32), [VMEM] * 9, 1 << 30,
        in_hbm(tokens_flat), gain_flat, mix, mix_other, in_hbm(rounded), *decays,
    )
    gain = jnp.tile(out_gain.reshape(2, 1, 16), (1, HEADS, 1)).reshape(2, 256)
    mixed = call(
        out_kernel, shape((rows, width), bf16), [VMEM] * 5, 1 << 30,
        returned.reshape(WIDTH, LANES), parts, gain, mix, mix_other,
    )
    return mixed.reshape(seqs, toks, width)


def solution(mesh):
    finer = Mesh(mesh.devices.reshape(mesh.shape["sp"], 4, 4, 2), ("sp", "dp_0", "dp_1", "dp_2"))
    rows = P(DP, None)
    in_specs = (
        P(DP, "sp", None), P(), rows, rows, rows, rows, rows, P(), P(), P(), P(), P(), rows,
    )

    return jax.shard_map(
        body, mesh=finer, in_specs=in_specs, out_specs=P(DP, "sp", None), check_vma=False
    )
```

```python
import jax
import jax.numpy as jnp
from jax import lax
from jax.experimental import pallas as pl
from jax.experimental.pallas import tpu as pltpu
from jax.sharding import Mesh
from jax.sharding import PartitionSpec as P

DP = ("dp_0", "dp_1", "dp_2")
PLANE = ("dp_0", "dp_1")
HEAD = 32
HEADS = 16
WIDTH = 512
BLOCK = 64
LANES = 128
ALL = 2 * WIDTH + LANES
COLUMNS = 8 * 32
SENT = COLUMNS + 32 + 32 + 8
EPS = 1e-06
GROUP = [(z + 12) % 16 for z in range(16)]
f32 = jnp.float32
bf16 = jnp.bfloat16


def dot(a, b):
    return jnp.dot(a, b, preferred_element_type=f32)


def dot_tn(a, b):
    return lax.dot_general(a, b, (((0,), (0,)), ((), ())), preferred_element_type=f32)


def dot_nt(a, b):
    return lax.dot_general(a, b, (((1,), (1,)), ((), ())), preferred_element_type=f32)


def halves(x):
    high = x.astype(bf16)
    return high, (x - high.astype(f32)).astype(bf16)


def grid_of(shape):
    return lax.broadcasted_iota(jnp.int32, shape, 0), lax.broadcasted_iota(jnp.int32, shape, 1)


def as_bf16(mask):
    return jnp.where(mask, 1.0, 0.0).astype(bf16)


def pack_kernel(
    key_hbm, value_hbm, query_hbm, forward_hbm, backward_hbm, mix_hbm,
    out_ref, key_ref, value_ref, query_ref, forward_ref, backward_ref, mix_ref, sems,
):
    sources = (key_hbm, value_hbm, query_hbm, forward_hbm, backward_hbm, mix_hbm)
    targets = (key_ref, value_ref, query_ref, forward_ref, backward_ref, mix_ref)
    copies = [
        pltpu.make_async_copy(source, target, sems.at[i])
        for i, (source, target) in enumerate(zip(sources, targets))
    ]
    for copy in copies:
        copy.start()
    for copy in copies:
        copy.wait()
    row, col = grid_of((16, LANES))
    ranks = dot_tn(forward_ref[...], as_bf16(row == col)) + dot_tn(
        backward_ref[...], as_bf16(row + 16 == col)
    )
    packed = jnp.concatenate([ranks[8 * i : 8 * i + 8, :32] for i in range(4)], axis=1)
    for i in range(16):
        for group in range(4):
            lanes = slice(group * LANES, (group + 1) * LANES)
            out_ref[i, group * 32 : (group + 1) * 32] = key_ref[:, lanes]
            out_ref[i, (4 + group) * 32 : (5 + group) * 32] = value_ref[:, lanes]
        start = (i // 4) * LANES
        out_ref[i, COLUMNS : COLUMNS + 32] = query_ref[:, start : start + LANES]
        out_ref[i, COLUMNS + 32 : COLUMNS + 48] = mix_ref[:, 2 * start : 2 * start + LANES]
        out_ref[i, COLUMNS + 48 : COLUMNS + 64] = mix_ref[:, 2 * start + LANES : 2 * start + 2 * LANES]
        out_ref[i, COLUMNS + 64 :] = packed.astype(bf16)


def join_kernel(first_ref, second_ref, out_ref):
    count = first_ref.shape[0]
    out_ref[:count] = first_ref[...]
    out_ref[count:] = second_ref[...]


def slot_of(index, axis):
    apart = index ^ lax.axis_index(axis)
    return apart ^ (apart >> 1)


def normed_halves(tokens_ref, gain_ref):
    values = tokens_ref[...].astype(f32)
    scale = lax.rsqrt(jnp.mean(values * values, axis=-1, keepdims=True) + EPS)
    normed = (values * scale * gain_ref[...]).astype(bf16)
    return [
        jnp.concatenate(
            [normed[:, (2 * i + core) * 32 : (2 * i + core) * 32 + 32] for i in range(16)], axis=1
        )
        for core in range(2)
    ]


def norm_kernel(tokens_ref, gain_ref, normed_ref):
    for core, half in enumerate(normed_halves(tokens_ref, gain_ref)):
        normed_ref[core] = half


def rates_of(ranks, up_forward_ref, up_backward_ref, bias_forward_ref, bias_backward_ref):
    gates = jnp.concatenate(
        [
            dot(ranks[:, :16], up_forward_ref[...]) + bias_forward_ref[...],
            dot(ranks[:, 16:32], up_backward_ref[...]) + bias_backward_ref[...],
        ],
        axis=1,
    )
    return halves(jax.nn.log_sigmoid(gates) * (2.0 / (BLOCK * HEADS)))


def summed(parts, mask, way):
    row, col = grid_of((LANES, LANES))
    ones = as_bf16(mask(row, col) & ((row // BLOCK) == (col // BLOCK)))
    lanes = slice(way * WIDTH, (way + 1) * WIDTH)
    return dot(ones, parts[0][:, lanes]) + dot(ones, parts[1][:, lanes])


def block_kernel(
    normed_ref, own_ref, other_ref, up_forward_ref, up_backward_ref,
    bias_forward_ref, bias_backward_ref, payload_ref, rounded_ref,
):
    core = lax.axis_index("dp_2")

    def columns(ref, first):
        return jnp.concatenate(
            [ref[:, g * 32 : (g + 1) * 32, :].reshape(WIDTH, LANES) for g in (first, first + 1)], axis=1
        )

    def rank_columns(ref):
        packed = ref[:, COLUMNS + 64 :, :].astype(f32)
        rows = jnp.stack([packed[:, :, 32 * i : 32 * i + 32] for i in range(4)], axis=1)
        return rows.reshape(WIDTH, 32).astype(bf16)

    mine, theirs = normed_ref[core], normed_ref[1 - core]
    pieces = [
        dot(mine, columns(own_ref, first)) + dot(theirs, columns(other_ref, first))
        for first in (0, 2, 4, 6)
    ]
    pieces.append(dot(mine, rank_columns(own_ref)) + dot(theirs, rank_columns(other_ref)))
    pieces.append(jnp.zeros((2 * BLOCK, LANES - 32), f32))
    rounded = jnp.concatenate(pieces, axis=1).astype(bf16)
    rounded_ref[...] = rounded
    values = rounded[:, WIDTH : 2 * WIDTH]
    parts = rates_of(
        rounded[:, 2 * WIDTH :], up_forward_ref, up_backward_ref, bias_forward_ref, bias_backward_ref
    )
    high, low = parts
    row, col = grid_of((LANES, LANES))
    fwd, bwd = slice(0, WIDTH), slice(WIDTH, 2 * WIDTH)
    keys32 = rounded[:, :WIDTH].astype(f32)
    remain = (
        halves(keys32 * jnp.exp(summed(parts, lambda r, c: c > r, 0))),
        halves(keys32 * jnp.exp(summed(parts, lambda r, c: c < r, 1))),
    )
    hrow, hcol = grid_of((HEADS, WIDTH))
    mine = hrow == hcol // HEAD
    erow, ecol = grid_of((WIDTH, LANES))
    srow, scol = grid_of((8, 128))
    close = 0.0
    for way, span in ((0, fwd), (1, bwd)):
        pick = as_bf16(srow == scol // BLOCK)
        sums = dot(pick, high[:, span]) + dot(pick, low[:, span])
        for seq in range(2):
            line = jnp.where(mine, sums[seq : seq + 1], 0.0)
            place = as_bf16(ecol == (2 * way + seq) * HEAD + erow % HEAD)
            line_high, line_low = halves(line)
            both = jnp.concatenate([line_high, line_low], axis=0)
            close = close + dot(both, place)
    tail = lax.broadcasted_iota(jnp.int32, (HEADS, 8, LANES), 1)
    payload_ref[:, HEAD:, :] = jnp.where(
        tail == 0,
        close[:HEADS][:, None, :],
        jnp.where(tail == 1, close[HEADS:][:, None, :], 0.0),
    ).astype(bf16)
    diagonal = (row // HEAD) == (col // HEAD)
    erow, ecol = grid_of((4 * LANES, LANES))
    fold = as_bf16(((erow // LANES) * HEAD + erow % HEAD) == ecol)
    for group in range(4):
        lanes = slice(group * LANES, (group + 1) * LANES)
        parts = []
        for way in range(2):
            for seq in range(2):
                span = slice(seq * BLOCK, (seq + 1) * BLOCK)
                value = values[span, lanes]
                both = jnp.concatenate([half[span, lanes] for half in remain[way]], axis=0)
                state = dot_tn(both, jnp.concatenate([value, value], axis=0))
                parts.append(jnp.where(diagonal, state, 0.0).astype(bf16))
        folded = dot(jnp.concatenate(parts, axis=1), fold).astype(bf16)
        payload_ref[4 * group : 4 * group + 4, :HEAD, :] = folded.reshape(4, HEAD, LANES)


def scan_kernel(payload_ref, out_ref):
    row, col = grid_of((LANES, LANES))
    spread = as_bf16((row // HEAD) == (col // HEAD))
    crow, ccol = grid_of((HEAD, LANES))
    mine = ccol % HEAD == crow
    lines = payload_ref[:, HEAD : HEAD + 8, :].astype(f32)
    closing = 0.0
    for part in range(2):
        line = jnp.where(mine[None], lines[:, part : part + 1, :], 0.0)
        closing = closing + dot(line.astype(bf16).reshape(WIDTH, LANES), spread)
    decay = jnp.exp(closing)
    states = payload_ref[:, :HEAD, :].astype(f32).reshape(WIDTH, LANES)
    lane = lax.broadcasted_iota(jnp.int32, (HEAD, LANES), 1)
    ahead = [None] * HEADS
    behind = [None] * HEADS

    def at(x, i):
        return x[i * HEAD : (i + 1) * HEAD, :]

    carried = jnp.zeros((HEAD, LANES), f32)
    order = [GROUP.index(z) for z in range(HEADS)]
    for i in order:
        ahead[i] = carried
        carried = at(decay, i) * carried + at(states, i)
    carried = jnp.zeros((HEAD, LANES), f32)
    for i in reversed(order):
        behind[i] = carried
        carried = at(decay, i) * carried + at(states, i)
    for i in range(HEADS):
        out_ref[i * HEAD : (i + 1) * HEAD, :] = jnp.where(
            lane < LANES // 2, ahead[i], behind[i]
        ).astype(bf16)


def query_kernel(
    tokens_ref, gain_ref, own_ref, other_ref, rounded_ref, up_forward_ref, up_backward_ref,
    bias_forward_ref, bias_backward_ref, out_ref,
):
    core = lax.axis_index("dp_2")

    def weights(ref):
        return jnp.concatenate(
            [
                ref[slot_of(quarter, "dp_0"), :, :32, :].reshape(WIDTH, LANES)
                for quarter in range(4)
            ],
            axis=1,
        )

    first, second = normed_halves(tokens_ref, gain_ref)
    projected = dot(jnp.where(core == 0, first, second), weights(own_ref)) + dot(
        jnp.where(core == 0, second, first), weights(other_ref)
    )
    queries = projected.astype(bf16).astype(f32) * HEAD ** (-0.5)
    keys = rounded_ref[:, :WIDTH].astype(f32)
    parts = rates_of(
        rounded_ref[:, 2 * WIDTH :], up_forward_ref, up_backward_ref, bias_forward_ref, bias_backward_ref
    )
    decayed, inverse = [], []
    for way, mask in ((0, lambda r, c: c <= r), (1, lambda r, c: c >= r)):
        running = summed(parts, mask, way)
        product = queries * jnp.exp(running)
        out_ref[:, (way + 1) * WIDTH : (way + 2) * WIDTH] = product
        decayed.append(product.astype(bf16))
        inverse.append((keys * jnp.exp(-running)).astype(bf16))
    row, col = grid_of((WIDTH, WIDTH))
    natural = ((col % 256) // 16) * HEAD + (col // 256) * 16 + col % 16
    values = dot(rounded_ref[:, WIDTH : 2 * WIDTH], as_bf16(row == natural)).astype(bf16)
    row, col = grid_of((WIDTH, 256))
    own_lanes = as_bf16((row // BLOCK) == (col // HEAD))
    srow, scol = grid_of((WIDTH, BLOCK))
    lower = (srow % BLOCK) >= scol
    upper = (srow % BLOCK) <= scol
    vrow, vcol = grid_of((WIDTH, LANES))
    own_values = (vrow // BLOCK) == (vcol // 16)
    for seq in range(2):
        span = slice(seq * BLOCK, (seq + 1) * BLOCK)
        for group in range(2):
            wide = slice(group * 256, (group + 1) * 256)
            scores = 0.0
            for way, mask in ((0, lower), (1, upper)):
                stacked = jnp.concatenate([decayed[way][span, wide]] * 8, axis=0) * own_lanes
                scores = scores + jnp.where(mask, dot_nt(stacked, inverse[way][span, wide]), 0.0)
            scores = scores.astype(bf16)
            for half in range(2):
                start = half * 256 + group * LANES
                spread = dot(scores, values[span, start : start + LANES])
                spread = jnp.where(own_values, spread, 0.0)
                total = spread[:BLOCK]
                for head in range(1, 8):
                    total = total + spread[head * BLOCK : (head + 1) * BLOCK]
                out_ref[span, start : start + LANES] = total


def out_kernel(states_ref, parts_ref, gain_ref, own_ref, other_ref, out_ref):
    core = lax.axis_index("dp_2")
    row, col = grid_of((LANES, 8 * LANES))
    source = (col // 256) * HEAD + ((col // LANES) % 2) * 16 + col % 16
    widen = as_bf16(row == source)
    row, col = grid_of((256, 8 * LANES))
    diagonal = (row // HEAD) == ((col % LANES) // 16)
    full = [
        jnp.where(diagonal, dot(states_ref[g * 256 : (g + 1) * 256, :], widen), 0.0).astype(bf16)
        for g in range(2)
    ]
    totals = [[], []]
    for seq in range(2):
        span = slice(seq * BLOCK, (seq + 1) * BLOCK)
        sides = [[], []]
        for group in range(2):
            queries = jnp.concatenate(
                [
                    parts_ref[span, (way + 1) * WIDTH + group * 256 : (way + 1) * WIDTH + group * 256 + 256]
                    for way in range(2)
                ],
                axis=1,
            )
            right = jnp.concatenate(
                [full[group][:, (2 * way + seq) * 256 : (2 * way + seq + 1) * 256] for way in range(2)],
                axis=0,
            )
            across = dot(jnp.concatenate(halves(queries), axis=0), right)
            across = across[:BLOCK] + across[BLOCK:]
            for half in range(2):
                start = half * 256 + group * LANES
                sides[half].append(
                    parts_ref[span, start : start + LANES] + across[:, half * LANES : (half + 1) * LANES]
                )
        for half in range(2):
            totals[half].append(jnp.concatenate(sides[half], axis=1))
    combined = [jnp.concatenate(total, axis=0) for total in totals]
    high, low = halves(combined[0] * combined[0] + combined[1] * combined[1])
    row, col = grid_of((256, 256))
    ones = as_bf16((row // 16) == (col // 16))
    scale = lax.rsqrt((dot(high, ones) + dot(low, ones)) * (1.0 / HEAD) + EPS)
    attended = [
        (combined[half] * scale * gain_ref[half : half + 1, :]).astype(bf16) for half in range(2)
    ]
    mine = jnp.where(core == 0, attended[0], attended[1])
    theirs = jnp.where(core == 0, attended[1], attended[0])
    for quarter in range(4):
        slot = slot_of(quarter, "dp_0")

        def weights(ref):
            return jnp.concatenate(
                [ref[slot, :, rows : rows + 16, :].reshape(256, LANES) for rows in (32, 48)], axis=1
            )

        out_ref[:, quarter * 256 : (quarter + 1) * 256] = (
            dot(mine, weights(own_ref)) + dot(theirs, weights(other_ref))
        ).astype(bf16)


VMEM = pl.BlockSpec(memory_space=pltpu.VMEM)


def call(kernel, outs, specs, cycles, *args, scratch=()):
    many = isinstance(outs, tuple)
    return pl.pallas_call(
        kernel,
        out_shape=outs,
        in_specs=specs,
        out_specs=(VMEM,) * len(outs) if many else VMEM,
        scratch_shapes=scratch,
        cost_estimate=pl.CostEstimate(flops=cycles, bytes_accessed=1 << 20, transcendentals=0),
        compiler_params=pltpu.CompilerParams(vmem_limit_bytes=16 << 20),
    )(*args)


def in_hbm(x):
    return pltpu.with_memory_space_constraint(x, pltpu.HBM)


def swapped(x):
    return lax.ppermute(x, "dp_2", [(0, 1), (1, 0)])


def body(
    tokens, norm_gain, w_query, w_key, w_value, w_rank_forward, w_rank_backward,
    up_forward, up_backward, bias_forward, bias_backward, out_gain, w_out,
):
    seqs, toks, width = tokens.shape
    rows = seqs * toks
    shape = jax.ShapeDtypeStruct
    tokens_flat, gain_flat = tokens.reshape(rows, width), norm_gain.reshape(1, width)
    hbm = pl.BlockSpec(memory_space=pltpu.HBM)
    sources = [
        in_hbm(x)
        for x in (w_key, w_value, w_query, w_rank_forward.T, w_rank_backward.T, w_out)
    ]
    send = call(
        pack_kernel, shape((16, SENT, LANES), bf16), [hbm] * 6, 1 << 26, *sources,
        scratch=[pltpu.VMEM(x.shape, bf16) for x in sources] + [pltpu.SemaphoreType.DMA((6,))],
    )
    own = lax.all_to_all(send, PLANE, 0, 0)
    other = swapped(own)
    mix = own[None, :, COLUMNS : COLUMNS + 64, :]
    for flip in (1, 3):
        arrived = lax.ppermute(mix, "dp_0", [(i, i ^ flip) for i in range(4)])
        mix = call(
            join_kernel, shape((2 * mix.shape[0], 16, 64, LANES), bf16), [VMEM] * 2, 1 << 26,
            mix, arrived,
        )
    normed = call(
        norm_kernel, shape((2, rows, 512), bf16), [VMEM, VMEM], 1 << 28,
        tokens_flat, gain_flat,
    )
    decays = (
        up_forward, up_backward, bias_forward.reshape(1, WIDTH), bias_backward.reshape(1, WIDTH)
    )
    payload, rounded = call(
        block_kernel,
        (
            shape((HEADS, 40, LANES), bf16), pltpu.HBM((rows, ALL), bf16),
        ),
        [VMEM] * 7, 1 << 30, normed, own, other, *decays,
    )
    inbound = lax.all_to_all(payload, "sp", 0, 0, axis_index_groups=[GROUP])
    mix_other = swapped(mix)
    states = call(
        scan_kernel, shape((WIDTH, LANES), bf16), [VMEM], 1 << 28,
        inbound,
    )
    returned = lax.all_to_all(
        states.reshape(HEADS, HEAD, LANES), "sp", 0, 0, axis_index_groups=[GROUP]
    )
    parts = call(
        query_kernel, pltpu.HBM((rows, 3 * WIDTH), f32), [VMEM] * 9, 1 << 30,
        in_hbm(tokens_flat), gain_flat, mix, mix_other, in_hbm(rounded), *decays,
    )
    gain = jnp.tile(out_gain.reshape(2, 1, 16), (1, HEADS, 1)).reshape(2, 256)
    mixed = call(
        out_kernel, shape((rows, width), bf16), [VMEM] * 5, 1 << 30,
        returned.reshape(WIDTH, LANES), parts, gain, mix, mix_other,
    )
    return mixed.reshape(seqs, toks, width)


def solution(mesh):
    finer = Mesh(mesh.devices.reshape(mesh.shape["sp"], 4, 4, 2), ("sp", "dp_0", "dp_1", "dp_2"))
    rows = P(DP, None)
    in_specs = (
        P(DP, "sp", None), P(), rows, rows, rows, rows, rows, P(), P(), P(), P(), P(), rows,
    )

    return jax.shard_map(
        body, mesh=finer, in_specs=in_specs, out_specs=P(DP, "sp", None), check_vma=False
    )
```

```python
import jax
import jax.numpy as jnp
from jax import lax
from jax.experimental import pallas as pl
from jax.experimental.pallas import tpu as pltpu
from jax.sharding import Mesh
from jax.sharding import PartitionSpec as P

DP = ("dp_0", "dp_1", "dp_2")
PLANE = ("dp_0", "dp_1")
HEAD = 32
HEADS = 16
WIDTH = 512
BLOCK = 64
LANES = 128
ALL = 2 * WIDTH + LANES
COLUMNS = 8 * 32
SENT = COLUMNS + 32 + 32 + 8
EPS = 1e-06
GROUP = [(z + 12) % 16 for z in range(16)]
PLANE_GROUP = [(i + 15) % 16 for i in range(16)]
f32 = jnp.float32
bf16 = jnp.bfloat16


def dot(a, b):
    return jnp.dot(a, b, preferred_element_type=f32)


def dot_tn(a, b):
    return lax.dot_general(a, b, (((0,), (0,)), ((), ())), preferred_element_type=f32)


def dot_nt(a, b):
    return lax.dot_general(a, b, (((1,), (1,)), ((), ())), preferred_element_type=f32)


def halves(x):
    high = x.astype(bf16)
    return high, (x - high.astype(f32)).astype(bf16)


def grid_of(shape):
    return lax.broadcasted_iota(jnp.int32, shape, 0), lax.broadcasted_iota(jnp.int32, shape, 1)


def as_bf16(mask):
    return jnp.where(mask, 1.0, 0.0).astype(bf16)


def pack_kernel(
    key_hbm, value_hbm, query_hbm, forward_hbm, backward_hbm, mix_hbm,
    out_ref, key_ref, value_ref, query_ref, forward_ref, backward_ref, mix_ref, sems,
):
    sources = (key_hbm, value_hbm, query_hbm, forward_hbm, backward_hbm, mix_hbm)
    targets = (key_ref, value_ref, query_ref, forward_ref, backward_ref, mix_ref)
    copies = [
        pltpu.make_async_copy(source, target, sems.at[i])
        for i, (source, target) in enumerate(zip(sources, targets))
    ]
    for copy in copies:
        copy.start()
    for which, (ref, first) in enumerate(((key_ref, 0), (value_ref, 4))):
        copies[which].wait()
        for i in range(16):
            for group in range(4):
                lanes = slice(group * LANES, (group + 1) * LANES)
                out_ref[i, (first + group) * 32 : (first + group + 1) * 32] = ref[:, lanes]
    for copy in copies[2:]:
        copy.wait()
    row, col = grid_of((16, LANES))
    ranks = dot_tn(forward_ref[...], as_bf16(row == col)) + dot_tn(
        backward_ref[...], as_bf16(row + 16 == col)
    )
    packed = jnp.concatenate([ranks[8 * i : 8 * i + 8, :32] for i in range(4)], axis=1)
    for i, peer in enumerate(PLANE_GROUP):
        start = (peer // 4) * LANES
        out_ref[i, COLUMNS : COLUMNS + 32] = query_ref[:, start : start + LANES]
        out_ref[i, COLUMNS + 32 : COLUMNS + 48] = mix_ref[:, 2 * start : 2 * start + LANES]
        out_ref[i, COLUMNS + 48 : COLUMNS + 64] = mix_ref[:, 2 * start + LANES : 2 * start + 2 * LANES]
        out_ref[i, COLUMNS + 64 :] = packed.astype(bf16)


def join_kernel(first_ref, second_ref, out_ref):
    count = first_ref.shape[0]
    out_ref[:count] = first_ref[...]
    out_ref[count:] = second_ref[...]


def slot_of(index, axis):
    apart = index ^ lax.axis_index(axis)
    return apart ^ (apart >> 1)


def normed_halves(tokens_ref, gain_ref):
    values = tokens_ref[...].astype(f32)
    scale = lax.rsqrt(jnp.mean(values * values, axis=-1, keepdims=True) + EPS)
    normed = (values * scale * gain_ref[...]).astype(bf16)
    return [
        jnp.concatenate(
            [normed[:, (2 * i + core) * 32 : (2 * i + core) * 32 + 32] for i in PLANE_GROUP], axis=1
        )
        for core in range(2)
    ]


def norm_kernel(tokens_ref, gain_ref, normed_ref):
    for core, half in enumerate(normed_halves(tokens_ref, gain_ref)):
        normed_ref[core] = half


def rates_of(ranks, up_forward_ref, up_backward_ref, bias_forward_ref, bias_backward_ref):
    gates = jnp.concatenate(
        [
            dot(ranks[:, :16], up_forward_ref[...]) + bias_forward_ref[...],
            dot(ranks[:, 16:32], up_backward_ref[...]) + bias_backward_ref[...],
        ],
        axis=1,
    )
    log_sigmoid = jnp.minimum(gates, 0.0) - jnp.log1p(jnp.exp(-jnp.abs(gates)))
    return halves(log_sigmoid * (2.0 / (BLOCK * HEADS)))


def summed(parts, mask, way):
    row, col = grid_of((LANES, LANES))
    ones = as_bf16(mask(row, col) & ((row // BLOCK) == (col // BLOCK)))
    lanes = slice(way * WIDTH, (way + 1) * WIDTH)
    return dot(ones, parts[0][:, lanes]) + dot(ones, parts[1][:, lanes])


def block_kernel(
    normed_ref, own_ref, other_ref, up_forward_ref, up_backward_ref,
    bias_forward_ref, bias_backward_ref, payload_ref, rounded_ref,
):
    core = lax.axis_index("dp_2")

    def columns(ref, first):
        return jnp.concatenate(
            [ref[:, g * 32 : (g + 1) * 32, :].reshape(WIDTH, LANES) for g in (first, first + 1)], axis=1
        )

    def rank_columns(ref):
        packed = ref[:, COLUMNS + 64 :, :].astype(f32)
        rows = jnp.stack([packed[:, :, 32 * i : 32 * i + 32] for i in range(4)], axis=1)
        return rows.reshape(WIDTH, 32).astype(bf16)

    mine, theirs = normed_ref[core], normed_ref[1 - core]
    pieces = [
        dot(mine, columns(own_ref, first)) + dot(theirs, columns(other_ref, first))
        for first in (0, 2, 4, 6)
    ]
    pieces.append(dot(mine, rank_columns(own_ref)) + dot(theirs, rank_columns(other_ref)))
    pieces.append(jnp.zeros((2 * BLOCK, LANES - 32), f32))
    rounded = jnp.concatenate(pieces, axis=1).astype(bf16)
    rounded_ref[...] = rounded
    values = rounded[:, WIDTH : 2 * WIDTH]
    parts = rates_of(
        rounded[:, 2 * WIDTH :], up_forward_ref, up_backward_ref, bias_forward_ref, bias_backward_ref
    )
    high, low = parts
    row, col = grid_of((LANES, LANES))
    fwd, bwd = slice(0, WIDTH), slice(WIDTH, 2 * WIDTH)
    keys32 = rounded[:, :WIDTH].astype(f32)
    remain = (
        halves(keys32 * jnp.exp(summed(parts, lambda r, c: c > r, 0))),
        halves(keys32 * jnp.exp(summed(parts, lambda r, c: c < r, 1))),
    )
    hrow, hcol = grid_of((HEADS, WIDTH))
    mine = hrow == hcol // HEAD
    erow, ecol = grid_of((WIDTH, LANES))
    fold = as_bf16(((erow // LANES) * HEAD + erow % HEAD) == ecol)
    srow, scol = grid_of((8, 128))
    pick = as_bf16(srow == scol // BLOCK)
    lines = []
    for span in (fwd, bwd):
        sums = dot(pick, high[:, span]) + dot(pick, low[:, span])
        for seq in range(2):
            line = jnp.where(mine, sums[seq : seq + 1], 0.0)
            lines.append(
                line[:, :LANES] + line[:, LANES : 2 * LANES]
                + line[:, 2 * LANES : 3 * LANES] + line[:, 3 * LANES :]
            )
    close = dot(jnp.concatenate(halves(jnp.concatenate(lines, axis=1)), axis=0), fold)
    tail = lax.broadcasted_iota(jnp.int32, (HEADS, 8, LANES), 1)
    payload_ref[:, HEAD:, :] = jnp.where(
        tail == 0,
        close[:HEADS][:, None, :],
        jnp.where(tail == 1, close[HEADS:][:, None, :], 0.0),
    ).astype(bf16)
    diagonal = (row // HEAD) == (col // HEAD)
    for group in range(4):
        lanes = slice(group * LANES, (group + 1) * LANES)
        parts = []
        for way in range(2):
            for seq in range(2):
                span = slice(seq * BLOCK, (seq + 1) * BLOCK)
                value = values[span, lanes]
                both = jnp.concatenate([half[span, lanes] for half in remain[way]], axis=0)
                state = dot_tn(both, jnp.concatenate([value, value], axis=0))
                parts.append(jnp.where(diagonal, state, 0.0).astype(bf16))
        folded = dot(jnp.concatenate(parts, axis=1), fold).astype(bf16)
        payload_ref[4 * group : 4 * group + 4, :HEAD, :] = folded.reshape(4, HEAD, LANES)


def scan_kernel(payload_ref, out_ref):
    row, col = grid_of((LANES, LANES))
    spread = as_bf16((row // HEAD) == (col // HEAD))
    crow, ccol = grid_of((HEAD, LANES))
    mine = ccol % HEAD == crow
    lines = payload_ref[:, HEAD : HEAD + 8, :].astype(f32)
    closing = 0.0
    for part in range(2):
        line = jnp.where(mine[None], lines[:, part : part + 1, :], 0.0)
        closing = closing + dot(line.astype(bf16).reshape(WIDTH, LANES), spread)
    decay = jnp.exp(closing)
    states = payload_ref[:, :HEAD, :].astype(f32).reshape(WIDTH, LANES)
    lane = lax.broadcasted_iota(jnp.int32, (HEAD, LANES), 1)
    ahead = [None] * HEADS
    behind = [None] * HEADS

    def at(x, i):
        return x[i * HEAD : (i + 1) * HEAD, :]

    carried = jnp.zeros((HEAD, LANES), f32)
    order = [GROUP.index(z) for z in range(HEADS)]
    for i in order:
        ahead[i] = carried
        carried = at(decay, i) * carried + at(states, i)
    carried = jnp.zeros((HEAD, LANES), f32)
    for i in reversed(order):
        behind[i] = carried
        carried = at(decay, i) * carried + at(states, i)
    for i in range(HEADS):
        out_ref[i * HEAD : (i + 1) * HEAD, :] = jnp.where(
            lane < LANES // 2, ahead[i], behind[i]
        ).astype(bf16)


def query_kernel(
    tokens_ref, gain_ref, own_ref, other_ref, rounded_ref, up_forward_ref, up_backward_ref,
    bias_forward_ref, bias_backward_ref, out_ref,
):
    core = lax.axis_index("dp_2")

    def weights(ref):
        return jnp.concatenate(
            [
                ref[slot_of(quarter, "dp_0"), :, :32, :].reshape(WIDTH, LANES)
                for quarter in range(4)
            ],
            axis=1,
        )

    first, second = normed_halves(tokens_ref, gain_ref)
    projected = dot(jnp.where(core == 0, first, second), weights(own_ref)) + dot(
        jnp.where(core == 0, second, first), weights(other_ref)
    )
    queries = projected.astype(bf16).astype(f32) * HEAD ** (-0.5)
    keys = rounded_ref[:, :WIDTH].astype(f32)
    parts = rates_of(
        rounded_ref[:, 2 * WIDTH :], up_forward_ref, up_backward_ref, bias_forward_ref, bias_backward_ref
    )
    decayed, inverse = [], []
    for way, mask in ((0, lambda r, c: c <= r), (1, lambda r, c: c >= r)):
        running = summed(parts, mask, way)
        product = queries * jnp.exp(running)
        out_ref[:, (way + 1) * WIDTH : (way + 2) * WIDTH] = product
        decayed.append(product.astype(bf16))
        inverse.append((keys * jnp.exp(-running)).astype(bf16))
    row, col = grid_of((WIDTH, WIDTH))
    natural = ((col % 256) // 16) * HEAD + (col // 256) * 16 + col % 16
    values = dot(rounded_ref[:, WIDTH : 2 * WIDTH], as_bf16(row == natural)).astype(bf16)
    row, col = grid_of((WIDTH, 256))
    own_lanes = as_bf16((row // BLOCK) == (col // HEAD))
    srow, scol = grid_of((WIDTH, BLOCK))
    lower = (srow % BLOCK) >= scol
    upper = (srow % BLOCK) <= scol
    vrow, vcol = grid_of((WIDTH, LANES))
    own_values = (vrow // BLOCK) == (vcol // 16)
    for seq in range(2):
        span = slice(seq * BLOCK, (seq + 1) * BLOCK)
        for group in range(2):
            wide = slice(group * 256, (group + 1) * 256)
            scores = 0.0
            for way, mask in ((0, lower), (1, upper)):
                stacked = jnp.concatenate([decayed[way][span, wide]] * 8, axis=0) * own_lanes
                scores = scores + jnp.where(mask, dot_nt(stacked, inverse[way][span, wide]), 0.0)
            scores = scores.astype(bf16)
            for half in range(2):
                start = half * 256 + group * LANES
                spread = dot(scores, values[span, start : start + LANES])
                spread = jnp.where(own_values, spread, 0.0)
                total = spread[:BLOCK]
                for head in range(1, 8):
                    total = total + spread[head * BLOCK : (head + 1) * BLOCK]
                out_ref[span, start : start + LANES] = total


def out_kernel(
    states_ref, parts_hbm, gain_ref, own_ref, other_ref, out_ref, parts_ref, sems
):
    spans = [slice(seq * BLOCK, (seq + 1) * BLOCK) for seq in range(2)]
    fetches = [
        pltpu.make_async_copy(parts_hbm.at[span], parts_ref.at[span], sems.at[seq])
        for seq, span in enumerate(spans)
    ]
    for fetch in fetches:
        fetch.start()
    core = lax.axis_index("dp_2")
    row, col = grid_of((LANES, 8 * LANES))
    source = (col // 256) * HEAD + ((col // LANES) % 2) * 16 + col % 16
    widen = as_bf16(row == source)
    row, col = grid_of((256, 8 * LANES))
    diagonal = (row // HEAD) == ((col % LANES) // 16)
    full = [
        jnp.where(diagonal, dot(states_ref[g * 256 : (g + 1) * 256, :], widen), 0.0).astype(bf16)
        for g in range(2)
    ]
    totals = [[], []]
    for seq, span in enumerate(spans):
        fetches[seq].wait()
        sides = [[], []]
        for group in range(2):
            queries = jnp.concatenate(
                [
                    parts_ref[span, (way + 1) * WIDTH + group * 256 : (way + 1) * WIDTH + group * 256 + 256]
                    for way in range(2)
                ],
                axis=1,
            )
            right = jnp.concatenate(
                [full[group][:, (2 * way + seq) * 256 : (2 * way + seq + 1) * 256] for way in range(2)],
                axis=0,
            )
            across = dot(jnp.concatenate(halves(queries), axis=0), right)
            across = across[:BLOCK] + across[BLOCK:]
            for half in range(2):
                start = half * 256 + group * LANES
                sides[half].append(
                    parts_ref[span, start : start + LANES] + across[:, half * LANES : (half + 1) * LANES]
                )
        for half in range(2):
            totals[half].append(jnp.concatenate(sides[half], axis=1))
    combined = [jnp.concatenate(total, axis=0) for total in totals]
    high, low = halves(combined[0] * combined[0] + combined[1] * combined[1])
    row, col = grid_of((256, 256))
    ones = as_bf16((row // 16) == (col // 16))
    scale = lax.rsqrt((dot(high, ones) + dot(low, ones)) * (1.0 / HEAD) + EPS)
    attended = [
        (combined[half] * scale * gain_ref[half : half + 1, :]).astype(bf16) for half in range(2)
    ]
    mine = jnp.where(core == 0, attended[0], attended[1])
    theirs = jnp.where(core == 0, attended[1], attended[0])
    for quarter in range(4):
        slot = slot_of(quarter, "dp_0")

        def weights(ref):
            return jnp.concatenate(
                [
                    jnp.concatenate(
                        [ref[slot, 1:, rows : rows + 16, :], ref[slot, :1, rows : rows + 16, :]], axis=0
                    ).reshape(256, LANES)
                    for rows in (32, 48)
                ],
                axis=1,
            )

        out_ref[:, quarter * 256 : (quarter + 1) * 256] = (
            dot(mine, weights(own_ref)) + dot(theirs, weights(other_ref))
        ).astype(bf16)


VMEM = pl.BlockSpec(memory_space=pltpu.VMEM)


def call(kernel, outs, specs, cycles, *args, scratch=()):
    many = isinstance(outs, tuple)
    return pl.pallas_call(
        kernel,
        out_shape=outs,
        in_specs=specs,
        out_specs=(VMEM,) * len(outs) if many else VMEM,
        scratch_shapes=scratch,
        cost_estimate=pl.CostEstimate(flops=cycles, bytes_accessed=1 << 20, transcendentals=0),
        compiler_params=pltpu.CompilerParams(vmem_limit_bytes=16 << 20),
    )(*args)


def in_hbm(x):
    return pltpu.with_memory_space_constraint(x, pltpu.HBM)


def swapped(x):
    return lax.ppermute(x, "dp_2", [(0, 1), (1, 0)])


def body(
    tokens, norm_gain, w_query, w_key, w_value, w_rank_forward, w_rank_backward,
    up_forward, up_backward, bias_forward, bias_backward, out_gain, w_out,
):
    seqs, toks, width = tokens.shape
    rows = seqs * toks
    shape = jax.ShapeDtypeStruct
    tokens_flat, gain_flat = tokens.reshape(rows, width), norm_gain.reshape(1, width)
    hbm = pl.BlockSpec(memory_space=pltpu.HBM)
    sources = [
        in_hbm(x)
        for x in (w_key, w_value, w_query, w_rank_forward.T, w_rank_backward.T, w_out)
    ]
    send = call(
        pack_kernel, shape((16, SENT, LANES), bf16), [hbm] * 6, 1 << 26, *sources,
        scratch=[pltpu.VMEM(x.shape, bf16) for x in sources] + [pltpu.SemaphoreType.DMA((6,))],
    )
    own = lax.all_to_all(send, PLANE, 0, 0, axis_index_groups=[PLANE_GROUP])
    other = swapped(own)
    mix = own[None, :, COLUMNS : COLUMNS + 64, :]
    for flip in (1, 3):
        arrived = lax.ppermute(mix, "dp_0", [(i, i ^ flip) for i in range(4)])
        mix = call(
            join_kernel, shape((2 * mix.shape[0], 16, 64, LANES), bf16), [VMEM] * 2, 1 << 26,
            mix, arrived,
        )
    normed = call(
        norm_kernel, shape((2, rows, 512), bf16), [VMEM, VMEM], 1 << 28,
        tokens_flat, gain_flat,
    )
    decays = (
        up_forward, up_backward, bias_forward.reshape(1, WIDTH), bias_backward.reshape(1, WIDTH)
    )
    payload, rounded = call(
        block_kernel,
        (
            shape((HEADS, 40, LANES), bf16), pltpu.HBM((rows, ALL), bf16),
        ),
        [VMEM] * 7, 1 << 30, normed, own, other, *decays,
    )
    inbound = lax.all_to_all(payload, "sp", 0, 0, axis_index_groups=[GROUP])
    mix_other = swapped(mix)
    states = call(
        scan_kernel, shape((WIDTH, LANES), bf16), [VMEM], 1 << 28,
        inbound,
    )
    returned = lax.all_to_all(
        states.reshape(HEADS, HEAD, LANES), "sp", 0, 0, axis_index_groups=[GROUP]
    )
    parts = call(
        query_kernel, pltpu.HBM((rows, 3 * WIDTH), f32), [VMEM] * 9, 1 << 30,
        in_hbm(tokens_flat), gain_flat, mix, mix_other, in_hbm(rounded), *decays,
    )
    gain = jnp.tile(out_gain.reshape(2, 1, 16), (1, HEADS, 1)).reshape(2, 256)
    mixed = call(
        out_kernel, shape((rows, width), bf16), [VMEM, hbm] + [VMEM] * 3, 1 << 30,
        returned.reshape(WIDTH, LANES), in_hbm(parts), gain, mix, mix_other,
        scratch=[pltpu.VMEM((rows, 3 * WIDTH), f32), pltpu.SemaphoreType.DMA((2,))],
    )
    return mixed.reshape(seqs, toks, width)


def solution(mesh):
    finer = Mesh(mesh.devices.reshape(mesh.shape["sp"], 4, 4, 2), ("sp", "dp_0", "dp_1", "dp_2"))
    rows = P(DP, None)
    in_specs = (
        P(DP, "sp", None), P(), rows, rows, rows, rows, rows, P(), P(), P(), P(), P(), rows,
    )

    return jax.shard_map(
        body, mesh=finer, in_specs=in_specs, out_specs=P(DP, "sp", None), check_vma=False
    )
```

```python
import jax
import jax.numpy as jnp
from jax import lax
from jax.experimental import pallas as pl
from jax.experimental.pallas import tpu as pltpu
from jax.sharding import Mesh
from jax.sharding import PartitionSpec as P

DP = ("dp_0", "dp_1", "dp_2")
PLANE = ("dp_0", "dp_1")
HEAD = 32
HEADS = 16
WIDTH = 512
BLOCK = 64
LANES = 128
ALL = 2 * WIDTH + LANES
COLUMNS = 8 * 32
SENT = COLUMNS + 32 + 32 + 8
EPS = 1e-06
GROUP = [(z + 12) % 16 for z in range(16)]
PLANE_GROUP = [(i + 15) % 16 for i in range(16)]
f32 = jnp.float32
bf16 = jnp.bfloat16


def dot(a, b):
    return jnp.dot(a, b, preferred_element_type=f32)


def dot_tn(a, b):
    return lax.dot_general(a, b, (((0,), (0,)), ((), ())), preferred_element_type=f32)


def dot_nt(a, b):
    return lax.dot_general(a, b, (((1,), (1,)), ((), ())), preferred_element_type=f32)


def halves(x):
    high = x.astype(bf16)
    return high, (x - high.astype(f32)).astype(bf16)


def grid_of(shape):
    return lax.broadcasted_iota(jnp.int32, shape, 0), lax.broadcasted_iota(jnp.int32, shape, 1)


def as_bf16(mask):
    return jnp.where(mask, 1.0, 0.0).astype(bf16)


def pack_kernel(
    key_hbm, value_hbm, query_hbm, forward_hbm, backward_hbm, mix_hbm,
    out_ref, key_ref, value_ref, query_ref, forward_ref, backward_ref, mix_ref, sems,
):
    sources = (key_hbm, value_hbm, query_hbm, forward_hbm, backward_hbm, mix_hbm)
    targets = (key_ref, value_ref, query_ref, forward_ref, backward_ref, mix_ref)
    copies = [
        pltpu.make_async_copy(source, target, sems.at[i])
        for i, (source, target) in enumerate(zip(sources, targets))
    ]
    for copy in copies:
        copy.start()
    for which, (ref, first) in enumerate(((key_ref, 0), (value_ref, 4))):
        copies[which].wait()
        for i in range(16):
            for group in range(4):
                lanes = slice(group * LANES, (group + 1) * LANES)
                out_ref[i, (first + group) * 32 : (first + group + 1) * 32] = ref[:, lanes]
    for copy in copies[2:]:
        copy.wait()
    row, col = grid_of((16, LANES))
    ranks = dot_tn(forward_ref[...], as_bf16(row == col)) + dot_tn(
        backward_ref[...], as_bf16(row + 16 == col)
    )
    packed = jnp.concatenate([ranks[8 * i : 8 * i + 8, :32] for i in range(4)], axis=1)
    for i, peer in enumerate(PLANE_GROUP):
        start = (peer // 4) * LANES
        out_ref[i, COLUMNS : COLUMNS + 32] = query_ref[:, start : start + LANES]
        out_ref[i, COLUMNS + 32 : COLUMNS + 48] = mix_ref[:, 2 * start : 2 * start + LANES]
        out_ref[i, COLUMNS + 48 : COLUMNS + 64] = mix_ref[:, 2 * start + LANES : 2 * start + 2 * LANES]
        out_ref[i, COLUMNS + 64 :] = packed.astype(bf16)


def join_kernel(first_ref, second_ref, out_ref):
    count = first_ref.shape[0]
    out_ref[:count] = first_ref[...]
    out_ref[count:] = second_ref[...]


def split_kernel(first_ref, second_ref, query_ref, mix_ref):
    for part, ref in enumerate((first_ref, second_ref)):
        query_ref[2 * part : 2 * part + 2] = ref[:, :, :32, :]
        mix_ref[2 * part : 2 * part + 2] = ref[:, :, 32:, :]


def slot_of(index, axis):
    apart = index ^ lax.axis_index(axis)
    return apart ^ (apart >> 1)


def normed_halves(tokens_ref, gain_ref):
    values = tokens_ref[...].astype(f32)
    scale = lax.rsqrt(jnp.mean(values * values, axis=-1, keepdims=True) + EPS)
    normed = (values * scale * gain_ref[...]).astype(bf16)
    return [
        jnp.concatenate(
            [normed[:, (2 * i + core) * 32 : (2 * i + core) * 32 + 32] for i in PLANE_GROUP], axis=1
        )
        for core in range(2)
    ]


def norm_kernel(tokens_ref, gain_ref, normed_ref):
    for core, half in enumerate(normed_halves(tokens_ref, gain_ref)):
        normed_ref[core] = half


def rates_of(ranks, up_forward_ref, up_backward_ref, bias_forward_ref, bias_backward_ref):
    gates = jnp.concatenate(
        [
            dot(ranks[:, :16], up_forward_ref[...]) + bias_forward_ref[...],
            dot(ranks[:, 16:32], up_backward_ref[...]) + bias_backward_ref[...],
        ],
        axis=1,
    )
    log_sigmoid = jnp.minimum(gates, 0.0) - jnp.log1p(jnp.exp(-jnp.abs(gates)))
    return halves(log_sigmoid * (2.0 / (BLOCK * HEADS)))


def summed(parts, mask, way):
    row, col = grid_of((LANES, LANES))
    ones = as_bf16(mask(row, col) & ((row // BLOCK) == (col // BLOCK)))
    lanes = slice(way * WIDTH, (way + 1) * WIDTH)
    return dot(ones, parts[0][:, lanes]) + dot(ones, parts[1][:, lanes])


def block_kernel(
    normed_ref, own_ref, other_ref, up_forward_ref, up_backward_ref,
    bias_forward_ref, bias_backward_ref, payload_ref, rounded_ref,
):
    core = lax.axis_index("dp_2")

    def columns(ref, first):
        return jnp.concatenate(
            [ref[:, g * 32 : (g + 1) * 32, :].reshape(WIDTH, LANES) for g in (first, first + 1)], axis=1
        )

    def rank_columns(ref):
        packed = ref[:, COLUMNS + 64 :, :].astype(f32)
        rows = jnp.stack([packed[:, :, 32 * i : 32 * i + 32] for i in range(4)], axis=1)
        return rows.reshape(WIDTH, 32).astype(bf16)

    mine, theirs = normed_ref[core], normed_ref[1 - core]
    pieces = [
        dot(mine, columns(own_ref, first)) + dot(theirs, columns(other_ref, first))
        for first in (0, 2, 4, 6)
    ]
    pieces.append(dot(mine, rank_columns(own_ref)) + dot(theirs, rank_columns(other_ref)))
    pieces.append(jnp.zeros((2 * BLOCK, LANES - 32), f32))
    rounded = jnp.concatenate(pieces, axis=1).astype(bf16)
    rounded_ref[...] = rounded
    values = rounded[:, WIDTH : 2 * WIDTH]
    parts = rates_of(
        rounded[:, 2 * WIDTH :], up_forward_ref, up_backward_ref, bias_forward_ref, bias_backward_ref
    )
    high, low = parts
    row, col = grid_of((LANES, LANES))
    fwd, bwd = slice(0, WIDTH), slice(WIDTH, 2 * WIDTH)
    keys32 = rounded[:, :WIDTH].astype(f32)
    remain = (
        halves(keys32 * jnp.exp(summed(parts, lambda r, c: c > r, 0))),
        halves(keys32 * jnp.exp(summed(parts, lambda r, c: c < r, 1))),
    )
    hrow, hcol = grid_of((HEADS, WIDTH))
    mine = hrow == hcol // HEAD
    erow, ecol = grid_of((WIDTH, LANES))
    fold = as_bf16(((erow // LANES) * HEAD + erow % HEAD) == ecol)
    srow, scol = grid_of((8, 128))
    pick = as_bf16(srow == scol // BLOCK)
    lines = []
    for span in (fwd, bwd):
        sums = dot(pick, high[:, span]) + dot(pick, low[:, span])
        for seq in range(2):
            line = jnp.where(mine, sums[seq : seq + 1], 0.0)
            lines.append(
                line[:, :LANES] + line[:, LANES : 2 * LANES]
                + line[:, 2 * LANES : 3 * LANES] + line[:, 3 * LANES :]
            )
    close = dot(jnp.concatenate(halves(jnp.concatenate(lines, axis=1)), axis=0), fold)
    tail = lax.broadcasted_iota(jnp.int32, (HEADS, 8, LANES), 1)
    payload_ref[:, HEAD:, :] = jnp.where(
        tail == 0,
        close[:HEADS][:, None, :],
        jnp.where(tail == 1, close[HEADS:][:, None, :], 0.0),
    ).astype(bf16)
    diagonal = (row // HEAD) == (col // HEAD)
    for group in range(4):
        lanes = slice(group * LANES, (group + 1) * LANES)
        parts = []
        for way in range(2):
            for seq in range(2):
                span = slice(seq * BLOCK, (seq + 1) * BLOCK)
                value = values[span, lanes]
                both = jnp.concatenate([half[span, lanes] for half in remain[way]], axis=0)
                state = dot_tn(both, jnp.concatenate([value, value], axis=0))
                parts.append(jnp.where(diagonal, state, 0.0).astype(bf16))
        folded = dot(jnp.concatenate(parts, axis=1), fold).astype(bf16)
        payload_ref[4 * group : 4 * group + 4, :HEAD, :] = folded.reshape(4, HEAD, LANES)


def scan_kernel(payload_ref, out_ref):
    row, col = grid_of((LANES, LANES))
    spread = as_bf16((row // HEAD) == (col // HEAD))
    crow, ccol = grid_of((HEAD, LANES))
    mine = ccol % HEAD == crow
    lines = payload_ref[:, HEAD : HEAD + 8, :].astype(f32)
    closing = 0.0
    for part in range(2):
        line = jnp.where(mine[None], lines[:, part : part + 1, :], 0.0)
        closing = closing + dot(line.astype(bf16).reshape(WIDTH, LANES), spread)
    decay = jnp.exp(closing)
    states = payload_ref[:, :HEAD, :].astype(f32).reshape(WIDTH, LANES)
    lane = lax.broadcasted_iota(jnp.int32, (HEAD, LANES), 1)
    ahead = [None] * HEADS
    behind = [None] * HEADS

    def at(x, i):
        return x[i * HEAD : (i + 1) * HEAD, :]

    carried = jnp.zeros((HEAD, LANES), f32)
    order = [GROUP.index(z) for z in range(HEADS)]
    for i in order:
        ahead[i] = carried
        carried = at(decay, i) * carried + at(states, i)
    carried = jnp.zeros((HEAD, LANES), f32)
    for i in reversed(order):
        behind[i] = carried
        carried = at(decay, i) * carried + at(states, i)
    for i in range(HEADS):
        out_ref[i * HEAD : (i + 1) * HEAD, :] = jnp.where(
            lane < LANES // 2, ahead[i], behind[i]
        ).astype(bf16)


def query_kernel(
    tokens_ref, gain_ref, own_ref, other_ref, rounded_ref, up_forward_ref, up_backward_ref,
    bias_forward_ref, bias_backward_ref, out_ref,
):
    core = lax.axis_index("dp_2")

    def weights(ref):
        return jnp.concatenate(
            [
                ref[slot_of(quarter, "dp_0")].reshape(WIDTH, LANES)
                for quarter in range(4)
            ],
            axis=1,
        )

    first, second = normed_halves(tokens_ref, gain_ref)
    projected = dot(jnp.where(core == 0, first, second), weights(own_ref)) + dot(
        jnp.where(core == 0, second, first), weights(other_ref)
    )
    queries = projected.astype(bf16).astype(f32) * HEAD ** (-0.5)
    keys = rounded_ref[:, :WIDTH].astype(f32)
    parts = rates_of(
        rounded_ref[:, 2 * WIDTH :], up_forward_ref, up_backward_ref, bias_forward_ref, bias_backward_ref
    )
    decayed, inverse = [], []
    for way, mask in ((0, lambda r, c: c <= r), (1, lambda r, c: c >= r)):
        running = summed(parts, mask, way)
        product = queries * jnp.exp(running)
        out_ref[:, (way + 1) * WIDTH : (way + 2) * WIDTH] = product
        decayed.append(product.astype(bf16))
        inverse.append((keys * jnp.exp(-running)).astype(bf16))
    row, col = grid_of((WIDTH, WIDTH))
    natural = ((col % 256) // 16) * HEAD + (col // 256) * 16 + col % 16
    values = dot(rounded_ref[:, WIDTH : 2 * WIDTH], as_bf16(row == natural)).astype(bf16)
    row, col = grid_of((WIDTH, 256))
    own_lanes = as_bf16((row // BLOCK) == (col // HEAD))
    srow, scol = grid_of((WIDTH, BLOCK))
    lower = (srow % BLOCK) >= scol
    upper = (srow % BLOCK) <= scol
    vrow, vcol = grid_of((WIDTH, LANES))
    own_values = (vrow // BLOCK) == (vcol // 16)
    for seq in range(2):
        span = slice(seq * BLOCK, (seq + 1) * BLOCK)
        for group in range(2):
            wide = slice(group * 256, (group + 1) * 256)
            scores = 0.0
            for way, mask in ((0, lower), (1, upper)):
                stacked = jnp.concatenate([decayed[way][span, wide]] * 8, axis=0) * own_lanes
                scores = scores + jnp.where(mask, dot_nt(stacked, inverse[way][span, wide]), 0.0)
            scores = scores.astype(bf16)
            for half in range(2):
                start = half * 256 + group * LANES
                spread = dot(scores, values[span, start : start + LANES])
                spread = jnp.where(own_values, spread, 0.0)
                total = spread[:BLOCK]
                for head in range(1, 8):
                    total = total + spread[head * BLOCK : (head + 1) * BLOCK]
                out_ref[span, start : start + LANES] = total


def out_kernel(
    states_ref, parts_ref, gain_ref, own_hbm, other_ref, out_ref, own_ref, sem
):
    fetch = pltpu.make_async_copy(own_hbm, own_ref, sem)
    fetch.start()
    spans = [slice(seq * BLOCK, (seq + 1) * BLOCK) for seq in range(2)]
    core = lax.axis_index("dp_2")
    row, col = grid_of((LANES, 8 * LANES))
    source = (col // 256) * HEAD + ((col // LANES) % 2) * 16 + col % 16
    widen = as_bf16(row == source)
    row, col = grid_of((256, 8 * LANES))
    diagonal = (row // HEAD) == ((col % LANES) // 16)
    full = [
        jnp.where(diagonal, dot(states_ref[g * 256 : (g + 1) * 256, :], widen), 0.0).astype(bf16)
        for g in range(2)
    ]
    totals = [[], []]
    for seq, span in enumerate(spans):
        sides = [[], []]
        for group in range(2):
            queries = jnp.concatenate(
                [
                    parts_ref[span, (way + 1) * WIDTH + group * 256 : (way + 1) * WIDTH + group * 256 + 256]
                    for way in range(2)
                ],
                axis=1,
            )
            right = jnp.concatenate(
                [full[group][:, (2 * way + seq) * 256 : (2 * way + seq + 1) * 256] for way in range(2)],
                axis=0,
            )
            across = dot(jnp.concatenate(halves(queries), axis=0), right)
            across = across[:BLOCK] + across[BLOCK:]
            for half in range(2):
                start = half * 256 + group * LANES
                sides[half].append(
                    parts_ref[span, start : start + LANES] + across[:, half * LANES : (half + 1) * LANES]
                )
        for half in range(2):
            totals[half].append(jnp.concatenate(sides[half], axis=1))
    combined = [jnp.concatenate(total, axis=0) for total in totals]
    high, low = halves(combined[0] * combined[0] + combined[1] * combined[1])
    row, col = grid_of((256, 256))
    ones = as_bf16((row // 16) == (col // 16))
    scale = lax.rsqrt((dot(high, ones) + dot(low, ones)) * (1.0 / HEAD) + EPS)
    attended = [
        (combined[half] * scale * gain_ref[half : half + 1, :]).astype(bf16) for half in range(2)
    ]
    mine = jnp.where(core == 0, attended[0], attended[1])
    theirs = jnp.where(core == 0, attended[1], attended[0])
    fetch.wait()
    for quarter in range(4):
        slot = slot_of(quarter, "dp_0")

        def weights(ref):
            return jnp.concatenate(
                [
                    jnp.concatenate(
                        [ref[slot, 1:, rows : rows + 16, :], ref[slot, :1, rows : rows + 16, :]], axis=0
                    ).reshape(256, LANES)
                    for rows in (0, 16)
                ],
                axis=1,
            )

        out_ref[:, quarter * 256 : (quarter + 1) * 256] = (
            dot(mine, weights(own_ref)) + dot(theirs, weights(other_ref))
        ).astype(bf16)


VMEM = pl.BlockSpec(memory_space=pltpu.VMEM)


def call(kernel, outs, specs, cycles, *args, scratch=()):
    many = isinstance(outs, tuple)
    return pl.pallas_call(
        kernel,
        out_shape=outs,
        in_specs=specs,
        out_specs=(VMEM,) * len(outs) if many else VMEM,
        scratch_shapes=scratch,
        cost_estimate=pl.CostEstimate(flops=cycles, bytes_accessed=1 << 20, transcendentals=0),
        compiler_params=pltpu.CompilerParams(vmem_limit_bytes=16 << 20),
    )(*args)


def in_hbm(x):
    return pltpu.with_memory_space_constraint(x, pltpu.HBM)


def swapped(x):
    return lax.ppermute(x, "dp_2", [(0, 1), (1, 0)])


def body(
    tokens, norm_gain, w_query, w_key, w_value, w_rank_forward, w_rank_backward,
    up_forward, up_backward, bias_forward, bias_backward, out_gain, w_out,
):
    seqs, toks, width = tokens.shape
    rows = seqs * toks
    shape = jax.ShapeDtypeStruct
    tokens_flat, gain_flat = tokens.reshape(rows, width), norm_gain.reshape(1, width)
    hbm = pl.BlockSpec(memory_space=pltpu.HBM)
    sources = [
        in_hbm(x)
        for x in (w_key, w_value, w_query, w_rank_forward.T, w_rank_backward.T, w_out)
    ]
    send = call(
        pack_kernel, shape((16, SENT, LANES), bf16), [hbm] * 6, 1 << 26, *sources,
        scratch=[pltpu.VMEM(x.shape, bf16) for x in sources] + [pltpu.SemaphoreType.DMA((6,))],
    )
    own = lax.all_to_all(send, PLANE, 0, 0, axis_index_groups=[PLANE_GROUP])
    other = swapped(own)
    mix = own[None, :, COLUMNS : COLUMNS + 64, :]
    for step, flip in enumerate((1, 3)):
        arrived = lax.ppermute(mix, "dp_0", [(i, i ^ flip) for i in range(4)])
        if step == 0:
            mix = call(
                join_kernel, shape((2, 16, 64, LANES), bf16), [VMEM] * 2, 1 << 26, mix, arrived
            )
        else:
            query, mix = call(
                split_kernel,
                (shape((4, 16, 32, LANES), bf16), pltpu.HBM((4, 16, 32, LANES), bf16)),
                [VMEM] * 2, 1 << 26,
                mix, arrived,
            )
    normed = call(
        norm_kernel, shape((2, rows, 512), bf16), [VMEM, VMEM], 1 << 28,
        tokens_flat, gain_flat,
    )
    decays = (
        up_forward, up_backward, bias_forward.reshape(1, WIDTH), bias_backward.reshape(1, WIDTH)
    )
    payload, rounded = call(
        block_kernel,
        (
            shape((HEADS, 40, LANES), bf16), pltpu.HBM((rows, ALL), bf16),
        ),
        [VMEM] * 7, 1 << 30, normed, own, other, *decays,
    )
    inbound = lax.all_to_all(payload, "sp", 0, 0, axis_index_groups=[GROUP])
    query_other = swapped(query)
    mix_other = swapped(mix)
    states = call(
        scan_kernel, shape((WIDTH, LANES), bf16), [VMEM], 1 << 28,
        inbound,
    )
    returned = lax.all_to_all(
        states.reshape(HEADS, HEAD, LANES), "sp", 0, 0, axis_index_groups=[GROUP]
    )
    parts = call(
        query_kernel, shape((rows, 3 * WIDTH), f32), [VMEM] * 9, 1 << 30,
        in_hbm(tokens_flat), gain_flat, query, query_other, in_hbm(rounded), *decays,
    )
    gain = jnp.tile(out_gain.reshape(2, 1, 16), (1, HEADS, 1)).reshape(2, 256)
    mixed = call(
        out_kernel, shape((rows, width), bf16), [VMEM] * 3 + [hbm, VMEM], 1 << 30,
        returned.reshape(WIDTH, LANES), parts, gain, in_hbm(mix), mix_other,
        scratch=[pltpu.VMEM((4, 16, 32, LANES), bf16), pltpu.SemaphoreType.DMA],
    )
    return mixed.reshape(seqs, toks, width)


def solution(mesh):
    finer = Mesh(mesh.devices.reshape(mesh.shape["sp"], 4, 4, 2), ("sp", "dp_0", "dp_1", "dp_2"))
    rows = P(DP, None)
    in_specs = (
        P(DP, "sp", None), P(), rows, rows, rows, rows, rows, P(), P(), P(), P(), P(), rows,
    )

    return jax.shard_map(
        body, mesh=finer, in_specs=in_specs, out_specs=P(DP, "sp", None), check_vma=False
    )
```

```python
import jax
import jax.numpy as jnp
from jax import lax
from jax.experimental import pallas as pl
from jax.experimental.pallas import tpu as pltpu
from jax.sharding import Mesh
from jax.sharding import PartitionSpec as P

DP = ("dp_0", "dp_1", "dp_2")
PLANE = ("dp_0", "dp_1")
HEAD = 32
HEADS = 16
WIDTH = 512
BLOCK = 64
LANES = 128
ALL = 2 * WIDTH + LANES
COLUMNS = 8 * 32
SENT = COLUMNS + 32 + 32 + 8
EPS = 1e-06
GROUP = [(z + 12) % 16 for z in range(16)]
PLANE_GROUP = [(i + 15) % 16 for i in range(16)]
f32 = jnp.float32
bf16 = jnp.bfloat16


def dot(a, b):
    return jnp.dot(a, b, preferred_element_type=f32)


def dot_tn(a, b):
    return lax.dot_general(a, b, (((0,), (0,)), ((), ())), preferred_element_type=f32)


def dot_nt(a, b):
    return lax.dot_general(a, b, (((1,), (1,)), ((), ())), preferred_element_type=f32)


def halves(x):
    high = x.astype(bf16)
    return high, (x - high.astype(f32)).astype(bf16)


def grid_of(shape):
    return lax.broadcasted_iota(jnp.int32, shape, 0), lax.broadcasted_iota(jnp.int32, shape, 1)


def as_bf16(mask):
    return jnp.where(mask, 1.0, 0.0).astype(bf16)


def pack_kernel(
    key_hbm, value_hbm, query_hbm, forward_hbm, backward_hbm, mix_hbm,
    out_ref, key_ref, value_ref, query_ref, forward_ref, backward_ref, mix_ref, sems,
):
    sources = (key_hbm, value_hbm, query_hbm, forward_hbm, backward_hbm, mix_hbm)
    targets = (key_ref, value_ref, query_ref, forward_ref, backward_ref, mix_ref)
    copies = [
        pltpu.make_async_copy(source, target, sems.at[i])
        for i, (source, target) in enumerate(zip(sources, targets))
    ]
    for copy in copies:
        copy.start()
    for which, (ref, first) in enumerate(((key_ref, 0), (value_ref, 4))):
        copies[which].wait()
        for i in range(16):
            for group in range(4):
                lanes = slice(group * LANES, (group + 1) * LANES)
                out_ref[i, (first + group) * 32 : (first + group + 1) * 32] = ref[:, lanes]
    for copy in copies[2:]:
        copy.wait()
    row, col = grid_of((16, LANES))
    ranks = dot_tn(forward_ref[...], as_bf16(row == col)) + dot_tn(
        backward_ref[...], as_bf16(row + 16 == col)
    )
    packed = jnp.concatenate([ranks[8 * i : 8 * i + 8, :32] for i in range(4)], axis=1)
    for i, peer in enumerate(PLANE_GROUP):
        start = (peer // 4) * LANES
        out_ref[i, COLUMNS : COLUMNS + 32] = query_ref[:, start : start + LANES]
        out_ref[i, COLUMNS + 32 : COLUMNS + 48] = mix_ref[:, 2 * start : 2 * start + LANES]
        out_ref[i, COLUMNS + 48 : COLUMNS + 64] = mix_ref[:, 2 * start + LANES : 2 * start + 2 * LANES]
        out_ref[i, COLUMNS + 64 :] = packed.astype(bf16)


def join_kernel(first_ref, second_ref, out_ref):
    count = first_ref.shape[0]
    out_ref[:count] = first_ref[...]
    out_ref[count:] = second_ref[...]


def split_kernel(first_ref, second_ref, query_ref, mix_ref):
    for part, ref in enumerate((first_ref, second_ref)):
        query_ref[2 * part : 2 * part + 2] = ref[:, :, :32, :]
        mix_ref[2 * part : 2 * part + 2] = ref[:, :, 32:, :]


def slot_of(index, axis):
    apart = index ^ lax.axis_index(axis)
    return apart ^ (apart >> 1)


def normed_halves(tokens_ref, gain_ref):
    values = tokens_ref[...].astype(f32)
    scale = lax.rsqrt(jnp.mean(values * values, axis=-1, keepdims=True) + EPS)
    normed = (values * scale * gain_ref[...]).astype(bf16)
    return [
        jnp.concatenate(
            [normed[:, (2 * i + core) * 32 : (2 * i + core) * 32 + 32] for i in PLANE_GROUP], axis=1
        )
        for core in range(2)
    ]


def norm_kernel(tokens_ref, gain_ref, normed_ref):
    for core, half in enumerate(normed_halves(tokens_ref, gain_ref)):
        normed_ref[core] = half


def rates_of(ranks, up_forward_ref, up_backward_ref, bias_forward_ref, bias_backward_ref):
    gates = jnp.concatenate(
        [
            dot(ranks[:, :16], up_forward_ref[...]) + bias_forward_ref[...],
            dot(ranks[:, 16:32], up_backward_ref[...]) + bias_backward_ref[...],
        ],
        axis=1,
    )
    log_sigmoid = jnp.minimum(gates, 0.0) - jnp.log1p(jnp.exp(-jnp.abs(gates)))
    return halves(log_sigmoid * (2.0 / (BLOCK * HEADS)))


def summed(parts, mask, way):
    row, col = grid_of((LANES, LANES))
    ones = as_bf16(mask(row, col) & ((row // BLOCK) == (col // BLOCK)))
    lanes = slice(way * WIDTH, (way + 1) * WIDTH)
    return dot(ones, parts[0][:, lanes]) + dot(ones, parts[1][:, lanes])


def block_kernel(
    normed_ref, own_ref, other_ref, up_forward_ref, up_backward_ref,
    bias_forward_ref, bias_backward_ref, payload_ref, rounded_ref,
):
    core = lax.axis_index("dp_2")

    def columns(ref, first):
        return jnp.concatenate(
            [ref[:, g * 32 : (g + 1) * 32, :].reshape(WIDTH, LANES) for g in (first, first + 1)], axis=1
        )

    def rank_columns(ref):
        packed = ref[:, COLUMNS + 64 :, :].astype(f32)
        rows = jnp.stack([packed[:, :, 32 * i : 32 * i + 32] for i in range(4)], axis=1)
        return rows.reshape(WIDTH, 32).astype(bf16)

    mine, theirs = normed_ref[core], normed_ref[1 - core]
    pieces = [
        dot(mine, columns(own_ref, first)) + dot(theirs, columns(other_ref, first))
        for first in (0, 2, 4, 6)
    ]
    pieces.append(dot(mine, rank_columns(own_ref)) + dot(theirs, rank_columns(other_ref)))
    pieces.append(jnp.zeros((2 * BLOCK, LANES - 32), f32))
    rounded = jnp.concatenate(pieces, axis=1).astype(bf16)
    rounded_ref[...] = rounded
    values = rounded[:, WIDTH : 2 * WIDTH]
    parts = rates_of(
        rounded[:, 2 * WIDTH :], up_forward_ref, up_backward_ref, bias_forward_ref, bias_backward_ref
    )
    high, low = parts
    row, col = grid_of((LANES, LANES))
    fwd, bwd = slice(0, WIDTH), slice(WIDTH, 2 * WIDTH)
    keys32 = rounded[:, :WIDTH].astype(f32)
    remain = (
        halves(keys32 * jnp.exp(summed(parts, lambda r, c: c > r, 0))),
        halves(keys32 * jnp.exp(summed(parts, lambda r, c: c < r, 1))),
    )
    hrow, hcol = grid_of((HEADS, WIDTH))
    mine = hrow == hcol // HEAD
    erow, ecol = grid_of((WIDTH, LANES))
    fold = as_bf16(((erow // LANES) * HEAD + erow % HEAD) == ecol)
    srow, scol = grid_of((8, 128))
    pick = as_bf16(srow == scol // BLOCK)
    lines = []
    for span in (fwd, bwd):
        sums = dot(pick, high[:, span]) + dot(pick, low[:, span])
        for seq in range(2):
            line = jnp.where(mine, sums[seq : seq + 1], 0.0)
            lines.append(
                line[:, :LANES] + line[:, LANES : 2 * LANES]
                + line[:, 2 * LANES : 3 * LANES] + line[:, 3 * LANES :]
            )
    close = dot(jnp.concatenate(halves(jnp.concatenate(lines, axis=1)), axis=0), fold)
    tail = lax.broadcasted_iota(jnp.int32, (HEADS, 8, LANES), 1)
    payload_ref[:, HEAD:, :] = jnp.where(
        tail == 0,
        close[:HEADS][:, None, :],
        jnp.where(tail == 1, close[HEADS:][:, None, :], 0.0),
    ).astype(bf16)
    diagonal = (row // HEAD) == (col // HEAD)
    for group in range(4):
        lanes = slice(group * LANES, (group + 1) * LANES)
        parts = []
        for way in range(2):
            for seq in range(2):
                span = slice(seq * BLOCK, (seq + 1) * BLOCK)
                value = values[span, lanes]
                both = jnp.concatenate([half[span, lanes] for half in remain[way]], axis=0)
                state = dot_tn(both, jnp.concatenate([value, value], axis=0))
                parts.append(jnp.where(diagonal, state, 0.0).astype(bf16))
        folded = dot(jnp.concatenate(parts, axis=1), fold).astype(bf16)
        payload_ref[4 * group : 4 * group + 4, :HEAD, :] = folded.reshape(4, HEAD, LANES)


def scan_kernel(payload_ref, out_ref):
    row, col = grid_of((LANES, LANES))
    spread = as_bf16((row // HEAD) == (col // HEAD))
    crow, ccol = grid_of((HEAD, LANES))
    mine = ccol % HEAD == crow
    lines = payload_ref[:, HEAD : HEAD + 8, :].astype(f32)
    closing = 0.0
    for part in range(2):
        line = jnp.where(mine[None], lines[:, part : part + 1, :], 0.0)
        closing = closing + dot(line.astype(bf16).reshape(WIDTH, LANES), spread)
    decay = jnp.exp(closing)
    states = payload_ref[:, :HEAD, :].astype(f32).reshape(WIDTH, LANES)
    lane = lax.broadcasted_iota(jnp.int32, (HEAD, LANES), 1)
    ahead = [None] * HEADS
    behind = [None] * HEADS

    def at(x, i):
        return x[i * HEAD : (i + 1) * HEAD, :]

    carried = jnp.zeros((HEAD, LANES), f32)
    order = [GROUP.index(z) for z in range(HEADS)]
    for i in order:
        ahead[i] = carried
        carried = at(decay, i) * carried + at(states, i)
    carried = jnp.zeros((HEAD, LANES), f32)
    for i in reversed(order):
        behind[i] = carried
        carried = at(decay, i) * carried + at(states, i)
    for i in range(HEADS):
        out_ref[i * HEAD : (i + 1) * HEAD, :] = jnp.where(
            lane < LANES // 2, ahead[i], behind[i]
        ).astype(bf16)


def query_kernel(
    tokens_ref, gain_ref, own_ref, other_ref, rounded_ref, up_forward_ref, up_backward_ref,
    bias_forward_ref, bias_backward_ref, out_ref,
):
    core = lax.axis_index("dp_2")

    def weights(ref):
        return jnp.concatenate(
            [
                ref[slot_of(quarter, "dp_0")].reshape(WIDTH, LANES)
                for quarter in range(4)
            ],
            axis=1,
        )

    first, second = normed_halves(tokens_ref, gain_ref)
    projected = dot(jnp.where(core == 0, first, second), weights(own_ref)) + dot(
        jnp.where(core == 0, second, first), weights(other_ref)
    )
    queries = projected.astype(bf16).astype(f32) * HEAD ** (-0.5)
    keys = rounded_ref[:, :WIDTH].astype(f32)
    parts = rates_of(
        rounded_ref[:, 2 * WIDTH :], up_forward_ref, up_backward_ref, bias_forward_ref, bias_backward_ref
    )
    decayed, inverse = [], []
    for way, mask in ((0, lambda r, c: c <= r), (1, lambda r, c: c >= r)):
        running = summed(parts, mask, way)
        product = queries * jnp.exp(running)
        out_ref[:, (way + 1) * WIDTH : (way + 2) * WIDTH] = product
        decayed.append(product.astype(bf16))
        inverse.append((keys * jnp.exp(-running)).astype(bf16))
    row, col = grid_of((WIDTH, WIDTH))
    natural = ((col % 256) // 16) * HEAD + (col // 256) * 16 + col % 16
    values = dot(rounded_ref[:, WIDTH : 2 * WIDTH], as_bf16(row == natural)).astype(bf16)
    row, col = grid_of((WIDTH, 256))
    own_lanes = as_bf16((row // BLOCK) == (col // HEAD))
    srow, scol = grid_of((WIDTH, BLOCK))
    lower = (srow % BLOCK) >= scol
    upper = (srow % BLOCK) <= scol
    vrow, vcol = grid_of((WIDTH, LANES))
    own_values = (vrow // BLOCK) == (vcol // 16)
    for seq in range(2):
        span = slice(seq * BLOCK, (seq + 1) * BLOCK)
        for group in range(2):
            wide = slice(group * 256, (group + 1) * 256)
            scores = 0.0
            for way, mask in ((0, lower), (1, upper)):
                stacked = jnp.concatenate([decayed[way][span, wide]] * 8, axis=0) * own_lanes
                scores = scores + jnp.where(mask, dot_nt(stacked, inverse[way][span, wide]), 0.0)
            scores = scores.astype(bf16)
            for half in range(2):
                start = half * 256 + group * LANES
                spread = dot(scores, values[span, start : start + LANES])
                spread = jnp.where(own_values, spread, 0.0)
                total = spread[:BLOCK]
                for head in range(1, 8):
                    total = total + spread[head * BLOCK : (head + 1) * BLOCK]
                out_ref[span, start : start + LANES] = total


def out_kernel(
    states_ref, parts_ref, gain_ref, own_ref, other_ref, out_ref
):
    spans = [slice(seq * BLOCK, (seq + 1) * BLOCK) for seq in range(2)]
    core = lax.axis_index("dp_2")
    row, col = grid_of((LANES, 8 * LANES))
    source = (col // 256) * HEAD + ((col // LANES) % 2) * 16 + col % 16
    widen = as_bf16(row == source)
    row, col = grid_of((256, 8 * LANES))
    diagonal = (row // HEAD) == ((col % LANES) // 16)
    full = [
        jnp.where(diagonal, dot(states_ref[g * 256 : (g + 1) * 256, :], widen), 0.0).astype(bf16)
        for g in range(2)
    ]
    totals = [[], []]
    for seq, span in enumerate(spans):
        sides = [[], []]
        for group in range(2):
            queries = jnp.concatenate(
                [
                    parts_ref[span, (way + 1) * WIDTH + group * 256 : (way + 1) * WIDTH + group * 256 + 256]
                    for way in range(2)
                ],
                axis=1,
            )
            right = jnp.concatenate(
                [full[group][:, (2 * way + seq) * 256 : (2 * way + seq + 1) * 256] for way in range(2)],
                axis=0,
            )
            across = dot(jnp.concatenate(halves(queries), axis=0), right)
            across = across[:BLOCK] + across[BLOCK:]
            for half in range(2):
                start = half * 256 + group * LANES
                sides[half].append(
                    parts_ref[span, start : start + LANES] + across[:, half * LANES : (half + 1) * LANES]
                )
        for half in range(2):
            totals[half].append(jnp.concatenate(sides[half], axis=1))
    combined = [jnp.concatenate(total, axis=0) for total in totals]
    high, low = halves(combined[0] * combined[0] + combined[1] * combined[1])
    row, col = grid_of((256, 256))
    ones = as_bf16((row // 16) == (col // 16))
    scale = lax.rsqrt((dot(high, ones) + dot(low, ones)) * (1.0 / HEAD) + EPS)
    attended = [
        (combined[half] * scale * gain_ref[half : half + 1, :]).astype(bf16) for half in range(2)
    ]
    mine = jnp.where(core == 0, attended[0], attended[1])
    theirs = jnp.where(core == 0, attended[1], attended[0])
    for quarter in range(4):
        slot = slot_of(quarter, "dp_0")

        def weights(ref):
            return jnp.concatenate(
                [
                    jnp.concatenate(
                        [ref[slot, 1:, rows : rows + 16, :], ref[slot, :1, rows : rows + 16, :]], axis=0
                    ).reshape(256, LANES)
                    for rows in (0, 16)
                ],
                axis=1,
            )

        out_ref[:, quarter * 256 : (quarter + 1) * 256] = (
            dot(mine, weights(own_ref)) + dot(theirs, weights(other_ref))
        ).astype(bf16)


VMEM = pl.BlockSpec(memory_space=pltpu.VMEM)


def call(kernel, outs, specs, cycles, *args, scratch=()):
    many = isinstance(outs, tuple)
    return pl.pallas_call(
        kernel,
        out_shape=outs,
        in_specs=specs,
        out_specs=(VMEM,) * len(outs) if many else VMEM,
        scratch_shapes=scratch,
        cost_estimate=pl.CostEstimate(flops=cycles, bytes_accessed=1 << 20, transcendentals=0),
        compiler_params=pltpu.CompilerParams(vmem_limit_bytes=16 << 20),
    )(*args)


def in_hbm(x):
    return pltpu.with_memory_space_constraint(x, pltpu.HBM)


def swapped(x):
    return lax.ppermute(x, "dp_2", [(0, 1), (1, 0)])


def body(
    tokens, norm_gain, w_query, w_key, w_value, w_rank_forward, w_rank_backward,
    up_forward, up_backward, bias_forward, bias_backward, out_gain, w_out,
):
    seqs, toks, width = tokens.shape
    rows = seqs * toks
    shape = jax.ShapeDtypeStruct
    tokens_flat, gain_flat = tokens.reshape(rows, width), norm_gain.reshape(1, width)
    hbm = pl.BlockSpec(memory_space=pltpu.HBM)
    sources = [
        in_hbm(x)
        for x in (w_key, w_value, w_query, w_rank_forward.T, w_rank_backward.T, w_out)
    ]
    send = call(
        pack_kernel, shape((16, SENT, LANES), bf16), [hbm] * 6, 1 << 26, *sources,
        scratch=[pltpu.VMEM(x.shape, bf16) for x in sources] + [pltpu.SemaphoreType.DMA((6,))],
    )
    own = lax.all_to_all(send, PLANE, 0, 0, axis_index_groups=[PLANE_GROUP])
    other = swapped(own)
    mix = own[None, :, COLUMNS : COLUMNS + 64, :]
    for step, flip in enumerate((1, 3)):
        arrived = lax.ppermute(mix, "dp_0", [(i, i ^ flip) for i in range(4)])
        if step == 0:
            mix = call(
                join_kernel, shape((2, 16, 64, LANES), bf16), [VMEM] * 2, 1 << 26, mix, arrived
            )
        else:
            query, mix = call(
                split_kernel,
                (pltpu.HBM((4, 16, 32, LANES), bf16), shape((4, 16, 32, LANES), bf16)),
                [VMEM] * 2, 1 << 26,
                mix, arrived,
            )
    normed = call(
        norm_kernel, shape((2, rows, 512), bf16), [VMEM, VMEM], 1 << 28,
        tokens_flat, gain_flat,
    )
    decays = (
        up_forward, up_backward, bias_forward.reshape(1, WIDTH), bias_backward.reshape(1, WIDTH)
    )
    payload, rounded = call(
        block_kernel,
        (
            shape((HEADS, 40, LANES), bf16), pltpu.HBM((rows, ALL), bf16),
        ),
        [VMEM] * 7, 1 << 30, normed, own, other, *decays,
    )
    inbound = lax.all_to_all(payload, "sp", 0, 0, axis_index_groups=[GROUP])
    query_other = swapped(query)
    mix_other = swapped(mix)
    states = call(
        scan_kernel, shape((WIDTH, LANES), bf16), [VMEM], 1 << 28,
        inbound,
    )
    returned = lax.all_to_all(
        states.reshape(HEADS, HEAD, LANES), "sp", 0, 0, axis_index_groups=[GROUP]
    )
    parts = call(
        query_kernel, shape((rows, 3 * WIDTH), f32), [VMEM] * 9, 1 << 30,
        in_hbm(tokens_flat), gain_flat, query, query_other, in_hbm(rounded), *decays,
    )
    gain = jnp.tile(out_gain.reshape(2, 1, 16), (1, HEADS, 1)).reshape(2, 256)
    mixed = call(
        out_kernel, shape((rows, width), bf16), [VMEM] * 5, 1 << 30,
        returned.reshape(WIDTH, LANES), parts, gain, mix, mix_other,
    )
    return mixed.reshape(seqs, toks, width)


def solution(mesh):
    finer = Mesh(mesh.devices.reshape(mesh.shape["sp"], 4, 4, 2), ("sp", "dp_0", "dp_1", "dp_2"))
    rows = P(DP, None)
    in_specs = (
        P(DP, "sp", None), P(), rows, rows, rows, rows, rows, P(), P(), P(), P(), P(), rows,
    )

    return jax.shard_map(
        body, mesh=finer, in_specs=in_specs, out_specs=P(DP, "sp", None), check_vma=False
    )
```

```python
import jax
import jax.numpy as jnp
from jax import lax
from jax.experimental import pallas as pl
from jax.experimental.pallas import tpu as pltpu
from jax.sharding import Mesh
from jax.sharding import PartitionSpec as P

DP = ("dp_0", "dp_1", "dp_2")
PLANE = ("dp_0", "dp_1")
HEAD = 32
HEADS = 16
WIDTH = 512
BLOCK = 64
LANES = 128
ALL = 2 * WIDTH + LANES
COLUMNS = 8 * 32
SENT = COLUMNS + 32 + 32 + 8
EPS = 1e-06
GROUP = [(z + 12) % 16 for z in range(16)]
RETURN_GROUP = [(z + 14) % 16 for z in range(16)]
PLANE_GROUP = [(i + 15) % 16 for i in range(16)]
f32 = jnp.float32
bf16 = jnp.bfloat16


def dot(a, b):
    return jnp.dot(a, b, preferred_element_type=f32)


def dot_tn(a, b):
    return lax.dot_general(a, b, (((0,), (0,)), ((), ())), preferred_element_type=f32)


def dot_nt(a, b):
    return lax.dot_general(a, b, (((1,), (1,)), ((), ())), preferred_element_type=f32)


def halves(x):
    high = x.astype(bf16)
    return high, (x - high.astype(f32)).astype(bf16)


def grid_of(shape):
    return lax.broadcasted_iota(jnp.int32, shape, 0), lax.broadcasted_iota(jnp.int32, shape, 1)


def as_bf16(mask):
    return jnp.where(mask, 1.0, 0.0).astype(bf16)


def pack_kernel(
    key_hbm, value_hbm, query_hbm, forward_hbm, backward_hbm, mix_hbm,
    out_ref, key_ref, value_ref, query_ref, forward_ref, backward_ref, mix_ref, sems,
):
    sources = (key_hbm, value_hbm, query_hbm, forward_hbm, backward_hbm, mix_hbm)
    targets = (key_ref, value_ref, query_ref, forward_ref, backward_ref, mix_ref)
    copies = [
        pltpu.make_async_copy(source, target, sems.at[i])
        for i, (source, target) in enumerate(zip(sources, targets))
    ]
    for copy in copies:
        copy.start()
    for which, (ref, first) in enumerate(((key_ref, 0), (value_ref, 4))):
        copies[which].wait()
        for i in range(16):
            for group in range(4):
                lanes = slice(group * LANES, (group + 1) * LANES)
                out_ref[i, (first + group) * 32 : (first + group + 1) * 32] = ref[:, lanes]
    for copy in copies[2:]:
        copy.wait()
    row, col = grid_of((16, LANES))
    ranks = dot_tn(forward_ref[...], as_bf16(row == col)) + dot_tn(
        backward_ref[...], as_bf16(row + 16 == col)
    )
    packed = jnp.concatenate([ranks[8 * i : 8 * i + 8, :32] for i in range(4)], axis=1)
    for i, peer in enumerate(PLANE_GROUP):
        start = (peer // 4) * LANES
        out_ref[i, COLUMNS : COLUMNS + 32] = query_ref[:, start : start + LANES]
        out_ref[i, COLUMNS + 32 : COLUMNS + 48] = mix_ref[:, 2 * start : 2 * start + LANES]
        out_ref[i, COLUMNS + 48 : COLUMNS + 64] = mix_ref[:, 2 * start + LANES : 2 * start + 2 * LANES]
        out_ref[i, COLUMNS + 64 :] = packed.astype(bf16)


def join_kernel(first_ref, second_ref, out_ref):
    count = first_ref.shape[0]
    out_ref[:count] = first_ref[...]
    out_ref[count:] = second_ref[...]


def split_kernel(first_ref, second_ref, query_ref, mix_ref):
    for part, ref in enumerate((first_ref, second_ref)):
        query_ref[2 * part : 2 * part + 2] = ref[:, :, :32, :]
        mix_ref[2 * part : 2 * part + 2] = ref[:, :, 32:, :]


def slot_of(index, axis):
    apart = index ^ lax.axis_index(axis)
    return apart ^ (apart >> 1)


def normed_halves(tokens_ref, gain_ref):
    values = tokens_ref[...].astype(f32)
    scale = lax.rsqrt(jnp.mean(values * values, axis=-1, keepdims=True) + EPS)
    normed = (values * scale * gain_ref[...]).astype(bf16)
    return [
        jnp.concatenate(
            [normed[:, (2 * i + core) * 32 : (2 * i + core) * 32 + 32] for i in PLANE_GROUP], axis=1
        )
        for core in range(2)
    ]


def norm_kernel(tokens_ref, gain_ref, normed_ref):
    for core, half in enumerate(normed_halves(tokens_ref, gain_ref)):
        normed_ref[core] = half


def rates_of(ranks, up_forward_ref, up_backward_ref, bias_forward_ref, bias_backward_ref):
    gates = jnp.concatenate(
        [
            dot(ranks[:, :16], up_forward_ref[...]) + bias_forward_ref[...],
            dot(ranks[:, 16:32], up_backward_ref[...]) + bias_backward_ref[...],
        ],
        axis=1,
    )
    log_sigmoid = jnp.minimum(gates, 0.0) - jnp.log1p(jnp.exp(-jnp.abs(gates)))
    return halves(log_sigmoid * (2.0 / (BLOCK * HEADS)))


def summed(parts, mask, way):
    row, col = grid_of((LANES, LANES))
    ones = as_bf16(mask(row, col) & ((row // BLOCK) == (col // BLOCK)))
    lanes = slice(way * WIDTH, (way + 1) * WIDTH)
    return dot(ones, parts[0][:, lanes]) + dot(ones, parts[1][:, lanes])


def block_kernel(
    normed_ref, own_ref, other_ref, up_forward_ref, up_backward_ref,
    bias_forward_ref, bias_backward_ref, payload_ref, rounded_hbm,
    rounded_ref, sem,
):
    core = lax.axis_index("dp_2")

    def columns(ref, first):
        return jnp.concatenate(
            [ref[:, g * 32 : (g + 1) * 32, :].reshape(WIDTH, LANES) for g in (first, first + 1)], axis=1
        )

    def rank_columns(ref):
        packed = ref[:, COLUMNS + 64 :, :].astype(f32)
        rows = jnp.stack([packed[:, :, 32 * i : 32 * i + 32] for i in range(4)], axis=1)
        return rows.reshape(WIDTH, 32).astype(bf16)

    mine, theirs = normed_ref[core], normed_ref[1 - core]
    pieces = [
        dot(mine, columns(own_ref, first)) + dot(theirs, columns(other_ref, first))
        for first in (0, 2, 4, 6)
    ]
    pieces.append(dot(mine, rank_columns(own_ref)) + dot(theirs, rank_columns(other_ref)))
    pieces.append(jnp.zeros((2 * BLOCK, LANES - 32), f32))
    rounded = jnp.concatenate(pieces, axis=1).astype(bf16)
    rounded_ref[...] = rounded
    send = pltpu.make_async_copy(rounded_ref, rounded_hbm, sem)
    send.start()
    values = rounded[:, WIDTH : 2 * WIDTH]
    parts = rates_of(
        rounded[:, 2 * WIDTH :], up_forward_ref, up_backward_ref, bias_forward_ref, bias_backward_ref
    )
    high, low = parts
    row, col = grid_of((LANES, LANES))
    fwd, bwd = slice(0, WIDTH), slice(WIDTH, 2 * WIDTH)
    keys32 = rounded[:, :WIDTH].astype(f32)
    remain = (
        halves(keys32 * jnp.exp(summed(parts, lambda r, c: c > r, 0))),
        halves(keys32 * jnp.exp(summed(parts, lambda r, c: c < r, 1))),
    )
    hrow, hcol = grid_of((HEADS, WIDTH))
    mine = hrow == hcol // HEAD
    erow, ecol = grid_of((WIDTH, LANES))
    fold = as_bf16(((erow // LANES) * HEAD + erow % HEAD) == ecol)
    srow, scol = grid_of((8, 128))
    pick = as_bf16(srow == scol // BLOCK)
    lines = []
    for span in (fwd, bwd):
        sums = dot(pick, high[:, span]) + dot(pick, low[:, span])
        for seq in range(2):
            line = jnp.where(mine, sums[seq : seq + 1], 0.0)
            lines.append(
                line[:, :LANES] + line[:, LANES : 2 * LANES]
                + line[:, 2 * LANES : 3 * LANES] + line[:, 3 * LANES :]
            )
    close = dot(jnp.concatenate(halves(jnp.concatenate(lines, axis=1)), axis=0), fold)
    tail = lax.broadcasted_iota(jnp.int32, (HEADS, 8, LANES), 1)
    payload_ref[:, HEAD:, :] = jnp.where(
        tail == 0,
        close[:HEADS][:, None, :],
        jnp.where(tail == 1, close[HEADS:][:, None, :], 0.0),
    ).astype(bf16)
    diagonal = (row // HEAD) == (col // HEAD)
    for group in range(4):
        lanes = slice(group * LANES, (group + 1) * LANES)
        parts = []
        for way in range(2):
            for seq in range(2):
                span = slice(seq * BLOCK, (seq + 1) * BLOCK)
                value = values[span, lanes]
                both = jnp.concatenate([half[span, lanes] for half in remain[way]], axis=0)
                state = dot_tn(both, jnp.concatenate([value, value], axis=0))
                parts.append(jnp.where(diagonal, state, 0.0).astype(bf16))
        folded = dot(jnp.concatenate(parts, axis=1), fold).astype(bf16)
        payload_ref[4 * group : 4 * group + 4, :HEAD, :] = folded.reshape(4, HEAD, LANES)
    send.wait()


def scan_kernel(payload_ref, out_ref):
    row, col = grid_of((LANES, LANES))
    spread = as_bf16((row // HEAD) == (col // HEAD))
    crow, ccol = grid_of((HEAD, LANES))
    mine = ccol % HEAD == crow
    lines = payload_ref[:, HEAD : HEAD + 8, :].astype(f32)
    closing = 0.0
    for part in range(2):
        line = jnp.where(mine[None], lines[:, part : part + 1, :], 0.0)
        closing = closing + dot(line.astype(bf16).reshape(WIDTH, LANES), spread)
    decay = jnp.exp(closing)
    states = payload_ref[:, :HEAD, :].astype(f32).reshape(WIDTH, LANES)
    lane = lax.broadcasted_iota(jnp.int32, (HEAD, LANES), 1)
    ahead = [None] * HEADS
    behind = [None] * HEADS

    def at(x, i):
        return x[i * HEAD : (i + 1) * HEAD, :]

    carried = jnp.zeros((HEAD, LANES), f32)
    order = [GROUP.index(z) for z in range(HEADS)]
    for i in order:
        ahead[i] = carried
        carried = at(decay, i) * carried + at(states, i)
    carried = jnp.zeros((HEAD, LANES), f32)
    for i in reversed(order):
        behind[i] = carried
        carried = at(decay, i) * carried + at(states, i)
    for i in range(HEADS):
        place = RETURN_GROUP.index(GROUP[i])
        out_ref[place * HEAD : (place + 1) * HEAD, :] = jnp.where(
            lane < LANES // 2, ahead[i], behind[i]
        ).astype(bf16)


def query_kernel(
    tokens_ref, gain_ref, own_ref, other_ref, rounded_ref, up_forward_ref, up_backward_ref,
    bias_forward_ref, bias_backward_ref, out_ref,
):
    core = lax.axis_index("dp_2")

    def weights(ref):
        return jnp.concatenate(
            [
                ref[slot_of(quarter, "dp_0")].reshape(WIDTH, LANES)
                for quarter in range(4)
            ],
            axis=1,
        )

    first, second = normed_halves(tokens_ref, gain_ref)
    projected = dot(jnp.where(core == 0, first, second), weights(own_ref)) + dot(
        jnp.where(core == 0, second, first), weights(other_ref)
    )
    queries = projected.astype(bf16).astype(f32) * HEAD ** (-0.5)
    keys = rounded_ref[:, :WIDTH].astype(f32)
    parts = rates_of(
        rounded_ref[:, 2 * WIDTH :], up_forward_ref, up_backward_ref, bias_forward_ref, bias_backward_ref
    )
    decayed, inverse = [], []
    for way, mask in ((0, lambda r, c: c <= r), (1, lambda r, c: c >= r)):
        running = summed(parts, mask, way)
        product = queries * jnp.exp(running)
        out_ref[:, (way + 1) * WIDTH : (way + 2) * WIDTH] = product
        decayed.append(product.astype(bf16))
        inverse.append((keys * jnp.exp(-running)).astype(bf16))
    row, col = grid_of((WIDTH, WIDTH))
    natural = ((col % 256) // 16) * HEAD + (col // 256) * 16 + col % 16
    values = dot(rounded_ref[:, WIDTH : 2 * WIDTH], as_bf16(row == natural)).astype(bf16)
    row, col = grid_of((WIDTH, 256))
    own_lanes = as_bf16((row // BLOCK) == (col // HEAD))
    srow, scol = grid_of((WIDTH, BLOCK))
    lower = (srow % BLOCK) >= scol
    upper = (srow % BLOCK) <= scol
    vrow, vcol = grid_of((WIDTH, LANES))
    own_values = (vrow // BLOCK) == (vcol // 16)
    for seq in range(2):
        span = slice(seq * BLOCK, (seq + 1) * BLOCK)
        for group in range(2):
            wide = slice(group * 256, (group + 1) * 256)
            scores = 0.0
            for way, mask in ((0, lower), (1, upper)):
                stacked = jnp.concatenate([decayed[way][span, wide]] * 8, axis=0) * own_lanes
                scores = scores + jnp.where(mask, dot_nt(stacked, inverse[way][span, wide]), 0.0)
            scores = scores.astype(bf16)
            for half in range(2):
                start = half * 256 + group * LANES
                spread = dot(scores, values[span, start : start + LANES])
                spread = jnp.where(own_values, spread, 0.0)
                total = spread[:BLOCK]
                for head in range(1, 8):
                    total = total + spread[head * BLOCK : (head + 1) * BLOCK]
                out_ref[span, start : start + LANES] = total


def out_kernel(
    states_ref, parts_ref, gain_ref, own_ref, other_ref, out_ref
):
    spans = [slice(seq * BLOCK, (seq + 1) * BLOCK) for seq in range(2)]
    core = lax.axis_index("dp_2")
    row, col = grid_of((LANES, 8 * LANES))
    source = (col // 256) * HEAD + ((col // LANES) % 2) * 16 + col % 16
    widen = as_bf16(row == source)
    row, col = grid_of((256, 8 * LANES))
    diagonal = (row // HEAD) == ((col % LANES) // 16)
    by_group = (
        jnp.concatenate([states_ref[14 * HEAD :, :], states_ref[: 6 * HEAD, :]], axis=0),
        states_ref[6 * HEAD : 14 * HEAD, :],
    )
    full = [jnp.where(diagonal, dot(rows, widen), 0.0).astype(bf16) for rows in by_group]
    totals = [[], []]
    for seq, span in enumerate(spans):
        sides = [[], []]
        for group in range(2):
            queries = jnp.concatenate(
                [
                    parts_ref[span, (way + 1) * WIDTH + group * 256 : (way + 1) * WIDTH + group * 256 + 256]
                    for way in range(2)
                ],
                axis=1,
            )
            right = jnp.concatenate(
                [full[group][:, (2 * way + seq) * 256 : (2 * way + seq + 1) * 256] for way in range(2)],
                axis=0,
            )
            across = dot(jnp.concatenate(halves(queries), axis=0), right)
            across = across[:BLOCK] + across[BLOCK:]
            for half in range(2):
                start = half * 256 + group * LANES
                sides[half].append(
                    parts_ref[span, start : start + LANES] + across[:, half * LANES : (half + 1) * LANES]
                )
        for half in range(2):
            totals[half].append(jnp.concatenate(sides[half], axis=1))
    combined = [jnp.concatenate(total, axis=0) for total in totals]
    high, low = halves(combined[0] * combined[0] + combined[1] * combined[1])
    row, col = grid_of((256, 256))
    ones = as_bf16((row // 16) == (col // 16))
    scale = lax.rsqrt((dot(high, ones) + dot(low, ones)) * (1.0 / HEAD) + EPS)
    attended = [
        (combined[half] * scale * gain_ref[half : half + 1, :]).astype(bf16) for half in range(2)
    ]
    mine = jnp.where(core == 0, attended[0], attended[1])
    theirs = jnp.where(core == 0, attended[1], attended[0])
    for quarter in range(4):
        slot = slot_of(quarter, "dp_0")

        def weights(ref):
            return jnp.concatenate(
                [
                    jnp.concatenate(
                        [ref[slot, 1:, rows : rows + 16, :], ref[slot, :1, rows : rows + 16, :]], axis=0
                    ).reshape(256, LANES)
                    for rows in (0, 16)
                ],
                axis=1,
            )

        out_ref[:, quarter * 256 : (quarter + 1) * 256] = (
            dot(mine, weights(own_ref)) + dot(theirs, weights(other_ref))
        ).astype(bf16)


VMEM = pl.BlockSpec(memory_space=pltpu.VMEM)


def call(kernel, outs, specs, cycles, *args, scratch=(), out_specs=None):
    many = isinstance(outs, tuple)
    return pl.pallas_call(
        kernel,
        out_shape=outs,
        in_specs=specs,
        out_specs=out_specs or ((VMEM,) * len(outs) if many else VMEM),
        scratch_shapes=scratch,
        cost_estimate=pl.CostEstimate(flops=cycles, bytes_accessed=1 << 20, transcendentals=0),
        compiler_params=pltpu.CompilerParams(vmem_limit_bytes=16 << 20),
    )(*args)


def in_hbm(x):
    return pltpu.with_memory_space_constraint(x, pltpu.HBM)


def swapped(x):
    return lax.ppermute(x, "dp_2", [(0, 1), (1, 0)])


def body(
    tokens, norm_gain, w_query, w_key, w_value, w_rank_forward, w_rank_backward,
    up_forward, up_backward, bias_forward, bias_backward, out_gain, w_out,
):
    seqs, toks, width = tokens.shape
    rows = seqs * toks
    shape = jax.ShapeDtypeStruct
    tokens_flat, gain_flat = tokens.reshape(rows, width), norm_gain.reshape(1, width)
    hbm = pl.BlockSpec(memory_space=pltpu.HBM)
    sources = [
        in_hbm(x)
        for x in (w_key, w_value, w_query, w_rank_forward.T, w_rank_backward.T, w_out)
    ]
    send = call(
        pack_kernel, shape((16, SENT, LANES), bf16), [hbm] * 6, 1 << 26, *sources,
        scratch=[pltpu.VMEM(x.shape, bf16) for x in sources] + [pltpu.SemaphoreType.DMA((6,))],
    )
    own = lax.all_to_all(send, PLANE, 0, 0, axis_index_groups=[PLANE_GROUP])
    other = swapped(own)
    mix = own[None, :, COLUMNS : COLUMNS + 64, :]
    for step, flip in enumerate((1, 3)):
        arrived = lax.ppermute(mix, "dp_0", [(i, i ^ flip) for i in range(4)])
        if step == 0:
            mix = call(
                join_kernel, shape((2, 16, 64, LANES), bf16), [VMEM] * 2, 1 << 26, mix, arrived
            )
        else:
            query, mix = call(
                split_kernel,
                (pltpu.HBM((4, 16, 32, LANES), bf16), shape((4, 16, 32, LANES), bf16)),
                [VMEM] * 2, 1 << 26,
                mix, arrived,
            )
    normed = call(
        norm_kernel, shape((2, rows, 512), bf16), [VMEM, VMEM], 1 << 28,
        tokens_flat, gain_flat,
    )
    decays = (
        up_forward, up_backward, bias_forward.reshape(1, WIDTH), bias_backward.reshape(1, WIDTH)
    )
    payload, rounded = call(
        block_kernel, (shape((HEADS, 40, LANES), bf16), pltpu.HBM((rows, ALL), bf16)),
        [VMEM] * 7, 1 << 30, normed, own, other, *decays, out_specs=(VMEM, hbm),
        scratch=[pltpu.VMEM((rows, ALL), bf16), pltpu.SemaphoreType.DMA],
    )
    inbound = lax.all_to_all(payload, "sp", 0, 0, axis_index_groups=[GROUP])
    query_other = swapped(query)
    mix_other = swapped(mix)
    states = call(
        scan_kernel, shape((WIDTH, LANES), bf16), [VMEM], 1 << 28,
        inbound,
    )
    returned = lax.all_to_all(
        states.reshape(HEADS, HEAD, LANES), "sp", 0, 0, axis_index_groups=[RETURN_GROUP]
    )
    parts = call(
        query_kernel, shape((rows, 3 * WIDTH), f32), [VMEM] * 9, 1 << 30,
        in_hbm(tokens_flat), gain_flat, in_hbm(query), query_other, in_hbm(rounded), *decays,
    )
    gain = jnp.tile(out_gain.reshape(2, 1, 16), (1, HEADS, 1)).reshape(2, 256)
    mixed = call(
        out_kernel, shape((rows, width), bf16), [VMEM] * 5, 1 << 30,
        returned.reshape(WIDTH, LANES), parts, gain, mix, mix_other,
    )
    return mixed.reshape(seqs, toks, width)


def solution(mesh):
    finer = Mesh(mesh.devices.reshape(mesh.shape["sp"], 4, 4, 2), ("sp", "dp_0", "dp_1", "dp_2"))
    rows = P(DP, None)
    in_specs = (
        P(DP, "sp", None), P(), rows, rows, rows, rows, rows, P(), P(), P(), P(), P(), rows,
    )

    return jax.shard_map(
        body, mesh=finer, in_specs=in_specs, out_specs=P(DP, "sp", None), check_vma=False
    )
```

```python
import jax
import jax.numpy as jnp
from jax import lax
from jax.experimental import pallas as pl
from jax.experimental.pallas import tpu as pltpu
from jax.sharding import Mesh
from jax.sharding import PartitionSpec as P

DP = ("dp_0", "dp_1", "dp_2")
PLANE = ("dp_0", "dp_1")
HEAD = 32
HEADS = 16
WIDTH = 512
BLOCK = 64
LANES = 128
ALL = 2 * WIDTH + LANES
COLUMNS = 8 * 32
SENT = COLUMNS + 32 + 32 + 8
EPS = 1e-06
GROUP = [(z + 12) % 16 for z in range(16)]
PLANE_GROUP = [(i + 15) % 16 for i in range(16)]
f32 = jnp.float32
bf16 = jnp.bfloat16


def dot(a, b):
    return jnp.dot(a, b, preferred_element_type=f32)


def dot_tn(a, b):
    return lax.dot_general(a, b, (((0,), (0,)), ((), ())), preferred_element_type=f32)


def dot_nt(a, b):
    return lax.dot_general(a, b, (((1,), (1,)), ((), ())), preferred_element_type=f32)


def halves(x):
    high = x.astype(bf16)
    return high, (x - high.astype(f32)).astype(bf16)


def grid_of(shape):
    return lax.broadcasted_iota(jnp.int32, shape, 0), lax.broadcasted_iota(jnp.int32, shape, 1)


def as_bf16(mask):
    return jnp.where(mask, 1.0, 0.0).astype(bf16)


def pack_kernel(
    key_hbm, value_hbm, query_hbm, forward_hbm, backward_hbm, mix_hbm,
    out_ref, key_ref, value_ref, query_ref, forward_ref, backward_ref, mix_ref, sems,
):
    sources = (key_hbm, value_hbm, query_hbm, forward_hbm, backward_hbm, mix_hbm)
    targets = (key_ref, value_ref, query_ref, forward_ref, backward_ref, mix_ref)
    copies = [
        pltpu.make_async_copy(source, target, sems.at[i])
        for i, (source, target) in enumerate(zip(sources, targets))
    ]
    for copy in copies:
        copy.start()
    for which, (ref, first) in enumerate(((key_ref, 0), (value_ref, 4))):
        copies[which].wait()
        for i in range(16):
            for group in range(4):
                lanes = slice(group * LANES, (group + 1) * LANES)
                out_ref[i, (first + group) * 32 : (first + group + 1) * 32] = ref[:, lanes]
    for copy in copies[2:]:
        copy.wait()
    row, col = grid_of((16, LANES))
    ranks = dot_tn(forward_ref[...], as_bf16(row == col)) + dot_tn(
        backward_ref[...], as_bf16(row + 16 == col)
    )
    packed = jnp.concatenate([ranks[8 * i : 8 * i + 8, :32] for i in range(4)], axis=1)
    for i, peer in enumerate(PLANE_GROUP):
        start = (peer // 4) * LANES
        out_ref[i, COLUMNS : COLUMNS + 32] = query_ref[:, start : start + LANES]
        out_ref[i, COLUMNS + 32 : COLUMNS + 48] = mix_ref[:, 2 * start : 2 * start + LANES]
        out_ref[i, COLUMNS + 48 : COLUMNS + 64] = mix_ref[:, 2 * start + LANES : 2 * start + 2 * LANES]
        out_ref[i, COLUMNS + 64 :] = packed.astype(bf16)


def join_kernel(first_ref, second_ref, out_ref):
    count = first_ref.shape[0]
    out_ref[:count] = first_ref[...]
    out_ref[count:] = second_ref[...]


def split_kernel(first_ref, second_ref, query_ref, mix_ref):
    for part, ref in enumerate((first_ref, second_ref)):
        query_ref[2 * part : 2 * part + 2] = ref[:, :, :32, :]
        mix_ref[2 * part : 2 * part + 2] = ref[:, :, 32:, :]


def slot_of(index, axis):
    apart = index ^ lax.axis_index(axis)
    return apart ^ (apart >> 1)


def normed_halves(tokens_ref, gain_ref):
    values = tokens_ref[...].astype(f32)
    scale = lax.rsqrt(jnp.mean(values * values, axis=-1, keepdims=True) + EPS)
    normed = (values * scale * gain_ref[...]).astype(bf16)
    return [
        jnp.concatenate(
            [normed[:, (2 * i + core) * 32 : (2 * i + core) * 32 + 32] for i in PLANE_GROUP], axis=1
        )
        for core in range(2)
    ]


def norm_kernel(tokens_ref, gain_ref, normed_ref):
    for core, half in enumerate(normed_halves(tokens_ref, gain_ref)):
        normed_ref[core] = half


def rates_of(ranks, up_forward_ref, up_backward_ref, bias_forward_ref, bias_backward_ref):
    gates = jnp.concatenate(
        [
            dot(ranks[:, :16], up_forward_ref[...]) + bias_forward_ref[...],
            dot(ranks[:, 16:32], up_backward_ref[...]) + bias_backward_ref[...],
        ],
        axis=1,
    )
    log_sigmoid = jnp.minimum(gates, 0.0) - jnp.log(1.0 + jnp.exp(-jnp.abs(gates)))
    return halves(log_sigmoid * (2.0 / (BLOCK * HEADS)))


def summed(parts, mask, way):
    row, col = grid_of((LANES, LANES))
    ones = as_bf16(mask(row, col) & ((row // BLOCK) == (col // BLOCK)))
    lanes = slice(way * WIDTH, (way + 1) * WIDTH)
    both = jnp.concatenate([part[:, lanes] for part in parts], axis=0)
    return dot(jnp.concatenate([ones, ones], axis=1), both)


def block_kernel(
    normed_ref, own_ref, other_ref, up_forward_ref, up_backward_ref,
    bias_forward_ref, bias_backward_ref, payload_ref, rounded_ref,
):
    core = lax.axis_index("dp_2")

    def columns(ref, first):
        return jnp.concatenate(
            [ref[:, g * 32 : (g + 1) * 32, :].reshape(WIDTH, LANES) for g in (first, first + 1)], axis=1
        )

    def rank_columns(ref):
        packed = ref[:, COLUMNS + 64 :, :].astype(f32)
        rows = jnp.stack([packed[:, :, 32 * i : 32 * i + 32] for i in range(4)], axis=1)
        return rows.reshape(WIDTH, 32).astype(bf16)

    rows = jnp.concatenate([normed_ref[core], normed_ref[1 - core]], axis=1)
    pieces = [
        dot(
            rows,
            jnp.concatenate([columns(own_ref, first), columns(other_ref, first)], axis=0),
        )
        for first in (0, 2, 4, 6)
    ]
    pieces.append(
        dot(rows, jnp.concatenate([rank_columns(own_ref), rank_columns(other_ref)], axis=0))
    )
    pieces.append(jnp.zeros((2 * BLOCK, LANES - 32), f32))
    rounded = jnp.concatenate(pieces, axis=1).astype(bf16)
    rounded_ref[...] = rounded
    values = rounded[:, WIDTH : 2 * WIDTH]
    parts = rates_of(
        rounded[:, 2 * WIDTH :], up_forward_ref, up_backward_ref, bias_forward_ref, bias_backward_ref
    )
    high, low = parts
    row, col = grid_of((LANES, LANES))
    fwd, bwd = slice(0, WIDTH), slice(WIDTH, 2 * WIDTH)
    keys32 = rounded[:, :WIDTH].astype(f32)
    remain = (
        halves(keys32 * jnp.exp(summed(parts, lambda r, c: c > r, 0))),
        halves(keys32 * jnp.exp(summed(parts, lambda r, c: c < r, 1))),
    )
    hrow, hcol = grid_of((HEADS, WIDTH))
    mine = hrow == hcol // HEAD
    erow, ecol = grid_of((WIDTH, LANES))
    fold = as_bf16(((erow // LANES) * HEAD + erow % HEAD) == ecol)
    srow, scol = grid_of((8, 128))
    pick = as_bf16(srow == scol // BLOCK)
    lines = []
    for span in (fwd, bwd):
        sums = dot(
            jnp.concatenate([pick, pick], axis=1),
            jnp.concatenate([high[:, span], low[:, span]], axis=0),
        )
        for seq in range(2):
            line = jnp.where(mine, sums[seq : seq + 1], 0.0)
            lines.append(
                line[:, :LANES] + line[:, LANES : 2 * LANES]
                + line[:, 2 * LANES : 3 * LANES] + line[:, 3 * LANES :]
            )
    close = dot(jnp.concatenate(halves(jnp.concatenate(lines, axis=1)), axis=0), fold)
    tail = lax.broadcasted_iota(jnp.int32, (HEADS, 8, LANES), 1)
    payload_ref[:, HEAD:, :] = jnp.where(
        tail == 0,
        close[:HEADS][:, None, :],
        jnp.where(tail == 1, close[HEADS:][:, None, :], 0.0),
    ).astype(bf16)
    drow, dcol = grid_of((LANES, 2 * LANES))
    diagonal = (drow // HEAD) == ((dcol % LANES) // HEAD)
    for group in range(4):
        lanes = slice(group * LANES, (group + 1) * LANES)
        value = values[:, lanes]
        empty = jnp.zeros((BLOCK, LANES), bf16)
        by_seq = jnp.concatenate(
            [
                jnp.concatenate([value[:BLOCK], empty], axis=0),
                jnp.concatenate([empty, value[BLOCK:]], axis=0),
            ],
            axis=1,
        )
        by_seq = jnp.concatenate([by_seq, by_seq], axis=0)
        parts = []
        for way in range(2):
            both = jnp.concatenate([half[:, lanes] for half in remain[way]], axis=0)
            state = dot_tn(both, by_seq)
            parts.append(jnp.where(diagonal, state, 0.0).astype(bf16))
        folded = dot(jnp.concatenate(parts, axis=1), fold).astype(bf16)
        payload_ref[4 * group : 4 * group + 4, :HEAD, :] = folded.reshape(4, HEAD, LANES)


def scan_kernel(payload_ref, out_ref):
    row, col = grid_of((LANES, LANES))
    spread = as_bf16((row // HEAD) == (col // HEAD))
    crow, ccol = grid_of((HEAD, LANES))
    mine = ccol % HEAD == crow
    lines = payload_ref[:, HEAD : HEAD + 8, :].astype(f32)
    closing = 0.0
    for part in range(2):
        line = jnp.where(mine[None], lines[:, part : part + 1, :], 0.0)
        closing = closing + dot(line.astype(bf16).reshape(WIDTH, LANES), spread)
    decay = jnp.exp(closing)
    states = payload_ref[:, :HEAD, :].astype(f32).reshape(WIDTH, LANES)
    lane = lax.broadcasted_iota(jnp.int32, (HEAD, LANES), 1)
    ahead = [None] * HEADS
    behind = [None] * HEADS

    def at(x, i):
        return x[i * HEAD : (i + 1) * HEAD, :]

    carried = jnp.zeros((HEAD, LANES), f32)
    order = [GROUP.index(z) for z in range(HEADS)]
    for i in order:
        ahead[i] = carried
        carried = at(decay, i) * carried + at(states, i)
    carried = jnp.zeros((HEAD, LANES), f32)
    for i in reversed(order):
        behind[i] = carried
        carried = at(decay, i) * carried + at(states, i)
    for i in range(HEADS):
        out_ref[i * HEAD : (i + 1) * HEAD, :] = jnp.where(
            lane < LANES // 2, ahead[i], behind[i]
        ).astype(bf16)


def query_kernel(
    tokens_ref, gain_ref, own_ref, other_ref, rounded_ref, up_forward_ref, up_backward_ref,
    bias_forward_ref, bias_backward_ref, out_ref,
):
    core = lax.axis_index("dp_2")

    def weights(ref):
        return jnp.concatenate(
            [
                ref[slot_of(quarter, "dp_0")].reshape(WIDTH, LANES)
                for quarter in range(4)
            ],
            axis=1,
        )

    first, second = normed_halves(tokens_ref, gain_ref)
    projected = dot(jnp.where(core == 0, first, second), weights(own_ref)) + dot(
        jnp.where(core == 0, second, first), weights(other_ref)
    )
    queries = projected.astype(bf16).astype(f32) * HEAD ** (-0.5)
    keys = rounded_ref[:, :WIDTH].astype(f32)
    parts = rates_of(
        rounded_ref[:, 2 * WIDTH :], up_forward_ref, up_backward_ref, bias_forward_ref, bias_backward_ref
    )
    decayed, inverse = [], []
    for way, mask in ((0, lambda r, c: c <= r), (1, lambda r, c: c >= r)):
        running = summed(parts, mask, way)
        product = queries * jnp.exp(running)
        out_ref[:, (way + 1) * WIDTH : (way + 2) * WIDTH] = product
        decayed.append(product.astype(bf16))
        inverse.append((keys * jnp.exp(-running)).astype(bf16))
    row, col = grid_of((WIDTH, WIDTH))
    natural = ((col % 256) // 16) * HEAD + (col // 256) * 16 + col % 16
    values = dot(rounded_ref[:, WIDTH : 2 * WIDTH], as_bf16(row == natural)).astype(bf16)
    row, col = grid_of((WIDTH, 256))
    own_lanes = as_bf16((row // BLOCK) == (col // HEAD))
    srow, scol = grid_of((WIDTH, BLOCK))
    lower = (srow % BLOCK) >= scol
    upper = (srow % BLOCK) <= scol
    vrow, vcol = grid_of((WIDTH, LANES))
    own_values = (vrow // BLOCK) == (vcol // 16)
    for seq in range(2):
        span = slice(seq * BLOCK, (seq + 1) * BLOCK)
        for group in range(2):
            wide = slice(group * 256, (group + 1) * 256)
            scores = 0.0
            for way, mask in ((0, lower), (1, upper)):
                stacked = jnp.concatenate([decayed[way][span, wide]] * 8, axis=0) * own_lanes
                scores = scores + jnp.where(mask, dot_nt(stacked, inverse[way][span, wide]), 0.0)
            scores = scores.astype(bf16)
            for half in range(2):
                start = half * 256 + group * LANES
                spread = dot(scores, values[span, start : start + LANES])
                spread = jnp.where(own_values, spread, 0.0)
                total = spread[:BLOCK]
                for head in range(1, 8):
                    total = total + spread[head * BLOCK : (head + 1) * BLOCK]
                out_ref[span, start : start + LANES] = total


def out_kernel(
    states_ref, parts_ref, gain_ref, own_ref, other_ref, out_ref
):
    spans = [slice(seq * BLOCK, (seq + 1) * BLOCK) for seq in range(2)]
    core = lax.axis_index("dp_2")
    row, col = grid_of((LANES, 8 * LANES))
    source = (col // 256) * HEAD + ((col // LANES) % 2) * 16 + col % 16
    widen = as_bf16(row == source)
    row, col = grid_of((256, 8 * LANES))
    diagonal = (row // HEAD) == ((col % LANES) // 16)
    full = [
        jnp.where(diagonal, dot(states_ref[g * 256 : (g + 1) * 256, :], widen), 0.0).astype(bf16)
        for g in range(2)
    ]
    totals = [[], []]
    for seq, span in enumerate(spans):
        sides = [[], []]
        for group in range(2):
            queries = jnp.concatenate(
                [
                    parts_ref[span, (way + 1) * WIDTH + group * 256 : (way + 1) * WIDTH + group * 256 + 256]
                    for way in range(2)
                ],
                axis=1,
            )
            right = jnp.concatenate(
                [full[group][:, (2 * way + seq) * 256 : (2 * way + seq + 1) * 256] for way in range(2)],
                axis=0,
            )
            across = dot(jnp.concatenate(halves(queries), axis=0), right)
            across = across[:BLOCK] + across[BLOCK:]
            for half in range(2):
                start = half * 256 + group * LANES
                sides[half].append(
                    parts_ref[span, start : start + LANES] + across[:, half * LANES : (half + 1) * LANES]
                )
        for half in range(2):
            totals[half].append(jnp.concatenate(sides[half], axis=1))
    combined = [jnp.concatenate(total, axis=0) for total in totals]
    high, low = halves(combined[0] * combined[0] + combined[1] * combined[1])
    row, col = grid_of((256, 256))
    ones = as_bf16((row // 16) == (col // 16))
    scale = lax.rsqrt((dot(high, ones) + dot(low, ones)) * (1.0 / HEAD) + EPS)
    attended = [
        (combined[half] * scale * gain_ref[half : half + 1, :]).astype(bf16) for half in range(2)
    ]
    mine = jnp.where(core == 0, attended[0], attended[1])
    theirs = jnp.where(core == 0, attended[1], attended[0])
    for quarter in range(4):
        slot = slot_of(quarter, "dp_0")

        def weights(ref):
            return jnp.concatenate(
                [
                    jnp.concatenate(
                        [ref[slot, 1:, rows : rows + 16, :], ref[slot, :1, rows : rows + 16, :]], axis=0
                    ).reshape(256, LANES)
                    for rows in (0, 16)
                ],
                axis=1,
            )

        out_ref[:, quarter * 256 : (quarter + 1) * 256] = (
            dot(mine, weights(own_ref)) + dot(theirs, weights(other_ref))
        ).astype(bf16)


VMEM = pl.BlockSpec(memory_space=pltpu.VMEM)


def call(kernel, outs, specs, cycles, *args, scratch=()):
    many = isinstance(outs, tuple)
    return pl.pallas_call(
        kernel,
        out_shape=outs,
        in_specs=specs,
        out_specs=(VMEM,) * len(outs) if many else VMEM,
        scratch_shapes=scratch,
        cost_estimate=pl.CostEstimate(flops=cycles, bytes_accessed=1 << 20, transcendentals=0),
        compiler_params=pltpu.CompilerParams(vmem_limit_bytes=16 << 20),
    )(*args)


def in_hbm(x):
    return pltpu.with_memory_space_constraint(x, pltpu.HBM)


def swapped(x):
    return lax.ppermute(x, "dp_2", [(0, 1), (1, 0)])


def body(
    tokens, norm_gain, w_query, w_key, w_value, w_rank_forward, w_rank_backward,
    up_forward, up_backward, bias_forward, bias_backward, out_gain, w_out,
):
    seqs, toks, width = tokens.shape
    rows = seqs * toks
    shape = jax.ShapeDtypeStruct
    tokens_flat, gain_flat = tokens.reshape(rows, width), norm_gain.reshape(1, width)
    hbm = pl.BlockSpec(memory_space=pltpu.HBM)
    sources = [
        in_hbm(x)
        for x in (w_key, w_value, w_query, w_rank_forward.T, w_rank_backward.T, w_out)
    ]
    send = call(
        pack_kernel, shape((16, SENT, LANES), bf16), [hbm] * 6, 1 << 26, *sources,
        scratch=[pltpu.VMEM(x.shape, bf16) for x in sources] + [pltpu.SemaphoreType.DMA((6,))],
    )
    own = lax.all_to_all(send, PLANE, 0, 0, axis_index_groups=[PLANE_GROUP])
    other = swapped(own)
    mix = own[None, :, COLUMNS : COLUMNS + 64, :]
    for step, flip in enumerate((1, 3)):
        arrived = lax.ppermute(mix, "dp_0", [(i, i ^ flip) for i in range(4)])
        if step == 0:
            mix = call(
                join_kernel, shape((2, 16, 64, LANES), bf16), [VMEM] * 2, 1 << 26, mix, arrived
            )
        else:
            query, mix = call(
                split_kernel,
                (pltpu.HBM((4, 16, 32, LANES), bf16), shape((4, 16, 32, LANES), bf16)),
                [VMEM] * 2, 1 << 26,
                mix, arrived,
            )
    normed = call(
        norm_kernel, shape((2, rows, 512), bf16), [VMEM, VMEM], 1 << 28,
        tokens_flat, gain_flat,
    )
    decays = (
        up_forward, up_backward, bias_forward.reshape(1, WIDTH), bias_backward.reshape(1, WIDTH)
    )
    payload, rounded = call(
        block_kernel,
        (
            shape((HEADS, 40, LANES), bf16), pltpu.HBM((rows, ALL), bf16),
        ),
        [VMEM] * 7, 1 << 30, normed, own, other, *decays,
    )
    inbound = lax.all_to_all(payload, "sp", 0, 0, axis_index_groups=[GROUP])
    query_other = swapped(query)
    mix_other = swapped(mix)
    states = call(
        scan_kernel, shape((WIDTH, LANES), bf16), [VMEM], 1 << 28,
        inbound,
    )
    returned = lax.all_to_all(
        states.reshape(HEADS, HEAD, LANES), "sp", 0, 0, axis_index_groups=[GROUP]
    )
    parts = call(
        query_kernel, shape((rows, 3 * WIDTH), f32), [VMEM] * 9, 1 << 30,
        in_hbm(tokens_flat), gain_flat, query, query_other, in_hbm(rounded), *decays,
    )
    gain = jnp.tile(out_gain.reshape(2, 1, 16), (1, HEADS, 1)).reshape(2, 256)
    mixed = call(
        out_kernel, shape((rows, width), bf16), [VMEM] * 5, 1 << 30,
        returned.reshape(WIDTH, LANES), parts, gain, mix, mix_other,
    )
    return mixed.reshape(seqs, toks, width)


def solution(mesh):
    finer = Mesh(mesh.devices.reshape(mesh.shape["sp"], 4, 4, 2), ("sp", "dp_0", "dp_1", "dp_2"))
    rows = P(DP, None)
    in_specs = (
        P(DP, "sp", None), P(), rows, rows, rows, rows, rows, P(), P(), P(), P(), P(), rows,
    )

    return jax.shard_map(
        body, mesh=finer, in_specs=in_specs, out_specs=P(DP, "sp", None), check_vma=False
    )
```

```python
import jax
import jax.numpy as jnp
from jax import lax
from jax.experimental import pallas as pl
from jax.experimental.pallas import tpu as pltpu
from jax.sharding import Mesh
from jax.sharding import PartitionSpec as P

DP = ("dp_0", "dp_1", "dp_2")
PLANE = ("dp_0", "dp_1")
HEAD = 32
HEADS = 16
WIDTH = 512
BLOCK = 64
LANES = 128
ALL = 2 * WIDTH + LANES
COLUMNS = 8 * 32
SENT = COLUMNS + 32 + 32 + 8
EPS = 1e-06
GROUP = [(z + 12) % 16 for z in range(16)]
PLANE_GROUP = [(5 * i + 15) % 16 for i in range(16)]
f32 = jnp.float32
bf16 = jnp.bfloat16


def dot(a, b):
    return jnp.dot(a, b, preferred_element_type=f32)


def dot_tn(a, b):
    return lax.dot_general(a, b, (((0,), (0,)), ((), ())), preferred_element_type=f32)


def dot_nt(a, b):
    return lax.dot_general(a, b, (((1,), (1,)), ((), ())), preferred_element_type=f32)


def halves(x):
    high = x.astype(bf16)
    return high, (x - high.astype(f32)).astype(bf16)


def grid_of(shape):
    return lax.broadcasted_iota(jnp.int32, shape, 0), lax.broadcasted_iota(jnp.int32, shape, 1)


def as_bf16(mask):
    return jnp.where(mask, 1.0, 0.0).astype(bf16)


def pack_kernel(
    key_hbm, value_hbm, query_hbm, forward_hbm, backward_hbm, mix_hbm,
    out_ref, key_ref, value_ref, query_ref, forward_ref, backward_ref, mix_ref, sems,
):
    sources = (key_hbm, value_hbm, query_hbm, forward_hbm, backward_hbm, mix_hbm)
    targets = (key_ref, value_ref, query_ref, forward_ref, backward_ref, mix_ref)
    copies = [
        pltpu.make_async_copy(source, target, sems.at[i])
        for i, (source, target) in enumerate(zip(sources, targets))
    ]
    for copy in copies:
        copy.start()
    for which, (ref, first) in enumerate(((key_ref, 0), (value_ref, 4))):
        copies[which].wait()
        for i in range(16):
            for group in range(4):
                lanes = slice(group * LANES, (group + 1) * LANES)
                out_ref[i, (first + group) * 32 : (first + group + 1) * 32] = ref[:, lanes]
    for copy in copies[2:]:
        copy.wait()
    row, col = grid_of((16, LANES))
    ranks = dot_tn(forward_ref[...], as_bf16(row == col)) + dot_tn(
        backward_ref[...], as_bf16(row + 16 == col)
    )
    packed = jnp.concatenate([ranks[8 * i : 8 * i + 8, :32] for i in range(4)], axis=1)
    for i, peer in enumerate(PLANE_GROUP):
        start = (peer // 4) * LANES
        out_ref[i, COLUMNS : COLUMNS + 32] = query_ref[:, start : start + LANES]
        out_ref[i, COLUMNS + 32 : COLUMNS + 48] = mix_ref[:, 2 * start : 2 * start + LANES]
        out_ref[i, COLUMNS + 48 : COLUMNS + 64] = mix_ref[:, 2 * start + LANES : 2 * start + 2 * LANES]
        out_ref[i, COLUMNS + 64 :] = packed.astype(bf16)


def join_kernel(first_ref, second_ref, out_ref):
    count = first_ref.shape[0]
    out_ref[:count] = first_ref[...]
    out_ref[count:] = second_ref[...]


def split_kernel(first_ref, second_ref, query_ref, mix_ref):
    for part, ref in enumerate((first_ref, second_ref)):
        query_ref[2 * part : 2 * part + 2] = ref[:, :, :32, :]
        mix_ref[2 * part : 2 * part + 2] = ref[:, :, 32:, :]


def slot_of(index, axis):
    apart = index ^ lax.axis_index(axis)
    return apart ^ (apart >> 1)


def normed_halves(tokens_ref, gain_ref):
    values = tokens_ref[...].astype(f32)
    scale = lax.rsqrt(jnp.mean(values * values, axis=-1, keepdims=True) + EPS)
    normed = (values * scale * gain_ref[...]).astype(bf16)
    return [
        jnp.concatenate(
            [normed[:, (2 * i + core) * 32 : (2 * i + core) * 32 + 32] for i in PLANE_GROUP], axis=1
        )
        for core in range(2)
    ]


def norm_kernel(tokens_ref, gain_ref, normed_ref):
    for core, half in enumerate(normed_halves(tokens_ref, gain_ref)):
        normed_ref[core] = half


def rates_of(ranks, up_forward_ref, up_backward_ref, bias_forward_ref, bias_backward_ref):
    gates = jnp.concatenate(
        [
            dot(ranks[:, :16], up_forward_ref[...]) + bias_forward_ref[...],
            dot(ranks[:, 16:32], up_backward_ref[...]) + bias_backward_ref[...],
        ],
        axis=1,
    )
    log_sigmoid = jnp.minimum(gates, 0.0) - jnp.log(1.0 + jnp.exp(-jnp.abs(gates)))
    return halves(log_sigmoid * (2.0 / (BLOCK * HEADS)))


def summed(parts, mask, way):
    row, col = grid_of((LANES, LANES))
    ones = as_bf16(mask(row, col) & ((row // BLOCK) == (col // BLOCK)))
    lanes = slice(way * WIDTH, (way + 1) * WIDTH)
    both = jnp.concatenate([part[:, lanes] for part in parts], axis=0)
    return dot(jnp.concatenate([ones, ones], axis=1), both)


def block_kernel(
    normed_ref, own_ref, other_ref, up_forward_ref, up_backward_ref,
    bias_forward_ref, bias_backward_ref, payload_ref, rounded_ref,
):
    core = lax.axis_index("dp_2")

    def columns(ref, first):
        return jnp.concatenate(
            [ref[:, g * 32 : (g + 1) * 32, :].reshape(WIDTH, LANES) for g in (first, first + 1)], axis=1
        )

    def rank_columns(ref):
        packed = ref[:, COLUMNS + 64 :, :].astype(f32)
        rows = jnp.stack([packed[:, :, 32 * i : 32 * i + 32] for i in range(4)], axis=1)
        return rows.reshape(WIDTH, 32).astype(bf16)

    rows = jnp.concatenate([normed_ref[core], normed_ref[1 - core]], axis=1)
    pieces = [
        dot(
            rows,
            jnp.concatenate([columns(own_ref, first), columns(other_ref, first)], axis=0),
        )
        for first in (0, 2, 4, 6)
    ]
    pieces.append(
        dot(rows, jnp.concatenate([rank_columns(own_ref), rank_columns(other_ref)], axis=0))
    )
    pieces.append(jnp.zeros((2 * BLOCK, LANES - 32), f32))
    rounded = jnp.concatenate(pieces, axis=1).astype(bf16)
    rounded_ref[...] = rounded
    values = rounded[:, WIDTH : 2 * WIDTH]
    parts = rates_of(
        rounded[:, 2 * WIDTH :], up_forward_ref, up_backward_ref, bias_forward_ref, bias_backward_ref
    )
    high, low = parts
    row, col = grid_of((LANES, LANES))
    fwd, bwd = slice(0, WIDTH), slice(WIDTH, 2 * WIDTH)
    keys32 = rounded[:, :WIDTH].astype(f32)
    remain = (
        halves(keys32 * jnp.exp(summed(parts, lambda r, c: c > r, 0))),
        halves(keys32 * jnp.exp(summed(parts, lambda r, c: c < r, 1))),
    )
    hrow, hcol = grid_of((HEADS, WIDTH))
    mine = hrow == hcol // HEAD
    erow, ecol = grid_of((WIDTH, LANES))
    fold = as_bf16(((erow // LANES) * HEAD + erow % HEAD) == ecol)
    srow, scol = grid_of((8, 128))
    pick = as_bf16(srow == scol // BLOCK)
    lines = []
    for span in (fwd, bwd):
        sums = dot(
            jnp.concatenate([pick, pick], axis=1),
            jnp.concatenate([high[:, span], low[:, span]], axis=0),
        )
        for seq in range(2):
            line = jnp.where(mine, sums[seq : seq + 1], 0.0)
            lines.append(
                line[:, :LANES] + line[:, LANES : 2 * LANES]
                + line[:, 2 * LANES : 3 * LANES] + line[:, 3 * LANES :]
            )
    close = dot(jnp.concatenate(halves(jnp.concatenate(lines, axis=1)), axis=0), fold)
    tail = lax.broadcasted_iota(jnp.int32, (HEADS, 8, LANES), 1)
    payload_ref[:, HEAD:, :] = jnp.where(
        tail == 0,
        close[:HEADS][:, None, :],
        jnp.where(tail == 1, close[HEADS:][:, None, :], 0.0),
    ).astype(bf16)
    drow, dcol = grid_of((LANES, 2 * LANES))
    diagonal = (drow // HEAD) == ((dcol % LANES) // HEAD)
    for group in range(4):
        lanes = slice(group * LANES, (group + 1) * LANES)
        value = values[:, lanes]
        empty = jnp.zeros((BLOCK, LANES), bf16)
        by_seq = jnp.concatenate(
            [
                jnp.concatenate([value[:BLOCK], empty], axis=0),
                jnp.concatenate([empty, value[BLOCK:]], axis=0),
            ],
            axis=1,
        )
        by_seq = jnp.concatenate([by_seq, by_seq], axis=0)
        parts = []
        for way in range(2):
            both = jnp.concatenate([half[:, lanes] for half in remain[way]], axis=0)
            state = dot_tn(both, by_seq)
            parts.append(jnp.where(diagonal, state, 0.0).astype(bf16))
        folded = dot(jnp.concatenate(parts, axis=1), fold).astype(bf16)
        payload_ref[4 * group : 4 * group + 4, :HEAD, :] = folded.reshape(4, HEAD, LANES)


def scan_kernel(payload_ref, out_ref):
    row, col = grid_of((LANES, LANES))
    spread = as_bf16((row // HEAD) == (col // HEAD))
    crow, ccol = grid_of((HEAD, LANES))
    mine = ccol % HEAD == crow
    lines = payload_ref[:, HEAD : HEAD + 8, :].astype(f32)
    closing = 0.0
    for part in range(2):
        line = jnp.where(mine[None], lines[:, part : part + 1, :], 0.0)
        closing = closing + dot(line.astype(bf16).reshape(WIDTH, LANES), spread)
    decay = jnp.exp(closing)
    states = payload_ref[:, :HEAD, :].astype(f32).reshape(WIDTH, LANES)
    lane = lax.broadcasted_iota(jnp.int32, (HEAD, LANES), 1)
    ahead = [None] * HEADS
    behind = [None] * HEADS

    def at(x, i):
        return x[i * HEAD : (i + 1) * HEAD, :]

    carried = jnp.zeros((HEAD, LANES), f32)
    order = [GROUP.index(z) for z in range(HEADS)]
    for i in order:
        ahead[i] = carried
        carried = at(decay, i) * carried + at(states, i)
    carried = jnp.zeros((HEAD, LANES), f32)
    for i in reversed(order):
        behind[i] = carried
        carried = at(decay, i) * carried + at(states, i)
    for i in range(HEADS):
        out_ref[i * HEAD : (i + 1) * HEAD, :] = jnp.where(
            lane < LANES // 2, ahead[i], behind[i]
        ).astype(bf16)


def query_kernel(
    tokens_ref, gain_ref, own_ref, other_ref, rounded_ref, up_forward_ref, up_backward_ref,
    bias_forward_ref, bias_backward_ref, out_ref,
):
    core = lax.axis_index("dp_2")

    def weights(ref):
        return jnp.concatenate(
            [
                ref[slot_of(quarter, "dp_0")].reshape(WIDTH, LANES)
                for quarter in range(4)
            ],
            axis=1,
        )

    first, second = normed_halves(tokens_ref, gain_ref)
    projected = dot(jnp.where(core == 0, first, second), weights(own_ref)) + dot(
        jnp.where(core == 0, second, first), weights(other_ref)
    )
    queries = projected.astype(bf16).astype(f32) * HEAD ** (-0.5)
    keys = rounded_ref[:, :WIDTH].astype(f32)
    parts = rates_of(
        rounded_ref[:, 2 * WIDTH :], up_forward_ref, up_backward_ref, bias_forward_ref, bias_backward_ref
    )
    decayed, inverse = [], []
    for way, mask in ((0, lambda r, c: c <= r), (1, lambda r, c: c >= r)):
        running = summed(parts, mask, way)
        product = queries * jnp.exp(running)
        out_ref[:, (way + 1) * WIDTH : (way + 2) * WIDTH] = product
        decayed.append(product.astype(bf16))
        inverse.append((keys * jnp.exp(-running)).astype(bf16))
    row, col = grid_of((WIDTH, WIDTH))
    natural = ((col % 256) // 16) * HEAD + (col // 256) * 16 + col % 16
    values = dot(rounded_ref[:, WIDTH : 2 * WIDTH], as_bf16(row == natural)).astype(bf16)
    row, col = grid_of((WIDTH, 256))
    own_lanes = as_bf16((row // BLOCK) == (col // HEAD))
    srow, scol = grid_of((WIDTH, BLOCK))
    lower = (srow % BLOCK) >= scol
    upper = (srow % BLOCK) <= scol
    vrow, vcol = grid_of((WIDTH, LANES))
    own_values = (vrow // BLOCK) == (vcol // 16)
    for seq in range(2):
        span = slice(seq * BLOCK, (seq + 1) * BLOCK)
        for group in range(2):
            wide = slice(group * 256, (group + 1) * 256)
            scores = 0.0
            for way, mask in ((0, lower), (1, upper)):
                stacked = jnp.concatenate([decayed[way][span, wide]] * 8, axis=0) * own_lanes
                scores = scores + jnp.where(mask, dot_nt(stacked, inverse[way][span, wide]), 0.0)
            scores = scores.astype(bf16)
            for half in range(2):
                start = half * 256 + group * LANES
                spread = dot(scores, values[span, start : start + LANES])
                spread = jnp.where(own_values, spread, 0.0)
                total = spread[:BLOCK]
                for head in range(1, 8):
                    total = total + spread[head * BLOCK : (head + 1) * BLOCK]
                out_ref[span, start : start + LANES] = total


def out_kernel(
    states_ref, parts_ref, gain_ref, own_ref, other_ref, out_ref
):
    spans = [slice(seq * BLOCK, (seq + 1) * BLOCK) for seq in range(2)]
    core = lax.axis_index("dp_2")
    row, col = grid_of((LANES, LANES))
    lead = row - col % 16
    widen = jnp.concatenate([as_bf16(lead == 16 * i) for i in range(8)], axis=1)
    row, col = grid_of((256, LANES))
    diagonal = (row // HEAD) == (col // 16)
    full = []
    for g in range(2):
        wide = dot(states_ref[g * 256 : (g + 1) * 256, :], widen)
        full.append(
            [
                jnp.where(diagonal, wide[:, i * LANES : (i + 1) * LANES], 0.0).astype(bf16)
                for i in range(8)
            ]
        )
    totals = [[], []]
    for seq, span in enumerate(spans):
        sides = [[], []]
        for group in range(2):
            queries = jnp.concatenate(
                [
                    parts_ref[span, (way + 1) * WIDTH + group * 256 : (way + 1) * WIDTH + group * 256 + 256]
                    for way in range(2)
                ],
                axis=1,
            )
            right = jnp.concatenate(
                [
                    jnp.concatenate(full[group][4 * way + 2 * seq : 4 * way + 2 * seq + 2], axis=1)
                    for way in range(2)
                ],
                axis=0,
            )
            across = dot(jnp.concatenate(halves(queries), axis=0), right)
            across = across[:BLOCK] + across[BLOCK:]
            for half in range(2):
                start = half * 256 + group * LANES
                sides[half].append(
                    parts_ref[span, start : start + LANES] + across[:, half * LANES : (half + 1) * LANES]
                )
        for half in range(2):
            totals[half].append(jnp.concatenate(sides[half], axis=1))
    combined = [jnp.concatenate(total, axis=0) for total in totals]
    high, low = halves(combined[0] * combined[0] + combined[1] * combined[1])
    row, col = grid_of((256, 256))
    ones = as_bf16((row // 16) == (col // 16))
    sums = dot(jnp.concatenate([high, low], axis=1), jnp.concatenate([ones, ones], axis=0))
    scale = lax.rsqrt(sums * (1.0 / HEAD) + EPS)
    attended = [
        (combined[half] * scale * gain_ref[half : half + 1, :]).astype(bf16) for half in range(2)
    ]
    mine = jnp.where(core == 0, attended[0], attended[1])
    theirs = jnp.where(core == 0, attended[1], attended[0])
    both = jnp.concatenate([mine, theirs], axis=1)
    for quarter in range(4):
        slot = slot_of(quarter, "dp_0")

        def weights(ref):
            return jnp.concatenate(
                [
                    jnp.concatenate(
                        [ref[slot, PLANE_GROUP.index(h), rows : rows + 16, :] for h in range(16)], axis=0
                    )
                    for rows in (0, 16)
                ],
                axis=1,
            )

        out_ref[:, quarter * 256 : (quarter + 1) * 256] = dot(
            both, jnp.concatenate([weights(own_ref), weights(other_ref)], axis=0)
        ).astype(bf16)


VMEM = pl.BlockSpec(memory_space=pltpu.VMEM)


def call(kernel, outs, specs, cycles, *args, scratch=()):
    many = isinstance(outs, tuple)
    return pl.pallas_call(
        kernel,
        out_shape=outs,
        in_specs=specs,
        out_specs=(VMEM,) * len(outs) if many else VMEM,
        scratch_shapes=scratch,
        cost_estimate=pl.CostEstimate(flops=cycles, bytes_accessed=1 << 20, transcendentals=0),
        compiler_params=pltpu.CompilerParams(vmem_limit_bytes=16 << 20),
    )(*args)


def in_hbm(x):
    return pltpu.with_memory_space_constraint(x, pltpu.HBM)


def swapped(x):
    return lax.ppermute(x, "dp_2", [(0, 1), (1, 0)])


def body(
    tokens, norm_gain, w_query, w_key, w_value, w_rank_forward, w_rank_backward,
    up_forward, up_backward, bias_forward, bias_backward, out_gain, w_out,
):
    seqs, toks, width = tokens.shape
    rows = seqs * toks
    shape = jax.ShapeDtypeStruct
    tokens_flat, gain_flat = tokens.reshape(rows, width), norm_gain.reshape(1, width)
    hbm = pl.BlockSpec(memory_space=pltpu.HBM)
    sources = [
        in_hbm(x)
        for x in (w_key, w_value, w_query, w_rank_forward.T, w_rank_backward.T, w_out)
    ]
    send = call(
        pack_kernel, shape((16, SENT, LANES), bf16), [hbm] * 6, 1 << 26, *sources,
        scratch=[pltpu.VMEM(x.shape, bf16) for x in sources] + [pltpu.SemaphoreType.DMA((6,))],
    )
    own = lax.all_to_all(send, PLANE, 0, 0, axis_index_groups=[PLANE_GROUP])
    other = swapped(own)
    mix = own[None, :, COLUMNS : COLUMNS + 64, :]
    for step, flip in enumerate((1, 3)):
        arrived = lax.ppermute(mix, "dp_0", [(i, i ^ flip) for i in range(4)])
        if step == 0:
            mix = call(
                join_kernel, shape((2, 16, 64, LANES), bf16), [VMEM] * 2, 1 << 26, mix, arrived
            )
        else:
            query, mix = call(
                split_kernel,
                (pltpu.HBM((4, 16, 32, LANES), bf16), shape((4, 16, 32, LANES), bf16)),
                [VMEM] * 2, 1 << 26,
                mix, arrived,
            )
    normed = call(
        norm_kernel, shape((2, rows, 512), bf16), [VMEM, VMEM], 1 << 28,
        tokens_flat, gain_flat,
    )
    decays = (
        up_forward, up_backward, bias_forward.reshape(1, WIDTH), bias_backward.reshape(1, WIDTH)
    )
    payload, rounded = call(
        block_kernel,
        (
            shape((HEADS, 40, LANES), bf16), pltpu.HBM((rows, ALL), bf16),
        ),
        [VMEM] * 7, 1 << 30, normed, own, other, *decays,
    )
    inbound = lax.all_to_all(payload, "sp", 0, 0, axis_index_groups=[GROUP])
    query_other = swapped(query)
    mix_other = swapped(mix)
    states = call(
        scan_kernel, shape((WIDTH, LANES), bf16), [VMEM], 1 << 28,
        inbound,
    )
    returned = lax.all_to_all(
        states.reshape(HEADS, HEAD, LANES), "sp", 0, 0, axis_index_groups=[GROUP]
    )
    parts = call(
        query_kernel, shape((rows, 3 * WIDTH), f32), [VMEM] * 9, 1 << 30,
        in_hbm(tokens_flat), gain_flat, in_hbm(query), query_other, in_hbm(rounded), *decays,
    )
    gain = jnp.tile(out_gain.reshape(2, 1, 16), (1, HEADS, 1)).reshape(2, 256)
    mixed = call(
        out_kernel, shape((rows, width), bf16), [VMEM] * 5, 1 << 30,
        returned.reshape(WIDTH, LANES), parts, gain, mix, mix_other,
    )
    return mixed.reshape(seqs, toks, width)


def solution(mesh):
    finer = Mesh(mesh.devices.reshape(mesh.shape["sp"], 4, 4, 2), ("sp", "dp_0", "dp_1", "dp_2"))
    rows = P(DP, None)
    in_specs = (
        P(DP, "sp", None), P(), rows, rows, rows, rows, rows, P(), P(), P(), P(), P(), rows,
    )

    return jax.shard_map(
        body, mesh=finer, in_specs=in_specs, out_specs=P(DP, "sp", None), check_vma=False
    )
```

```python
import jax
import jax.numpy as jnp
from jax import lax
from jax.experimental import pallas as pl
from jax.experimental.pallas import tpu as pltpu
from jax.sharding import Mesh
from jax.sharding import PartitionSpec as P

DP = ("dp_0", "dp_1", "dp_2")
PLANE = ("dp_0", "dp_1")
HEAD = 32
HEADS = 16
WIDTH = 512
BLOCK = 64
LANES = 128
ALL = 2 * WIDTH + LANES
COLUMNS = 8 * 32
SENT = COLUMNS + 32 + 32 + 8
EPS = 1e-06
GROUP = [(z + 10) % 16 for z in range(16)]
PLANE_GROUP = [(i + 15) % 16 for i in range(16)]
f32 = jnp.float32
bf16 = jnp.bfloat16


def dot(a, b):
    return jnp.dot(a, b, preferred_element_type=f32)


def dot_tn(a, b):
    return lax.dot_general(a, b, (((0,), (0,)), ((), ())), preferred_element_type=f32)


def dot_nt(a, b):
    return lax.dot_general(a, b, (((1,), (1,)), ((), ())), preferred_element_type=f32)


def halves(x):
    high = x.astype(bf16)
    return high, (x - high.astype(f32)).astype(bf16)


def grid_of(shape):
    return lax.broadcasted_iota(jnp.int32, shape, 0), lax.broadcasted_iota(jnp.int32, shape, 1)


def as_bf16(mask):
    return jnp.where(mask, 1.0, 0.0).astype(bf16)


def pack_kernel(
    key_hbm, value_hbm, query_hbm, forward_hbm, backward_hbm, mix_hbm,
    out_ref, key_ref, value_ref, query_ref, forward_ref, backward_ref, mix_ref, sems,
):
    sources = (key_hbm, value_hbm, query_hbm, forward_hbm, backward_hbm, mix_hbm)
    targets = (key_ref, value_ref, query_ref, forward_ref, backward_ref, mix_ref)
    copies = [
        pltpu.make_async_copy(source, target, sems.at[i])
        for i, (source, target) in enumerate(zip(sources, targets))
    ]
    for copy in copies:
        copy.start()
    for which, (ref, first) in enumerate(((key_ref, 0), (value_ref, 4))):
        copies[which].wait()
        for i in range(16):
            for group in range(4):
                lanes = slice(group * LANES, (group + 1) * LANES)
                out_ref[i, (first + group) * 32 : (first + group + 1) * 32] = ref[:, lanes]
    for copy in copies[2:]:
        copy.wait()
    row, col = grid_of((16, LANES))
    ranks = dot_tn(forward_ref[...], as_bf16(row == col)) + dot_tn(
        backward_ref[...], as_bf16(row + 16 == col)
    )
    packed = jnp.concatenate([ranks[8 * i : 8 * i + 8, :32] for i in range(4)], axis=1)
    for i, peer in enumerate(PLANE_GROUP):
        start = (peer // 4) * LANES
        out_ref[i, COLUMNS : COLUMNS + 32] = query_ref[:, start : start + LANES]
        out_ref[i, COLUMNS + 32 : COLUMNS + 48] = mix_ref[:, 2 * start : 2 * start + LANES]
        out_ref[i, COLUMNS + 48 : COLUMNS + 64] = mix_ref[:, 2 * start + LANES : 2 * start + 2 * LANES]
        out_ref[i, COLUMNS + 64 :] = packed.astype(bf16)


def join_kernel(first_ref, second_ref, out_ref):
    count = first_ref.shape[0]
    out_ref[:count] = first_ref[...]
    out_ref[count:] = second_ref[...]


def split_kernel(first_ref, second_ref, query_ref, mix_ref):
    for part, ref in enumerate((first_ref, second_ref)):
        query_ref[2 * part : 2 * part + 2] = ref[:, :, :32, :]
        mix_ref[2 * part : 2 * part + 2] = ref[:, :, 32:, :]


def slot_of(index, axis):
    apart = index ^ lax.axis_index(axis)
    return apart ^ (apart >> 1)


def normed_halves(tokens_ref, gain_ref):
    values = tokens_ref[...].astype(f32)
    scale = lax.rsqrt(jnp.mean(values * values, axis=-1, keepdims=True) + EPS)
    normed = (values * scale * gain_ref[...]).astype(bf16)
    return [
        jnp.concatenate(
            [normed[:, (2 * i + core) * 32 : (2 * i + core) * 32 + 32] for i in PLANE_GROUP], axis=1
        )
        for core in range(2)
    ]


def norm_kernel(tokens_ref, gain_ref, normed_ref):
    for core, half in enumerate(normed_halves(tokens_ref, gain_ref)):
        normed_ref[core] = half


def rates_of(ranks, up_forward_ref, up_backward_ref, bias_forward_ref, bias_backward_ref):
    gates = jnp.concatenate(
        [
            dot(ranks[:, :16], up_forward_ref[...]) + bias_forward_ref[...],
            dot(ranks[:, 16:32], up_backward_ref[...]) + bias_backward_ref[...],
        ],
        axis=1,
    )
    log_sigmoid = jnp.minimum(gates, 0.0) - jnp.log(1.0 + jnp.exp(-jnp.abs(gates)))
    return halves(log_sigmoid * (2.0 / (BLOCK * HEADS)))


def summed(parts, mask, way):
    row, col = grid_of((LANES, LANES))
    ones = as_bf16(mask(row, col) & ((row // BLOCK) == (col // BLOCK)))
    lanes = slice(way * WIDTH, (way + 1) * WIDTH)
    both = jnp.concatenate([part[:, lanes] for part in parts], axis=0)
    return dot(jnp.concatenate([ones, ones], axis=1), both)


def block_kernel(
    normed_ref, own_ref, other_ref, up_forward_ref, up_backward_ref,
    bias_forward_ref, bias_backward_ref, payload_ref, rounded_ref,
):
    core = lax.axis_index("dp_2")

    def columns(ref, first):
        return jnp.concatenate(
            [ref[:, g * 32 : (g + 1) * 32, :].reshape(WIDTH, LANES) for g in (first, first + 1)], axis=1
        )

    def rank_columns(ref):
        packed = ref[:, COLUMNS + 64 :, :].astype(f32)
        rows = jnp.stack([packed[:, :, 32 * i : 32 * i + 32] for i in range(4)], axis=1)
        return rows.reshape(WIDTH, 32).astype(bf16)

    rows = jnp.concatenate([normed_ref[core], normed_ref[1 - core]], axis=1)
    pieces = [
        dot(
            rows,
            jnp.concatenate([columns(own_ref, first), columns(other_ref, first)], axis=0),
        )
        for first in (0, 2, 4, 6)
    ]
    pieces.append(
        dot(rows, jnp.concatenate([rank_columns(own_ref), rank_columns(other_ref)], axis=0))
    )
    pieces.append(jnp.zeros((2 * BLOCK, LANES - 32), f32))
    rounded = jnp.concatenate(pieces, axis=1).astype(bf16)
    rounded_ref[...] = rounded
    values = rounded[:, WIDTH : 2 * WIDTH]
    parts = rates_of(
        rounded[:, 2 * WIDTH :], up_forward_ref, up_backward_ref, bias_forward_ref, bias_backward_ref
    )
    high, low = parts
    row, col = grid_of((LANES, LANES))
    fwd, bwd = slice(0, WIDTH), slice(WIDTH, 2 * WIDTH)
    keys32 = rounded[:, :WIDTH].astype(f32)
    remain = (
        halves(keys32 * jnp.exp(summed(parts, lambda r, c: c > r, 0))),
        halves(keys32 * jnp.exp(summed(parts, lambda r, c: c < r, 1))),
    )
    hrow, hcol = grid_of((HEADS, WIDTH))
    mine = hrow == hcol // HEAD
    erow, ecol = grid_of((WIDTH, LANES))
    fold = as_bf16(((erow // LANES) * HEAD + erow % HEAD) == ecol)
    srow, scol = grid_of((8, 128))
    pick = as_bf16(srow == scol // BLOCK)
    lines = []
    for span in (fwd, bwd):
        sums = dot(
            jnp.concatenate([pick, pick], axis=1),
            jnp.concatenate([high[:, span], low[:, span]], axis=0),
        )
        for seq in range(2):
            line = jnp.where(mine, sums[seq : seq + 1], 0.0)
            lines.append(
                line[:, :LANES] + line[:, LANES : 2 * LANES]
                + line[:, 2 * LANES : 3 * LANES] + line[:, 3 * LANES :]
            )
    close = dot(jnp.concatenate(halves(jnp.concatenate(lines, axis=1)), axis=0), fold)
    tail = lax.broadcasted_iota(jnp.int32, (HEADS, 8, LANES), 1)
    payload_ref[:, HEAD:, :] = jnp.where(
        tail == 0,
        close[:HEADS][:, None, :],
        jnp.where(tail == 1, close[HEADS:][:, None, :], 0.0),
    ).astype(bf16)
    drow, dcol = grid_of((LANES, 2 * LANES))
    diagonal = (drow // HEAD) == ((dcol % LANES) // HEAD)
    for group in range(4):
        lanes = slice(group * LANES, (group + 1) * LANES)
        value = values[:, lanes]
        empty = jnp.zeros((BLOCK, LANES), bf16)
        by_seq = jnp.concatenate(
            [
                jnp.concatenate([value[:BLOCK], empty], axis=0),
                jnp.concatenate([empty, value[BLOCK:]], axis=0),
            ],
            axis=1,
        )
        by_seq = jnp.concatenate([by_seq, by_seq], axis=0)
        parts = []
        for way in range(2):
            both = jnp.concatenate([half[:, lanes] for half in remain[way]], axis=0)
            state = dot_tn(both, by_seq)
            parts.append(jnp.where(diagonal, state, 0.0).astype(bf16))
        folded = dot(jnp.concatenate(parts, axis=1), fold).astype(bf16)
        payload_ref[4 * group : 4 * group + 4, :HEAD, :] = folded.reshape(4, HEAD, LANES)


def scan_kernel(payload_ref, out_ref):
    row, col = grid_of((LANES, LANES))
    spread = as_bf16((row // HEAD) == (col // HEAD))
    crow, ccol = grid_of((HEAD, LANES))
    mine = ccol % HEAD == crow
    lines = payload_ref[:, HEAD : HEAD + 8, :].astype(f32)
    closing = 0.0
    for part in range(2):
        line = jnp.where(mine[None], lines[:, part : part + 1, :], 0.0)
        closing = closing + dot(line.astype(bf16).reshape(WIDTH, LANES), spread)
    decay = jnp.exp(closing)
    states = payload_ref[:, :HEAD, :].astype(f32).reshape(WIDTH, LANES)
    lane = lax.broadcasted_iota(jnp.int32, (HEAD, LANES), 1)
    ahead = [None] * HEADS
    behind = [None] * HEADS

    def at(x, i):
        return x[i * HEAD : (i + 1) * HEAD, :]

    carried = jnp.zeros((HEAD, LANES), f32)
    order = [GROUP.index(z) for z in range(HEADS)]
    for i in order:
        ahead[i] = carried
        carried = at(decay, i) * carried + at(states, i)
    carried = jnp.zeros((HEAD, LANES), f32)
    for i in reversed(order):
        behind[i] = carried
        carried = at(decay, i) * carried + at(states, i)
    for i in range(HEADS):
        out_ref[i * HEAD : (i + 1) * HEAD, :] = jnp.where(
            lane < LANES // 2, ahead[i], behind[i]
        ).astype(bf16)


def query_kernel(
    tokens_ref, gain_ref, own_ref, other_ref, rounded_ref, up_forward_ref, up_backward_ref,
    bias_forward_ref, bias_backward_ref, out_ref,
):
    core = lax.axis_index("dp_2")

    def weights(ref):
        return jnp.concatenate(
            [
                ref[slot_of(quarter, "dp_0")].reshape(WIDTH, LANES)
                for quarter in range(4)
            ],
            axis=1,
        )

    first, second = normed_halves(tokens_ref, gain_ref)
    projected = dot(jnp.where(core == 0, first, second), weights(own_ref)) + dot(
        jnp.where(core == 0, second, first), weights(other_ref)
    )
    queries = projected.astype(bf16).astype(f32) * HEAD ** (-0.5)
    keys = rounded_ref[:, :WIDTH].astype(f32)
    parts = rates_of(
        rounded_ref[:, 2 * WIDTH :], up_forward_ref, up_backward_ref, bias_forward_ref, bias_backward_ref
    )
    decayed, inverse = [], []
    for way, mask in ((0, lambda r, c: c <= r), (1, lambda r, c: c >= r)):
        running = summed(parts, mask, way)
        product = queries * jnp.exp(running)
        out_ref[:, (way + 1) * WIDTH : (way + 2) * WIDTH] = product
        decayed.append(product.astype(bf16))
        inverse.append((keys * jnp.exp(-running)).astype(bf16))
    row, col = grid_of((WIDTH, WIDTH))
    natural = ((col % 256) // 16) * HEAD + (col // 256) * 16 + col % 16
    values = dot(rounded_ref[:, WIDTH : 2 * WIDTH], as_bf16(row == natural)).astype(bf16)
    row, col = grid_of((WIDTH, 256))
    own_lanes = as_bf16((row // BLOCK) == (col // HEAD))
    srow, scol = grid_of((WIDTH, BLOCK))
    lower = (srow % BLOCK) >= scol
    upper = (srow % BLOCK) <= scol
    vrow, vcol = grid_of((WIDTH, LANES))
    own_values = (vrow // BLOCK) == (vcol // 16)
    for seq in range(2):
        span = slice(seq * BLOCK, (seq + 1) * BLOCK)
        for group in range(2):
            wide = slice(group * 256, (group + 1) * 256)
            scores = 0.0
            for way, mask in ((0, lower), (1, upper)):
                stacked = jnp.concatenate([decayed[way][span, wide]] * 8, axis=0) * own_lanes
                scores = scores + jnp.where(mask, dot_nt(stacked, inverse[way][span, wide]), 0.0)
            scores = scores.astype(bf16)
            for half in range(2):
                start = half * 256 + group * LANES
                spread = dot(scores, values[span, start : start + LANES])
                spread = jnp.where(own_values, spread, 0.0)
                total = spread[:BLOCK]
                for head in range(1, 8):
                    total = total + spread[head * BLOCK : (head + 1) * BLOCK]
                out_ref[span, start : start + LANES] = total


def out_kernel(
    states_ref, parts_ref, gain_ref, own_ref, other_ref, out_ref
):
    spans = [slice(seq * BLOCK, (seq + 1) * BLOCK) for seq in range(2)]
    core = lax.axis_index("dp_2")
    row, col = grid_of((LANES, LANES))
    lead = row - col % 16
    widen = jnp.concatenate([as_bf16(lead == 16 * i) for i in range(8)], axis=1)
    row, col = grid_of((256, LANES))
    diagonal = (row // HEAD) == (col // 16)
    full = []
    for g in range(2):
        wide = dot(states_ref[g * 256 : (g + 1) * 256, :], widen)
        full.append(
            [
                jnp.where(diagonal, wide[:, i * LANES : (i + 1) * LANES], 0.0).astype(bf16)
                for i in range(8)
            ]
        )
    totals = [[], []]
    for seq, span in enumerate(spans):
        sides = [[], []]
        for group in range(2):
            queries = jnp.concatenate(
                [
                    parts_ref[span, (way + 1) * WIDTH + group * 256 : (way + 1) * WIDTH + group * 256 + 256]
                    for way in range(2)
                ],
                axis=1,
            )
            right = jnp.concatenate(
                [
                    jnp.concatenate(full[group][4 * way + 2 * seq : 4 * way + 2 * seq + 2], axis=1)
                    for way in range(2)
                ],
                axis=0,
            )
            across = dot(jnp.concatenate(halves(queries), axis=0), right)
            across = across[:BLOCK] + across[BLOCK:]
            for half in range(2):
                start = half * 256 + group * LANES
                sides[half].append(
                    parts_ref[span, start : start + LANES] + across[:, half * LANES : (half + 1) * LANES]
                )
        for half in range(2):
            totals[half].append(jnp.concatenate(sides[half], axis=1))
    combined = [jnp.concatenate(total, axis=0) for total in totals]
    high, low = halves(combined[0] * combined[0] + combined[1] * combined[1])
    row, col = grid_of((256, 256))
    ones = as_bf16((row // 16) == (col // 16))
    sums = dot(jnp.concatenate([high, low], axis=1), jnp.concatenate([ones, ones], axis=0))
    scale = lax.rsqrt(sums * (1.0 / HEAD) + EPS)
    attended = [
        (combined[half] * scale * gain_ref[half : half + 1, :]).astype(bf16) for half in range(2)
    ]
    mine = jnp.where(core == 0, attended[0], attended[1])
    theirs = jnp.where(core == 0, attended[1], attended[0])
    both = jnp.concatenate([mine, theirs], axis=1)
    for quarter in range(4):
        slot = slot_of(quarter, "dp_0")

        def weights(ref):
            return jnp.concatenate(
                [
                    jnp.concatenate(
                        [ref[slot, 1:, rows : rows + 16, :], ref[slot, :1, rows : rows + 16, :]], axis=0
                    ).reshape(256, LANES)
                    for rows in (0, 16)
                ],
                axis=1,
            )

        out_ref[:, quarter * 256 : (quarter + 1) * 256] = dot(
            both, jnp.concatenate([weights(own_ref), weights(other_ref)], axis=0)
        ).astype(bf16)


VMEM = pl.BlockSpec(memory_space=pltpu.VMEM)


def call(kernel, outs, specs, cycles, *args, scratch=()):
    many = isinstance(outs, tuple)
    return pl.pallas_call(
        kernel,
        out_shape=outs,
        in_specs=specs,
        out_specs=(VMEM,) * len(outs) if many else VMEM,
        scratch_shapes=scratch,
        cost_estimate=pl.CostEstimate(flops=cycles, bytes_accessed=1 << 20, transcendentals=0),
        compiler_params=pltpu.CompilerParams(vmem_limit_bytes=16 << 20),
    )(*args)


def in_hbm(x):
    return pltpu.with_memory_space_constraint(x, pltpu.HBM)


def swapped(x):
    return lax.ppermute(x, "dp_2", [(0, 1), (1, 0)])


def body(
    tokens, norm_gain, w_query, w_key, w_value, w_rank_forward, w_rank_backward,
    up_forward, up_backward, bias_forward, bias_backward, out_gain, w_out,
):
    seqs, toks, width = tokens.shape
    rows = seqs * toks
    shape = jax.ShapeDtypeStruct
    tokens_flat, gain_flat = tokens.reshape(rows, width), norm_gain.reshape(1, width)
    hbm = pl.BlockSpec(memory_space=pltpu.HBM)
    sources = [
        in_hbm(x)
        for x in (w_key, w_value, w_query, w_rank_forward.T, w_rank_backward.T, w_out)
    ]
    send = call(
        pack_kernel, shape((16, SENT, LANES), bf16), [hbm] * 6, 1 << 26, *sources,
        scratch=[pltpu.VMEM(x.shape, bf16) for x in sources] + [pltpu.SemaphoreType.DMA((6,))],
    )
    own = lax.all_to_all(send, PLANE, 0, 0, axis_index_groups=[PLANE_GROUP])
    other = swapped(own)
    mix = own[None, :, COLUMNS : COLUMNS + 64, :]
    for step, flip in enumerate((1, 3)):
        arrived = lax.ppermute(mix, "dp_0", [(i, i ^ flip) for i in range(4)])
        if step == 0:
            mix = call(
                join_kernel, shape((2, 16, 64, LANES), bf16), [VMEM] * 2, 1 << 26, mix, arrived
            )
        else:
            query, mix = call(
                split_kernel,
                (pltpu.HBM((4, 16, 32, LANES), bf16), shape((4, 16, 32, LANES), bf16)),
                [VMEM] * 2, 1 << 26,
                mix, arrived,
            )
    normed = call(
        norm_kernel, shape((2, rows, 512), bf16), [VMEM, VMEM], 1 << 28,
        tokens_flat, gain_flat,
    )
    decays = (
        up_forward, up_backward, bias_forward.reshape(1, WIDTH), bias_backward.reshape(1, WIDTH)
    )
    payload, rounded = call(
        block_kernel,
        (
            shape((HEADS, 40, LANES), bf16), pltpu.HBM((rows, ALL), bf16),
        ),
        [VMEM] * 7, 1 << 30, normed, own, other, *decays,
    )
    inbound = lax.all_to_all(payload, "sp", 0, 0, axis_index_groups=[GROUP])
    query_other = swapped(query)
    mix_other = swapped(mix)
    states = call(
        scan_kernel, shape((WIDTH, LANES), bf16), [VMEM], 1 << 28,
        inbound,
    )
    returned = lax.all_to_all(
        states.reshape(HEADS, HEAD, LANES), "sp", 0, 0, axis_index_groups=[GROUP]
    )
    parts = call(
        query_kernel, shape((rows, 3 * WIDTH), f32), [VMEM] * 9, 1 << 30,
        in_hbm(tokens_flat), gain_flat, in_hbm(query), query_other, in_hbm(rounded), *decays,
    )
    gain = jnp.tile(out_gain.reshape(2, 1, 16), (1, HEADS, 1)).reshape(2, 256)
    mixed = call(
        out_kernel, shape((rows, width), bf16), [VMEM] * 5, 1 << 30,
        returned.reshape(WIDTH, LANES), parts, gain, mix, mix_other,
    )
    return mixed.reshape(seqs, toks, width)


def solution(mesh):
    finer = Mesh(mesh.devices.reshape(mesh.shape["sp"], 4, 4, 2), ("sp", "dp_0", "dp_1", "dp_2"))
    rows = P(DP, None)
    in_specs = (
        P(DP, "sp", None), P(), rows, rows, rows, rows, rows, P(), P(), P(), P(), P(), rows,
    )

    return jax.shard_map(
        body, mesh=finer, in_specs=in_specs, out_specs=P(DP, "sp", None), check_vma=False
    )
```
